512 devices in a mesh: ep: 128 (over z, y, core), tp: 4 (over x).
Axes of the slice: x: 4, y: 8, z: 8, core: 2. Of those that a mesh axis runs over, the one named last changes fastest.
Arguments:
- tokens: bfloat16 [1024, 1024], P('ep'), may hold values from -6 to 6
- mix_gain: float32 [1024], replicated, may hold values from 0.1 to 1.9
- w_query: bfloat16 [1024, 512], P(None, 'tp'), may hold values from -0.1875 to 0.1875
- w_key: bfloat16 [1024, 512], P(None, 'tp'), may hold values from -0.1875 to 0.1875
- w_value: bfloat16 [1024, 1024], P(None, 'tp'), may hold values from -0.1875 to 0.1875
- w_ogate: bfloat16 [1024, 1024], P(None, 'tp'), may hold values from -0.1875 to 0.1875
- w_igate: bfloat16 [1024, 4], replicated, may hold values from -0.1875 to 0.1875
- w_fgate: bfloat16 [1024, 4], replicated, may hold values from -0.1875 to 0.1875
- forget_bias: float32 [4], replicated, may hold values from -1 to 3
- head_gain: float32 [1024], P('tp'), may hold values from 0.1 to 1.9
- w_out: bfloat16 [1024, 1024], P('tp'), may hold values from -0.1875 to 0.1875
- memory: float32 [1024, 4, 128, 256], P('ep', 'tp'), may hold values from -0.4 to 0.4
- normalizer: float32 [1024, 4, 128], P('ep', 'tp'), may hold values from -0.4 to 0.4
- running_max: float32 [1024, 4], P('ep', 'tp'), may hold values from -4 to 4
- ffn_gain: float32 [1024], replicated, may hold values from 0.1 to 1.9
- route: int32 [1024, 2], replicated, may hold values from 0 to 127, all different within a row; in each aligned block of 1024 rows (0 to 1023, 1024 to 2047, ...) at most 32 rows name the same one
- route_weight: float32 [1024, 2], replicated, may hold values from 0.05 to 1
- w_gate: bfloat16 [128, 1024, 512], P('ep', None, 'tp'), may hold values from -0.1875 to 0.1875
- w_up: bfloat16 [128, 1024, 512], P('ep', None, 'tp'), may hold values from -0.1875 to 0.1875
- w_down: bfloat16 [128, 512, 1024], P('ep', 'tp'), may hold values from -0.25 to 0.25
Outputs:
- mixed: bfloat16 [1024, 1024], P(None, 'ep')
- new_memory: float32 [1024, 4, 128, 256], P('ep', 'tp')
- new_normalizer: float32 [1024, 4, 128], P('ep', 'tp')
- new_max: float32 [1024, 4], P('ep', 'tp')
The draws below stay inside these ranges and needn't reach their ends.
Inputs may be any that keep to these rules, and one draw needn't show every extreme that they name: `route`: each expert is named by at most 32 routes in all, a bound that some block reaches; the two choices of a token differ.
All inputs are finite; a program needn't handle non-finite values.
Results may differ from the reference program's by a relative error of at most 0.014.
Values may be sent and summed in bfloat16 or wider, within the bound.
A program may use at most 64 MiB of HBM per device.

```python
import math
import jax
import jax.numpy as jnp
import numpy as np
from jax import lax

MODEL_WIDTH = 1024
HEADS = 4
QK = 128
DV = 256
EXPERT_HIDDEN = 512
TOPK = 2
TOKENS = 1024
EXPERTS = 128
EXPERT_CAPACITY = 32
N_TP = 4


def shard_levels(key, shape, split, low, largest):
    def one(dim, blocks):
        steps = jax.random.uniform(jax.random.fold_in(jax.random.fold_in(key, 6), dim), (blocks,), jnp.float32, low / len(split), largest / len(split))
        return jnp.repeat(jnp.exp(steps), shape[dim] // blocks).reshape((-1,) + (1,) * (len(shape) - dim - 1))

    level = one(*split[0])
    for cut in split[1:]:
        level = level * one(*cut)
    return level


def shared_out(key, own, number, rows, number_of, top, reach, lean):
    ranking = jax.random.permutation(key, number_of)
    packed, common = load_shares(number_of, rows * top, reach, lean, True), load_shares(number_of, rows * top, reach, lean, False)
    places = jnp.arange(number_of)

    def named(sizes, turn):
        used = int((sizes > 0).sum())
        fixed = max(1, used // 4)
        shifted = fixed + (places - fixed + turn * (used - fixed)) % max(1, number_of - fixed)
        return jnp.zeros((number_of,), jnp.int32).at[ranking[jnp.where(places < fixed, places, shifted)]].set(jnp.asarray(sizes, jnp.int32))

    sizes = jnp.where(number % 4 == 0, named(packed, number // 4), named(common, number - number // 4 - 1))
    mixed = jax.random.permutation(jax.random.fold_in(own, 3), number_of)
    source_of, taker = mixed[0:number_of // 2 * 2:2], mixed[1:number_of // 2 * 2:2]
    room = jnp.minimum(sizes[source_of] - 1, reach - sizes[taker]) // 2
    room = jnp.where((source_of == ranking[0]) | (taker == ranking[0]) | (sizes[taker] == 0), 0, jnp.maximum(room, 0))
    shifted = jax.random.randint(jax.random.fold_in(own, 4), (number_of // 2,), 0, 1 << 20) % (room + 1)
    sizes = sizes.at[source_of].add(-shifted).at[taker].add(shifted)
    items = jnp.searchsorted(jnp.cumsum(sizes), jnp.arange(rows * top), side="right").astype(jnp.int32)
    table = items.reshape(top, rows).T
    table = table[jax.random.permutation(jax.random.fold_in(own, 1), rows)]
    turn = jax.random.randint(jax.random.fold_in(own, 2), (rows, 1), 0, top)
    return jnp.take_along_axis(table, (jnp.arange(top)[None, :] + turn) % top, axis=1)


def load_shares(amount, total, most, skew, full):
    portions = [(1 << 20) // math.isqrt(rank ** skew) + 1 for rank in range(1, amount + 1)]
    largest = most if full else min(most, max(-(-total // amount), total * portions[0] // sum(portions)))
    least = 1 if total - largest >= amount - 1 else 0
    holding, spare = [largest] + [least] * (amount - 1), total - largest - least * (amount - 1)
    while spare > 0:
        free = [i for i in range(1, amount) if holding[i] < largest] or [i for i in range(1, amount) if holding[i] < most]
        whole, remaining = sum([portions[i] for i in free]), spare
        for i in free:
            addition = min(most - holding[i], max(1, remaining * portions[i] // whole), spare)
            holding[i] = holding[i] + addition
            spare = spare - addition
    return np.array(holding)


def scatter_about(key, dims, scale, most, split=(), kind=jnp.bfloat16):
    entries = scale * jax.random.normal(key, dims, jnp.float32)
    if split:
        entries = entries * shard_levels(key, dims, split, -0.22, 0.18)
    return jnp.clip(entries, -most, most).astype(kind)


def setup_inputs(seed: int = 0) -> dict:
    arg_keys = jax.random.split(jax.random.key(seed), 21)
    tokens = scatter_about(arg_keys[0], (TOKENS, MODEL_WIDTH), 1.0, 6.0, ((0, 128),))
    mix_gain = jnp.clip(1.0 + 0.18 * jax.random.normal(arg_keys[1], (MODEL_WIDTH,), jnp.float32), 0.1, 1.9)
    w_query = scatter_about(arg_keys[2], (MODEL_WIDTH, HEADS * QK), MODEL_WIDTH ** -0.5, 0.1875, ((1, 4),))
    w_key = scatter_about(arg_keys[3], (MODEL_WIDTH, HEADS * QK), MODEL_WIDTH ** -0.5, 0.1875, ((1, 4),))
    w_value = scatter_about(arg_keys[4], (MODEL_WIDTH, HEADS * DV), MODEL_WIDTH ** -0.5, 0.1875, ((1, 4),))
    w_ogate = scatter_about(arg_keys[5], (MODEL_WIDTH, HEADS * DV), MODEL_WIDTH ** -0.5, 0.1875, ((1, 4),))
    w_igate = scatter_about(arg_keys[6], (MODEL_WIDTH, HEADS), MODEL_WIDTH ** -0.5, 0.1875)
    w_fgate = scatter_about(arg_keys[7], (MODEL_WIDTH, HEADS), MODEL_WIDTH ** -0.5, 0.1875)
    forget_bias = jnp.clip(jax.random.uniform(arg_keys[8], (HEADS,), jnp.float32, -1.0, 3.0), -1.0, 3.0)
    head_gain = jnp.clip(1.0 + 0.18 * jax.random.normal(arg_keys[9], (HEADS * DV,), jnp.float32), 0.1, 1.9)
    w_out = scatter_about(arg_keys[10], (HEADS * DV, MODEL_WIDTH), (HEADS * DV) ** -0.5, 0.1875, ((0, 4),))
    memory = scatter_about(arg_keys[11], (TOKENS, HEADS, QK, DV), 0.06, 0.4, ((0, 128), (1, 4)), jnp.float32)
    normalizer = scatter_about(arg_keys[12], (TOKENS, HEADS, QK), 0.06, 0.4, ((0, 128), (1, 4)), jnp.float32)
    running_max = scatter_about(arg_keys[13], (TOKENS, HEADS), 1.0, 4.0, ((0, 128), (1, 4)), jnp.float32)
    ffn_gain = jnp.clip(1.0 + 0.18 * jax.random.normal(arg_keys[14], (MODEL_WIDTH,), jnp.float32), 0.1, 1.9)
    route_keys = jax.random.split(jax.random.fold_in(arg_keys[15], 1), TOKENS // TOKENS)
    route_turns = jax.random.permutation(jax.random.fold_in(arg_keys[15], 3), TOKENS // TOKENS)
    route = jax.vmap(lambda own, number: shared_out(jax.random.fold_in(arg_keys[15], 2), own, number, TOKENS, EXPERTS, TOPK, EXPERT_CAPACITY, 2))(route_keys, route_turns).reshape((TOKENS, TOPK))
    route_weight = jnp.clip(jnp.exp(jax.random.uniform(arg_keys[16], (TOKENS, TOPK), jnp.float32, math.log(0.05), math.log(1.0))), 0.05, 1.0)
    w_gate = scatter_about(arg_keys[17], (EXPERTS, MODEL_WIDTH, EXPERT_HIDDEN), MODEL_WIDTH ** -0.5, 0.1875, ((0, 128), (2, 4)))
    w_up = scatter_about(arg_keys[18], (EXPERTS, MODEL_WIDTH, EXPERT_HIDDEN), MODEL_WIDTH ** -0.5, 0.1875, ((0, 128), (2, 4)))
    w_down = scatter_about(arg_keys[19], (EXPERTS, EXPERT_HIDDEN, MODEL_WIDTH), EXPERT_HIDDEN ** -0.5, 0.25, ((0, 128), (1, 4)))
    return dict(tokens=tokens, mix_gain=mix_gain, w_query=w_query, w_key=w_key, w_value=w_value, w_ogate=w_ogate, w_igate=w_igate, w_fgate=w_fgate, forget_bias=forget_bias, head_gain=head_gain, w_out=w_out, memory=memory, normalizer=normalizer, running_max=running_max, ffn_gain=ffn_gain, route=route, route_weight=route_weight, w_gate=w_gate, w_up=w_up, w_down=w_down)


EPS = 1e-06

def round_trip(values):
    rounded = lax.optimization_barrier(values.astype(jnp.bfloat16))
    return rounded.astype(jnp.float32)

def norm_rows(values, gain):
    floats = values.astype(jnp.float32)
    scale = lax.rsqrt(lax.optimization_barrier(jnp.mean(floats * floats, axis=-1, keepdims=True)) + EPS)
    return (floats * scale * gain.astype(jnp.float32)).astype(jnp.bfloat16)

def slot_targets(route):
    flat = route.reshape(-1).astype(jnp.int32)
    onehot = (flat[:, None] == jnp.arange(EXPERTS, dtype=jnp.int32)[None, :]).astype(jnp.int32)
    before = jnp.cumsum(onehot, axis=0) - onehot
    slot = lax.optimization_barrier(jnp.sum(before * onehot, axis=1))
    return (flat * EXPERT_CAPACITY + slot).astype(jnp.int32)

def reference(tokens, mix_gain, w_query, w_key, w_value, w_ogate, w_igate, w_fgate, forget_bias, head_gain, w_out, memory, normalizer, running_max, ffn_gain, route, route_weight, w_gate, w_up, w_down):
    count = tokens.shape[0]
    normed = norm_rows(tokens, mix_gain)

    def project(weight, size):
        result = jnp.dot(normed, weight, preferred_element_type=jnp.float32)
        return round_trip(result).reshape(count, HEADS, size)
    query = project(w_query, QK)
    scaled_key = project(w_key, QK) * QK ** (-0.5)
    value = project(w_value, DV)
    ogate = project(w_ogate, DV)
    log_in = jnp.dot(normed, w_igate, preferred_element_type=jnp.float32)
    log_forget = jax.nn.log_sigmoid(jnp.dot(normed, w_fgate, preferred_element_type=jnp.float32) + forget_bias.astype(jnp.float32))
    new_max = jnp.maximum(log_forget + running_max, log_in)
    keep = jnp.exp(log_forget + running_max - new_max)
    admit = jnp.exp(log_in - new_max)
    floor = jnp.exp(-new_max)

    def per_head(items):
        state, norm_state, q_head, k_head, v_head, keep_head, admit_head, floor_head = items
        state = keep_head[:, None, None] * state + admit_head[:, None, None] * k_head[:, :, None] * v_head[:, None, :]
        norm_state = keep_head[:, None] * norm_state + admit_head[:, None] * k_head
        numer = jnp.einsum('tk,tkv->tv', q_head, state, precision=lax.Precision.HIGHEST)
        denom = lax.optimization_barrier(jnp.sum(q_head * norm_state, axis=1))
        read = numer / jnp.maximum(jnp.abs(denom), floor_head)[:, None]
        return (state, norm_state, read)
    heads_first = lambda a: jnp.moveaxis(a, 1, 0)
    states, norms, reads = lax.map(per_head, (heads_first(memory), heads_first(normalizer), heads_first(query), heads_first(scaled_key), heads_first(value), keep.T, admit.T, floor.T))
    new_memory = jnp.moveaxis(states, 0, 1)
    new_normalizer = jnp.moveaxis(norms, 0, 1)
    read = jnp.moveaxis(reads, 0, 1)
    scale = lax.rsqrt(lax.optimization_barrier(jnp.mean(read * read, axis=-1, keepdims=True)) + EPS)
    gated = (jax.nn.sigmoid(ogate) * read * scale * head_gain.reshape(HEADS, DV)).astype(jnp.bfloat16)
    partials = jnp.einsum('thv,hvd->htd', gated.astype(jnp.float32), w_out.reshape(HEADS, DV, MODEL_WIDTH).astype(jnp.float32))
    cell_out = lax.optimization_barrier(jnp.sum(round_trip(partials), axis=0))
    middle = (tokens.astype(jnp.float32) + cell_out).astype(jnp.bfloat16)
    routed_in = norm_rows(middle, ffn_gain)
    targets = slot_targets(route)
    slots = jnp.zeros((EXPERTS * EXPERT_CAPACITY, MODEL_WIDTH), jnp.bfloat16).at[targets].set(jnp.repeat(routed_in, TOPK, axis=0)).reshape(EXPERTS, EXPERT_CAPACITY, MODEL_WIDTH)

    def expert(items):
        rows, gate_m, up_m, down_matrix = items
        gate_v = jnp.dot(rows, gate_m, preferred_element_type=jnp.float32)
        up_v = jnp.dot(rows, up_m, preferred_element_type=jnp.float32)
        activation = (jax.nn.silu(gate_v) * up_v).astype(jnp.bfloat16)
        partial_pieces = jnp.einsum('pxt,xtl->xpl', activation.reshape(EXPERT_CAPACITY, N_TP, EXPERT_HIDDEN // N_TP).astype(jnp.float32), down_matrix.reshape(N_TP, EXPERT_HIDDEN // N_TP, MODEL_WIDTH).astype(jnp.float32))
        return lax.optimization_barrier(jnp.sum(round_trip(partial_pieces), axis=0)).astype(jnp.bfloat16)
    results = lax.map(expert, (slots, w_gate, w_up, w_down))
    picked = results.reshape(EXPERTS * EXPERT_CAPACITY, MODEL_WIDTH)[targets].reshape(count, TOPK, MODEL_WIDTH).astype(jnp.float32)
    weights = route_weight / lax.optimization_barrier(jnp.sum(route_weight, axis=1, keepdims=True))
    mixed = (middle.astype(jnp.float32) + lax.optimization_barrier(jnp.sum(picked * weights[:, :, None], axis=1))).astype(jnp.bfloat16)
    return (mixed, new_memory, new_normalizer, new_max)
```

```python
import functools

import jax
import jax.numpy as jnp
from jax import lax
from jax.experimental import pallas as pl
from jax.experimental.pallas import tpu as pltpu
from jax.sharding import Mesh
from jax.sharding import PartitionSpec as P

MESH = pl.DeviceIdType.MESH
CAP = 32
LANES = 128
EPS = 1e-06
F32 = jnp.float32
BF16 = jnp.bfloat16


def dot(a, b):
    return jnp.dot(a, b, preferred_element_type=F32)


def kernel(
    sizes,
    tok_h,
    mix_h,
    wq_h,
    wk_h,
    wv_h,
    wo_h,
    wi_h,
    wf_h,
    fb_h,
    hg_h,
    wout_h,
    mem_h,
    nrm_h,
    rmax_h,
    fg_h,
    route_h,
    rw_h,
    wgate_h,
    wup_h,
    wdown_h,
    mixed_ref,
    keep_ref,
    akey_ref,
    value_ref,
    newnorm_ref,
    newmax_ref,
    tok,
    mix,
    wq,
    wk,
    wv,
    wo,
    wi,
    wf,
    fb,
    hg,
    wout,
    mem,
    nrm,
    rmax,
    fg,
    route,
    rw,
    wgate,
    wup,
    wdown,
    load_sem,
    tgt,
    place,
    psend,
    precv,
    csend,
    crecv,
    esend,
    erecv,
    rsend,
    rrecv,
    stage,
    dsend,
    frecv,
    psem,
    csem,
    esem,
    rsem,
    dsem,
):
    nz, ny, nc, nx = sizes
    z, y, c, x = (lax.axis_index(a) for a in ("z", "y", "c", "x"))
    zy = z * ny + y
    ep = zy * nc + c
    rows, width = tok.shape
    groups = nx * nc
    quarter = width // nx
    chips = nz * ny
    owned = width // (chips * nc)
    owners = LANES // owned
    group = x * nc + c
    expert_count = chips * nc
    token_count = route.shape[1]

    hbm = (tok_h, mix_h, wq_h, wk_h, wv_h, wo_h, wi_h, wf_h, fb_h, hg_h, wout_h, mem_h, nrm_h, rmax_h)
    hbm += (fg_h, route_h, rw_h, wgate_h, wup_h, wdown_h)
    vmem = (tok, mix, wq, wk, wv, wo, wi, wf, fb, hg, wout, mem, nrm, rmax)
    vmem += (fg, route, rw, wgate, wup, wdown)
    loads = [pltpu.make_async_copy(h, v, load_sem.at[i]) for i, (h, v) in enumerate(zip(hbm, vmem))]
    for load in loads:
        load.start()

    barrier = pltpu.get_barrier_semaphore()

    def greet(target):
        pl.semaphore_signal(barrier, inc=1, device_id=target, device_id_type=MESH)

    def greet_plane(i, carry):
        tz, ty = lax.rem(z + i // ny, nz), lax.rem(y + i % ny, ny)

        @pl.when(i > 0)
        def _():
            greet((tz, ty, c, x))

        for dc in range(1, nc):
            greet((tz, ty, lax.rem(c + dc, nc), x))
        return carry

    lax.fori_loop(0, chips, greet_plane, 0)
    for dx in range(1, nx):
        for dc in range(nc):
            greet((z, y, lax.rem(c + dc, nc), lax.rem(x + dx, nx)))
    source_group = ep // owners
    source_x, source_c = source_group // nc, source_group % nc
    from_self = source_group == group

    def greet_sources(i, carry):
        tz, ty = lax.rem(z + i // ny, nz), lax.rem(y + i % ny, ny)

        @pl.when(jnp.logical_or(i > 0, jnp.logical_not(from_self)))
        def _():
            greet((tz, ty, source_c, source_x))

        return carry

    lax.fori_loop(0, chips, greet_sources, 0)

    for i in range(14):
        loads[i].wait()
    tokens = tok[...].astype(F32)
    mean = jnp.mean(tokens * tokens, axis=1, keepdims=True)
    normed = (tokens * lax.rsqrt(mean + EPS) * mix[...]).astype(BF16)
    query16 = dot(normed, wq[...]).astype(BF16)
    query = query16.astype(F32)
    qk = wq.shape[1]
    scaled_key = dot(normed, wk[...]).astype(BF16).astype(F32) * qk ** (-0.5)
    value = dot(normed, wv[...]).astype(BF16).astype(F32)
    ogate = dot(normed, wo[...]).astype(BF16).astype(F32)
    floats = normed.astype(F32)
    head_row = lax.broadcasted_iota(jnp.int32, wi.shape, 0) == x
    in_row = jnp.sum(jnp.where(head_row, wi[...].astype(F32), 0.0), axis=0, keepdims=True)
    forget_row = jnp.sum(jnp.where(head_row, wf[...].astype(F32), 0.0), axis=0, keepdims=True)
    log_in = jnp.sum(floats * in_row, axis=1, keepdims=True)
    head_lane = lax.broadcasted_iota(jnp.int32, fb.shape, 1) == x
    bias = jnp.sum(jnp.where(head_lane, fb[...], 0.0), axis=1, keepdims=True)
    forget_pre = jnp.sum(floats * forget_row, axis=1, keepdims=True) + bias
    log_forget = jnp.minimum(forget_pre, 0.0) - jnp.log1p(jnp.exp(-jnp.abs(forget_pre)))
    diagonal = lax.broadcasted_iota(jnp.int32, (rows, rows), 0) == lax.broadcasted_iota(
        jnp.int32, (rows, rows), 1
    )
    old_max = jnp.sum(
        jnp.where(diagonal, jnp.broadcast_to(rmax[...], (rows, rows)), 0.0), axis=1, keepdims=True
    )
    carried = log_forget + old_max
    new_max = jnp.maximum(carried, log_in)
    keep = jnp.exp(carried - new_max)
    admit = jnp.exp(log_in - new_max)
    akey = admit * scaled_key
    norm_state = keep * nrm[...] + akey
    keep_ref[...] = jnp.broadcast_to(keep, keep_ref.shape)
    akey_ref[...] = akey
    value_ref[...] = value
    newnorm_ref[...] = norm_state
    newmax_ref[...] = jnp.sum(
        jnp.where(diagonal, jnp.broadcast_to(new_max, (rows, rows)), 0.0), axis=0, keepdims=True
    )
    row_of = lax.broadcasted_iota(jnp.int32, value.shape, 0)
    kept = jnp.zeros_like(value)
    for t in range(rows):
        kept = jnp.where(row_of == t, dot(query16, mem[t].astype(BF16)), kept)
    numer = keep * kept + jnp.sum(query * akey, axis=1, keepdims=True) * value
    denom = jnp.sum(query * norm_state, axis=1, keepdims=True)
    read = numer / jnp.maximum(jnp.abs(denom), jnp.exp(-new_max))
    scale = lax.rsqrt(jnp.mean(read * read, axis=1, keepdims=True) + EPS)
    gated = (jax.nn.sigmoid(ogate) * read * scale * hg[...]).astype(BF16)
    partial = dot(gated, wout[...]).astype(BF16)
    for i in range(nx):
        psend[i] = partial[:, i * quarter : (i + 1) * quarter]

    loads[15].wait()
    expert_of = lax.broadcasted_iota(jnp.int32, (expert_count, token_count), 0)
    named = [expert_of == route[j : j + 1, :] for j in range(2)]
    either = jnp.where(jnp.logical_or(named[0], named[1]), 1.0, 0.0)
    block = min(256, token_count)
    earlier = (
        lax.broadcasted_iota(jnp.int32, (block, block), 0)
        < lax.broadcasted_iota(jnp.int32, (block, block), 1)
    ).astype(F32).astype(BF16)
    carry = jnp.zeros((expert_count, 1), F32)
    before = []
    for b in range(token_count // block):
        part = either[:, b * block : (b + 1) * block]
        before.append(dot(part.astype(BF16), earlier) + carry)
        carry = carry + jnp.sum(part, axis=1, keepdims=True)
    before = jnp.concatenate(before, axis=1)
    for j in range(2):
        slot = jnp.sum(jnp.where(named[j], before, 0.0), axis=0, keepdims=True)
        tgt[j : j + 1, :] = route[j : j + 1, :] * CAP + slot.astype(jnp.int32)
    slots_here = nc * CAP
    slot_id = lax.broadcasted_iota(jnp.int32, (slots_here, token_count), 0) + zy * slots_here
    hit = jnp.logical_or(slot_id == tgt[0:1, :], slot_id == tgt[1:2, :])
    place[...] = jnp.where(hit, 1.0, 0.0).astype(BF16)

    own_target = jnp.where(from_self, 1, 0)
    pl.semaphore_wait(barrier, chips * nc - 1 + (nx - 1) * nc + owners * nx - own_target)

    for dx in range(1, nx):
        tx = lax.rem(x + dx, nx)
        pltpu.make_async_remote_copy(
            src_ref=psend.at[tx],
            dst_ref=precv.at[dx - 1],
            send_sem=psem.at[0, dx - 1],
            recv_sem=psem.at[1, dx - 1],
            device_id=(z, y, c, tx),
            device_id_type=MESH,
        ).start()
    total = psend[x].astype(F32)
    for dx in range(1, nx):
        copy = pltpu.make_async_remote_copy(
            src_ref=psend.at[0],
            dst_ref=precv.at[dx - 1],
            send_sem=psem.at[0, dx - 1],
            recv_sem=psem.at[1, dx - 1],
            device_id=(z, y, c, lax.rem(x + dx, nx)),
            device_id_type=MESH,
        )
        copy.wait_recv()
        total = total + precv[dx - 1].astype(F32)
    own = tok[:, pl.ds(pl.multiple_of(x * quarter, quarter), quarter)].astype(F32)
    middle = (own + total).astype(BF16)
    for i in range(nc):
        csend[i] = middle[:, i * LANES : (i + 1) * LANES]

    def send_plane(i, carry):
        tz, ty = lax.rem(z + i // ny, nz), lax.rem(y + i % ny, ny)

        def send(tc):
            pltpu.make_async_remote_copy(
                src_ref=csend.at[tc],
                dst_ref=crecv.at[ep],
                send_sem=csem.at[0],
                recv_sem=csem.at[1],
                device_id=(tz, ty, tc, x),
                device_id_type=MESH,
            ).start()

        for dc in range(1, nc):
            send(lax.rem(c + dc, nc))

        @pl.when(i > 0)
        def _():
            send(c)

        return carry

    lax.fori_loop(0, chips, send_plane, 0)
    crecv[ep] = csend[c]
    others = crecv.at[pl.ds(0, chips * nc - 1)]
    plane = pltpu.make_async_remote_copy(
        src_ref=others,
        dst_ref=others,
        send_sem=csem.at[0],
        recv_sem=csem.at[1],
        device_id=(z, y, lax.rem(c + 1, nc), x),
        device_id_type=MESH,
    )
    plane.wait_recv()
    everyone = crecv[...].astype(F32).reshape(token_count, LANES).astype(BF16)
    slots = dot(place[...], everyone).astype(BF16)
    for i in range(nc):
        esend[i] = slots[i * CAP : (i + 1) * CAP]

    def chip_row(send, recv, sem, src_of, dst):
        copies = []
        for dx in range(nx):
            for dc in range(nc):
                if dx == 0 and dc == 0:
                    continue
                tx, tc = lax.rem(x + dx, nx), lax.rem(c + dc, nc)
                n = dx * nc + dc - 1
                copy = pltpu.make_async_remote_copy(
                    src_ref=send.at[src_of(tx, tc)],
                    dst_ref=recv.at[dst],
                    send_sem=sem.at[0, n],
                    recv_sem=sem.at[1, n],
                    device_id=(z, y, tc, tx),
                    device_id_type=MESH,
                )
                copy.start()
                copies.append(copy)
        return copies

    to_experts = chip_row(esend, erecv, esem, lambda tx, tc: tc, group)
    erecv[group] = esend[c]
    for i in (14, 17, 18, 19):
        loads[i].wait()
    for copy in to_experts:
        copy.wait_recv()
    stacked = jnp.concatenate([erecv[i] for i in range(groups)], axis=1).astype(F32)
    mean = jnp.mean(stacked * stacked, axis=1, keepdims=True)
    routed = (stacked * lax.rsqrt(mean + EPS) * fg[...]).astype(BF16)
    gate_v = dot(routed, wgate[...])
    up_v = dot(routed, wup[...])
    act = (gate_v * jax.nn.sigmoid(gate_v) * up_v).astype(BF16)
    down = dot(act, wdown[...]).astype(BF16)
    for i in range(groups):
        rsend[i] = down[:, i * LANES : (i + 1) * LANES]

    to_groups = chip_row(rsend, rrecv, rsem, lambda tx, tc: tx * nc + tc, group)
    rrecv[group] = rsend[group]
    stage[slots_here:, :] = jnp.zeros((LANES - slots_here, LANES), F32)
    here = nc * rows
    spot = pl.multiple_of(slots_here + lax.rem(zy, 4) * here, here)
    stage[pl.ds(spot, here), :] = crecv[pl.ds(zy * nc, nc)].astype(F32).reshape(here, LANES)
    for copy in to_groups:
        copy.wait_recv()
    for i in range(nc):
        result = rrecv[i].astype(F32)
        for j in range(1, nx):
            result = result + rrecv[j * nc + i].astype(F32)
        stage[i * CAP : (i + 1) * CAP, :] = result
    dsend[...] = stage[...].T.reshape(owners, owned, LANES).astype(BF16)

    count = owners * nx

    def send_owner(i, carry):
        n = lax.rem(i + zy, count)
        k, tx = n // nx, n % nx
        target = group * owners + k
        tc = target % nc
        tzy = target // nc

        @pl.when(jnp.logical_not(jnp.logical_and(target == ep, tx == x)))
        def _():
            pltpu.make_async_remote_copy(
                src_ref=dsend.at[k],
                dst_ref=frecv.at[zy],
                send_sem=dsem.at[0],
                recv_sem=dsem.at[1],
                device_id=(tzy // ny, tzy % ny, tc, tx),
                device_id_type=MESH,
            ).start()

        return carry

    lax.fori_loop(0, count, send_owner, 0)

    def arrivals(n):
        part = frecv.at[pl.ds(0, n)]
        return pltpu.make_async_remote_copy(
            src_ref=part,
            dst_ref=part,
            send_sem=dsem.at[0],
            recv_sem=dsem.at[1],
            device_id=(z, y, lax.rem(c + 1, nc), x),
            device_id_type=MESH,
        )

    loads[16].wait()

    @pl.when(from_self)
    def _():
        frecv[zy] = dsend[lax.rem(ep, owners)]
        arrivals(chips - 1).wait_recv()

    @pl.when(jnp.logical_not(from_self))
    def _():
        arrivals(chips).wait_recv()

    vregs = token_count // LANES
    lane = lax.broadcasted_iota(jnp.int32, (owned, LANES), 1)
    low = lane < slots_here
    names = []
    for j in range(2):
        for k in range(vregs):
            t = jnp.broadcast_to(tgt[j : j + 1, k * LANES : (k + 1) * LANES], (owned, LANES))
            names.append((jnp.bitwise_and(t, LANES - 1), lax.shift_right_logical(t, 7)))

    def pick(p, found):
        second = pltpu.roll(frecv[2 * p + 1].astype(F32), slots_here, 1)
        held = jnp.where(low, frecv[2 * p].astype(F32), second)
        return tuple(
            jnp.where(
                part == p,
                jnp.take_along_axis(held, index, axis=1, mode="promise_in_bounds"),
                f,
            )
            for f, (index, part) in zip(found, names)
        )

    nothing = jnp.zeros((owned, LANES), F32)
    found = lax.fori_loop(0, chips // 2, pick, (nothing,) * (2 * vregs))
    for k in range(vregs):
        halves = []
        for h in range(2):
            half = frecv[8 * k + 4 * h].astype(F32)
            for m in range(1, 4):
                half = half + frecv[8 * k + 4 * h + m].astype(F32)
            halves.append(half)
        mid = jnp.where(low, pltpu.roll(halves[0], slots_here, 1), halves[1])
        w0 = rw[0:1, k * LANES : (k + 1) * LANES]
        w1 = rw[1:2, k * LANES : (k + 1) * LANES]
        both = w0 + w1
        mixed = mid + (found[k] * (w0 / both) + found[vregs + k] * (w1 / both))
        mixed_ref[:, k * LANES : (k + 1) * LANES] = mixed.astype(BF16)

    for dx in range(1, nx):
        pltpu.make_async_remote_copy(
            src_ref=psend.at[0],
            dst_ref=precv.at[dx - 1],
            send_sem=psem.at[0, dx - 1],
            recv_sem=psem.at[1, dx - 1],
            device_id=(z, y, c, lax.rem(x + dx, nx)),
            device_id_type=MESH,
        ).wait_send()
    plane.wait_send()
    for copy in to_experts + to_groups:
        copy.wait_send()

    @pl.when(from_self)
    def _():
        arrivals(count - 1).wait_send()

    @pl.when(jnp.logical_not(from_self))
    def _():
        arrivals(count).wait_send()


def shards(
    sizes,
    tokens,
    mix_gain,
    w_query,
    w_key,
    w_value,
    w_ogate,
    w_igate,
    w_fgate,
    forget_bias,
    head_gain,
    w_out,
    memory,
    normalizer,
    running_max,
    ffn_gain,
    route,
    route_weight,
    w_gate,
    w_up,
    w_down,
):
    nz, ny, nc, nx = sizes
    rows, width = tokens.shape
    qk, dv = memory.shape[2:]
    chips = nz * ny
    quarter = width // nx
    groups = nx * nc
    owned = width // (chips * nc)
    owners = LANES // owned
    token_count = route.shape[0]
    operands = (
        tokens,
        mix_gain.reshape(1, -1),
        w_query,
        w_key,
        w_value,
        w_ogate,
        w_igate.T,
        w_fgate.T,
        forget_bias.reshape(1, -1),
        head_gain.reshape(1, -1),
        w_out,
        memory.reshape(rows, qk, dv),
        normalizer.reshape(rows, qk),
        running_max.T,
        ffn_gain.reshape(1, -1),
        route.T,
        route_weight.T,
        w_gate[0],
        w_up[0],
        w_down[0],
    )
    shape = jax.ShapeDtypeStruct
    vmem = pl.BlockSpec(memory_space=pltpu.VMEM)
    mixed, keep, akey, value, new_norm, new_max = pl.pallas_call(
        functools.partial(kernel, sizes),
        out_shape=(
            shape((owned, token_count), BF16),
            shape((rows, LANES), F32),
            shape((rows, qk), F32),
            shape((rows, dv), F32),
            shape((rows, qk), F32),
            shape((1, rows), F32),
        ),
        in_specs=[pl.BlockSpec(memory_space=pl.ANY)] * len(operands),
        out_specs=(vmem,) * 6,
        scratch_shapes=[pltpu.VMEM(a.shape, a.dtype) for a in operands]
        + [
            pltpu.SemaphoreType.DMA((len(operands),)),
            pltpu.VMEM((2, token_count), jnp.int32),
            pltpu.VMEM((nc * CAP, token_count), BF16),
            pltpu.VMEM((nx, rows, quarter), BF16),
            pltpu.VMEM((nx - 1, rows, quarter), BF16),
            pltpu.VMEM((nc, rows, LANES), BF16),
            pltpu.VMEM((chips * nc, rows, LANES), BF16),
            pltpu.VMEM((nc, CAP, LANES), BF16),
            pltpu.VMEM((groups, CAP, LANES), BF16),
            pltpu.VMEM((groups, CAP, LANES), BF16),
            pltpu.VMEM((groups, CAP, LANES), BF16),
            pltpu.VMEM((LANES, LANES), F32),
            pltpu.VMEM((owners, owned, LANES), BF16),
            pltpu.VMEM((max(chips, owners * nx), owned, LANES), BF16),
            pltpu.SemaphoreType.DMA((2, nx - 1)),
            pltpu.SemaphoreType.DMA((2,)),
            pltpu.SemaphoreType.DMA((2, groups - 1)),
            pltpu.SemaphoreType.DMA((2, groups - 1)),
            pltpu.SemaphoreType.DMA((2,)),
        ],
        compiler_params=pltpu.CompilerParams(collective_id=0, has_side_effects=True),
    )(*operands)
    state = keep[:, :1, None] * memory[:, 0] + akey[:, :, None] * value[:, None, :]
    return (mixed.T, state[:, None], new_norm[:, None], new_max.T)


def solution(mesh):
    nx = mesh.shape["tp"]
    nc = 2
    nz = mesh.shape["ep"] // nc
    ny = 1
    while ny * ny < nz:
        ny *= 2
    nz //= ny
    finer = Mesh(mesh.devices.reshape(nz, ny, nc, nx), ("z", "y", "c", "x"))
    ep = ("z", "y", "c")
    in_specs = (
        P(ep, None),
        P(),
        P(None, "x"),
        P(None, "x"),
        P(None, "x"),
        P(None, "x"),
        P(),
        P(),
        P(),
        P("x"),
        P("x", None),
        P(ep, "x", None, None),
        P(ep, "x", None),
        P(ep, "x"),
        P(),
        P(),
        P(),
        P(ep, None, "x"),
        P(ep, None, "x"),
        P(ep, "x", None),
    )
    out_specs = (P(None, ep), P(ep, "x", None, None), P(ep, "x", None), P(ep, "x"))
    return jax.shard_map(
        functools.partial(shards, (nz, ny, nc, nx)),
        mesh=finer,
        in_specs=in_specs,
        out_specs=out_specs,
        check_vma=False,
    )
```

```python
import functools

import jax
import jax.numpy as jnp
from jax import lax
from jax.experimental import pallas as pl
from jax.experimental.pallas import tpu as pltpu
from jax.sharding import Mesh
from jax.sharding import PartitionSpec as P

MESH = pl.DeviceIdType.MESH
CAP = 32
LANES = 128
EPS = 1e-06
F32 = jnp.float32
BF16 = jnp.bfloat16


def dot(a, b):
    return jnp.dot(a, b, preferred_element_type=F32)


def kernel(
    sizes,
    tok_h,
    mix_h,
    wq_h,
    wk_h,
    wv_h,
    wo_h,
    wi_h,
    wf_h,
    fb_h,
    hg_h,
    wout_h,
    mem_h,
    nrm_h,
    rmax_h,
    fg_h,
    route_h,
    wgate_h,
    wup_h,
    wdown_h,
    frecv,
    mrecv,
    tgt_ref,
    pack_ref,
    tok,
    mix,
    wq,
    wk,
    wv,
    wo,
    wi,
    wf,
    fb,
    hg,
    wout,
    mem,
    nrm,
    rmax,
    fg,
    route,
    wgate,
    wup,
    wdown,
    load_sem,
    tgt,
    pack,
    place,
    psend,
    precv,
    csend,
    crecv,
    esend,
    erecv,
    rsend,
    rrecv,
    msend,
    dsend,
    psem,
    csem,
    esem,
    rsem,
    msem,
    dsem,
    out_sem,
):
    nz, ny, nc, nx = sizes
    z, y, c, x = (lax.axis_index(a) for a in ("z", "y", "c", "x"))
    zy = z * ny + y
    ep = zy * nc + c
    rows, width = tok.shape
    groups = nx * nc
    quarter = width // nx
    chips = nz * ny
    owned = width // (chips * nc)
    owners = LANES // owned
    group = x * nc + c
    expert_count = chips * nc
    token_count = route.shape[1]

    barrier = pltpu.get_barrier_semaphore()

    def greet(target):
        pl.semaphore_signal(barrier, inc=1, device_id=target, device_id_type=MESH)

    y_order = sorted(range(ny), key=lambda d: -min(d, ny - d))

    def ring_z(i):
        shift = nz // 2 + jnp.where(i % 2 == 0, i // 2, -((i + 1) // 2))
        return lax.rem(z + shift, nz)

    def greet_plane(i, carry):
        tz = ring_z(i)
        for dy in y_order:
            ty = lax.rem(y + dy, ny)
            for dc in reversed(range(nc)):
                tc = lax.rem(c + dc, nc)
                if dy == 0 and dc == 0:

                    @pl.when(i < nz - 1)
                    def _():
                        greet((tz, ty, tc, x))
                else:
                    greet((tz, ty, tc, x))
        return carry

    lax.fori_loop(0, nz, greet_plane, 0)
    for dx in range(1, nx):
        for dc in range(nc):
            greet((z, y, lax.rem(c + dc, nc), lax.rem(x + dx, nx)))
    source_group = ep // owners
    source_x, source_c = source_group // nc, source_group % nc
    from_self = source_group == group

    hbm = (tok_h, mix_h, wq_h, wk_h, wv_h, wo_h, wi_h, wf_h, fb_h, hg_h, wout_h, mem_h, nrm_h, rmax_h)
    hbm += (fg_h, route_h, wgate_h, wup_h, wdown_h)
    vmem = (tok, mix, wq, wk, wv, wo, wi, wf, fb, hg, wout, mem, nrm, rmax)
    vmem += (fg, route, wgate, wup, wdown)
    loads = [pltpu.make_async_copy(h, v, load_sem.at[i]) for i, (h, v) in enumerate(zip(hbm, vmem))]
    for load in loads:
        load.start()

    for i in range(14):
        loads[i].wait()
    tokens = tok[...].astype(F32)
    mean = jnp.mean(tokens * tokens, axis=1, keepdims=True)
    normed = (tokens * lax.rsqrt(mean + EPS) * mix[...]).astype(BF16)
    query16 = dot(normed, wq[...]).astype(BF16)
    query = query16.astype(F32)
    scaled_key = dot(normed, wk[...]).astype(BF16).astype(F32) * wq.shape[1] ** (-0.5)
    value = dot(normed, wv[...]).astype(BF16).astype(F32)
    ogate = dot(normed, wo[...]).astype(BF16).astype(F32)
    floats = normed.astype(F32)
    head_row = lax.broadcasted_iota(jnp.int32, wi.shape, 0) == x
    in_row = jnp.sum(jnp.where(head_row, wi[...].astype(F32), 0.0), axis=0, keepdims=True)
    forget_row = jnp.sum(jnp.where(head_row, wf[...].astype(F32), 0.0), axis=0, keepdims=True)
    log_in = jnp.sum(floats * in_row, axis=1, keepdims=True)
    head_lane = lax.broadcasted_iota(jnp.int32, fb.shape, 1) == x
    bias = jnp.sum(jnp.where(head_lane, fb[...], 0.0), axis=1, keepdims=True)
    forget_pre = jnp.sum(floats * forget_row, axis=1, keepdims=True) + bias
    log_forget = jnp.minimum(forget_pre, 0.0) - jnp.log1p(jnp.exp(-jnp.abs(forget_pre)))
    diagonal = lax.broadcasted_iota(jnp.int32, (rows, rows), 0) == lax.broadcasted_iota(
        jnp.int32, (rows, rows), 1
    )
    old_max = jnp.sum(
        jnp.where(diagonal, jnp.broadcast_to(rmax[...], (rows, rows)), 0.0), axis=1, keepdims=True
    )
    carried = log_forget + old_max
    new_max = jnp.maximum(carried, log_in)
    keep = jnp.exp(carried - new_max)
    admit = jnp.exp(log_in - new_max)
    akey = admit * scaled_key
    norm_state = keep * nrm[...] + akey
    qk = wq.shape[1]
    dv = wv.shape[1]
    pack[:, 0:LANES] = jnp.broadcast_to(keep, (rows, LANES))
    pack[:, LANES : LANES + qk] = akey
    pack[:, LANES + qk : LANES + qk + dv] = value
    pack[:, LANES + qk + dv : LANES + 2 * qk + dv] = norm_state
    pack[:, LANES + 2 * qk + dv :] = jnp.broadcast_to(new_max, (rows, LANES))
    row_of = lax.broadcasted_iota(jnp.int32, value.shape, 0)
    kept = jnp.zeros_like(value)
    for t in range(rows):
        kept = jnp.where(row_of == t, dot(query16, mem[t].astype(BF16)), kept)
    numer = keep * kept + jnp.sum(query * akey, axis=1, keepdims=True) * value
    denom = jnp.sum(query * norm_state, axis=1, keepdims=True)
    read = numer / jnp.maximum(jnp.abs(denom), jnp.exp(-new_max))
    scale = lax.rsqrt(jnp.mean(read * read, axis=1, keepdims=True) + EPS)
    gated = (jax.nn.sigmoid(ogate) * read * scale * hg[...]).astype(BF16)
    partial = dot(gated, wout[...]).astype(BF16)
    for i in range(nx):
        psend[i] = partial[:, i * quarter : (i + 1) * quarter]

    loads[15].wait()
    expert_of = lax.broadcasted_iota(jnp.int32, (expert_count, token_count), 0)
    named = [expert_of == route[j : j + 1, :] for j in range(2)]
    either = jnp.where(jnp.logical_or(named[0], named[1]), 1.0, 0.0)
    block = min(256, token_count)
    earlier = (
        lax.broadcasted_iota(jnp.int32, (block, block), 0)
        < lax.broadcasted_iota(jnp.int32, (block, block), 1)
    ).astype(F32).astype(BF16)
    carry = jnp.zeros((expert_count, 1), F32)
    before = []
    for b in range(token_count // block):
        part = either[:, b * block : (b + 1) * block]
        before.append(dot(part.astype(BF16), earlier) + carry)
        carry = carry + jnp.sum(part, axis=1, keepdims=True)
    before = jnp.concatenate(before, axis=1)
    for j in range(2):
        slot = jnp.sum(jnp.where(named[j], before, 0.0), axis=0, keepdims=True)
        tgt[j : j + 1, :] = route[j : j + 1, :] * CAP + slot.astype(jnp.int32)
    slots_here = nc * CAP
    slot_id = lax.broadcasted_iota(jnp.int32, (slots_here, token_count), 0) + zy * slots_here
    hit = jnp.logical_or(slot_id == tgt[0:1, :], slot_id == tgt[1:2, :])
    place[...] = jnp.where(hit, 1.0, 0.0).astype(BF16)
    keeps = [
        pltpu.make_async_copy(tgt, tgt_ref, out_sem.at[0]),
        pltpu.make_async_copy(pack, pack_ref, out_sem.at[1]),
    ]
    for copy in keeps:
        copy.start()

    pl.semaphore_wait(barrier, chips * nc - 1 + (nx - 1) * nc)

    for dx in range(1, nx):
        tx = lax.rem(x + dx, nx)
        pltpu.make_async_remote_copy(
            src_ref=psend.at[tx],
            dst_ref=precv.at[dx - 1],
            send_sem=psem.at[0, dx - 1],
            recv_sem=psem.at[1, dx - 1],
            device_id=(z, y, c, tx),
            device_id_type=MESH,
        ).start()
    total = psend[x].astype(F32)
    for dx in range(1, nx):
        copy = pltpu.make_async_remote_copy(
            src_ref=psend.at[0],
            dst_ref=precv.at[dx - 1],
            send_sem=psem.at[0, dx - 1],
            recv_sem=psem.at[1, dx - 1],
            device_id=(z, y, c, lax.rem(x + dx, nx)),
            device_id_type=MESH,
        )
        copy.wait_recv()
        total = total + precv[dx - 1].astype(F32)
    own = tok[:, pl.ds(pl.multiple_of(x * quarter, quarter), quarter)].astype(F32)
    middle = (own + total).astype(BF16)
    for i in range(nc):
        csend[i] = middle[:, i * LANES : (i + 1) * LANES]

    def send_plane(i, carry):
        tz = ring_z(i)

        def send(ty, tc):
            pltpu.make_async_remote_copy(
                src_ref=csend.at[tc],
                dst_ref=crecv.at[ep],
                send_sem=csem.at[0],
                recv_sem=csem.at[1],
                device_id=(tz, ty, tc, x),
                device_id_type=MESH,
            ).start()

        for dy in y_order:
            ty = lax.rem(y + dy, ny)
            for dc in reversed(range(nc)):
                tc = lax.rem(c + dc, nc)
                if dy == 0 and dc == 0:

                    @pl.when(i < nz - 1)
                    def _():
                        send(ty, tc)
                else:
                    send(ty, tc)
        return carry

    lax.fori_loop(0, nz, send_plane, 0)
    crecv[ep] = csend[c]
    others = crecv.at[pl.ds(0, chips * nc - 1)]
    plane = pltpu.make_async_remote_copy(
        src_ref=others,
        dst_ref=others,
        send_sem=csem.at[0],
        recv_sem=csem.at[1],
        device_id=(z, y, lax.rem(c + 1, nc), x),
        device_id_type=MESH,
    )
    plane.wait_recv()
    everyone32 = crecv[...].astype(F32).reshape(token_count, LANES)
    slots = dot(place[...], everyone32.astype(BF16)).astype(BF16)
    for i in range(nc):
        esend[i] = slots[i * CAP : (i + 1) * CAP]

    def chip_row(send, recv, sem, src_of, dst):
        copies = []
        for dx in range(nx):
            for dc in range(nc):
                if dx == 0 and dc == 0:
                    continue
                tx, tc = lax.rem(x + dx, nx), lax.rem(c + dc, nc)
                n = dx * nc + dc - 1
                copy = pltpu.make_async_remote_copy(
                    src_ref=send.at[src_of(tx, tc)],
                    dst_ref=recv.at[dst],
                    send_sem=sem.at[0, n],
                    recv_sem=sem.at[1, n],
                    device_id=(z, y, tc, tx),
                    device_id_type=MESH,
                )
                copy.start()
                copies.append(copy)
        return copies

    to_experts = chip_row(esend, erecv, esem, lambda tx, tc: tc, group)
    erecv[group] = esend[c]

    @pl.when(from_self)
    def _():
        turned = everyone32.T
        for k in range(owners):
            msend[k] = turned[k * owned : (k + 1) * owned, :].astype(BF16)
        pltpu.make_async_copy(msend.at[lax.rem(ep, owners)], mrecv, out_sem.at[2]).start()

    for i in (14, 16, 17, 18):
        loads[i].wait()
    for copy in to_experts:
        copy.wait_recv()
    stacked = jnp.concatenate([erecv[i] for i in range(groups)], axis=1).astype(F32)
    mean = jnp.mean(stacked * stacked, axis=1, keepdims=True)
    routed = (stacked * lax.rsqrt(mean + EPS) * fg[...]).astype(BF16)
    gate_v = dot(routed, wgate[...])
    up_v = dot(routed, wup[...])
    act = (gate_v * jax.nn.sigmoid(gate_v) * up_v).astype(BF16)
    down = dot(act, wdown[...]).astype(BF16)
    for i in range(groups):
        rsend[i] = down[:, i * LANES : (i + 1) * LANES]

    to_groups = chip_row(rsend, rrecv, rsem, lambda tx, tc: tx * nc + tc, group)
    rrecv[group] = rsend[group]

    middle_copies = []
    for dx in range(nx):
        for dc in range(nc):
            if dx + dc > 0:
                tx, tc = lax.rem(x + dx, nx), lax.rem(c + dc, nc)
                copy = pltpu.make_async_remote_copy(
                    src_ref=msend.at[lax.rem(y * nc + tc, owners)],
                    dst_ref=mrecv,
                    send_sem=msem.at[0],
                    recv_sem=msem.at[1],
                    device_id=(z, y, tc, tx),
                    device_id_type=MESH,
                )
                middle_copies.append(copy)

    @pl.when(from_self)
    def _():
        for copy in middle_copies:
            copy.start()

    for copy in to_groups:
        copy.wait_recv()
    results = []
    for i in range(nc):
        result = rrecv[i].astype(F32)
        for j in range(1, nx):
            result = result + rrecv[j * nc + i].astype(F32)
        results.append(result)
    low = lax.broadcasted_iota(jnp.int32, (owners, owned // 2, LANES), 2) < slots_here
    turned = jnp.concatenate(results + results, axis=0).T.reshape(owners, owned, LANES)
    half = owned // 2
    dsend[...] = jnp.where(low, turned[:, :half], turned[:, half:]).astype(BF16)

    def send_owners(i, carry):
        shift = ny // 2 + jnp.where(i % 2 == 0, i // 2, -((i + 1) // 2))
        ty = lax.rem(y + shift, ny)

        def send(tc, tx):
            pltpu.make_async_remote_copy(
                src_ref=dsend.at[ty * nc + tc],
                dst_ref=frecv.at[zy],
                send_sem=dsem.at[0],
                recv_sem=dsem.at[1],
                device_id=(group, ty, tc, tx),
                device_id_type=MESH,
            ).start()

        for dx in sorted(range(nx), key=lambda d: -min(d, nx - d)):
            tx = lax.rem(x + dx, nx)
            for dc in reversed(range(nc)):
                tc = lax.rem(c + dc, nc)
                if dx == 0 and dc == 0:

                    @pl.when(jnp.logical_not(jnp.logical_and(from_self, i == ny - 1)))
                    def _():
                        send(tc, tx)
                else:
                    send(tc, tx)
        return carry

    lax.fori_loop(0, ny, send_owners, 0)

    def arrivals(n):
        part = frecv.at[pl.ds(0, n)]
        return pltpu.make_async_remote_copy(
            src_ref=part,
            dst_ref=part,
            send_sem=dsem.at[0],
            recv_sem=dsem.at[1],
            device_id=(z, y, lax.rem(c + 1, nc), x),
            device_id_type=MESH,
        )

    @pl.when(from_self)
    def _():
        own = pltpu.make_async_copy(dsend.at[lax.rem(ep, owners)], frecv.at[zy], out_sem.at[3])
        own.start()
        arrivals(chips - 1).wait_recv()
        own.wait()
        pltpu.make_async_copy(msend.at[lax.rem(ep, owners)], mrecv, out_sem.at[2]).wait()

    @pl.when(jnp.logical_not(from_self))
    def _():
        middle_copies[0].wait_recv()
        arrivals(chips).wait_recv()

    for copy in keeps:
        copy.wait()

    for dx in range(1, nx):
        pltpu.make_async_remote_copy(
            src_ref=psend.at[0],
            dst_ref=precv.at[dx - 1],
            send_sem=psem.at[0, dx - 1],
            recv_sem=psem.at[1, dx - 1],
            device_id=(z, y, c, lax.rem(x + dx, nx)),
            device_id_type=MESH,
        ).wait_send()
    plane.wait_send()
    for copy in to_experts + to_groups:
        copy.wait_send()

    @pl.when(from_self)
    def _():
        for copy in middle_copies:
            copy.wait_send()
        arrivals(chips - 1).wait_send()

    @pl.when(jnp.logical_not(from_self))
    def _():
        arrivals(chips).wait_send()


def combine(
    parts_h,
    mid_h,
    tgt_h,
    rw_h,
    pack_h,
    mem_h,
    mixed_ref,
    newmem_ref,
    newnorm_ref,
    newmax_ref,
    parts,
    mid,
    tgt,
    rw,
    pack,
    mem,
    state,
    load_sem,
    mem_sem,
    sem,
):
    rows, qk, dv = mem.shape
    chips, half, _ = parts.shape
    owned = 2 * half
    token_count = tgt.shape[1]
    loads = []
    for i, (h, v) in enumerate(
        ((pack_h, pack), (tgt_h, tgt), (parts_h, parts), (mid_h, mid), (rw_h, rw))
    ):
        loads.append(pltpu.make_async_copy(h, v, load_sem.at[i]))
    mem_loads = [pltpu.make_async_copy(mem_h.at[t], mem.at[t], mem_sem.at[t]) for t in range(rows)]
    for copy in loads + mem_loads:
        copy.start()
    loads[0].wait()
    copies = []
    value = pack[:, LANES + qk : LANES + qk + dv]
    for t in range(rows):
        key_columns = jnp.broadcast_to(pack[t : t + 1, LANES : LANES + qk], (LANES, LANES)).T
        key_columns = jnp.concatenate([key_columns] * (dv // LANES), axis=1)
        mem_loads[t].wait()
        state[t] = pack[t : t + 1, 0:1] * mem[t] + key_columns * value[t : t + 1, :]
        copy = pltpu.make_async_copy(state.at[t], newmem_ref.at[t], sem.at[t])
        copy.start()
        copies.append(copy)
    newnorm_ref[...] = pack[:, LANES + qk + dv : LANES + 2 * qk + dv]
    diagonal = lax.broadcasted_iota(jnp.int32, (rows, LANES), 0) == lax.broadcasted_iota(
        jnp.int32, (rows, LANES), 1
    )
    row = jnp.where(diagonal, pack[:, LANES + 2 * qk + dv :], 0.0)
    newmax_ref[...] = jnp.sum(row, axis=0, keepdims=True)[:, :rows]
    for copy in loads[1:]:
        copy.wait()

    low = lax.broadcasted_iota(jnp.int32, (chips // 2, half, LANES), 2) < LANES // 2
    both = parts[...].astype(F32).reshape(chips // 2, 2, half, LANES)
    even, odd = both[:, 0], both[:, 1]
    even_turned = pltpu.roll(even, LANES // 2, 2)
    odd_turned = pltpu.roll(odd, LANES // 2, 2)
    held = jnp.concatenate(
        [jnp.where(low, even, odd_turned), jnp.where(low, even_turned, odd)], axis=1
    )
    held = held.reshape(chips // 2 * owned, LANES).astype(BF16)
    lane_id = lax.broadcasted_iota(jnp.int32, (LANES, LANES), 0)
    for k in range(token_count // LANES):
        span = slice(k * LANES, (k + 1) * LANES)
        names = [tgt[j : j + 1, span] for j in range(2)]
        picks = jnp.concatenate(
            [
                jnp.where(lane_id == jnp.bitwise_and(n, LANES - 1), 1.0, 0.0).astype(BF16)
                for n in names
            ],
            axis=1,
        )
        found = dot(held, picks)
        total = []
        for j in range(2):
            place = jnp.broadcast_to(lax.shift_right_logical(names[j], 7), (owned, LANES))
            got = jnp.zeros((owned, LANES), F32)
            for p in range(chips // 2):
                part = found[p * owned : (p + 1) * owned, j * LANES : (j + 1) * LANES]
                got = jnp.where(place == p, part, got)
            total.append(got)
        w0, w1 = rw[0:1, span], rw[1:2, span]
        weighed = total[0] * (w0 / (w0 + w1)) + total[1] * (w1 / (w0 + w1))
        mixed_ref[:, span] = (mid[:, span].astype(F32) + weighed).astype(BF16)
    for copy in copies:
        copy.wait()


def shards(
    sizes,
    tokens,
    mix_gain,
    w_query,
    w_key,
    w_value,
    w_ogate,
    w_igate,
    w_fgate,
    forget_bias,
    head_gain,
    w_out,
    memory,
    normalizer,
    running_max,
    ffn_gain,
    route,
    route_weight,
    w_gate,
    w_up,
    w_down,
):
    nz, ny, nc, nx = sizes
    rows, width = tokens.shape
    qk, dv = memory.shape[2:]
    chips = nz * ny
    quarter = width // nx
    groups = nx * nc
    owned = width // (chips * nc)
    owners = LANES // owned
    token_count = route.shape[0]
    operands = (
        tokens,
        mix_gain.reshape(1, -1),
        w_query,
        w_key,
        w_value,
        w_ogate,
        w_igate.T,
        w_fgate.T,
        forget_bias.reshape(1, -1),
        head_gain.reshape(1, -1),
        w_out,
        memory.reshape(rows, qk, dv),
        normalizer.reshape(rows, qk),
        running_max.T,
        ffn_gain.reshape(1, -1),
        route.T,
        w_gate[0],
        w_up[0],
        w_down[0],
    )
    shape = jax.ShapeDtypeStruct
    vmem = pl.BlockSpec(memory_space=pltpu.VMEM)
    hbm = pl.BlockSpec(memory_space=pl.ANY)
    pack_width = LANES * 2 + 2 * qk + dv
    parts, mid, tgt, pack = pl.pallas_call(
        functools.partial(kernel, sizes),
        out_shape=(
            shape((chips, owned // 2, LANES), BF16),
            shape((owned, token_count), BF16),
            shape((2, token_count), jnp.int32),
            shape((rows, pack_width), F32),
        ),
        in_specs=[hbm] * len(operands),
        out_specs=(hbm,) * 4,
        scratch_shapes=[pltpu.VMEM(a.shape, a.dtype) for a in operands]
        + [
            pltpu.SemaphoreType.DMA((len(operands),)),
            pltpu.VMEM((2, token_count), jnp.int32),
            pltpu.VMEM((rows, pack_width), F32),
            pltpu.VMEM((nc * CAP, token_count), BF16),
            pltpu.VMEM((nx, rows, quarter), BF16),
            pltpu.VMEM((nx - 1, rows, quarter), BF16),
            pltpu.VMEM((nc, rows, LANES), BF16),
            pltpu.VMEM((chips * nc, rows, LANES), BF16),
            pltpu.VMEM((nc, CAP, LANES), BF16),
            pltpu.VMEM((groups, CAP, LANES), BF16),
            pltpu.VMEM((groups, CAP, LANES), BF16),
            pltpu.VMEM((groups, CAP, LANES), BF16),
            pltpu.VMEM((owners, owned, token_count), BF16),
            pltpu.VMEM((owners, owned // 2, LANES), BF16),
            pltpu.SemaphoreType.DMA((2, nx - 1)),
            pltpu.SemaphoreType.DMA((2,)),
            pltpu.SemaphoreType.DMA((2, groups - 1)),
            pltpu.SemaphoreType.DMA((2, groups - 1)),
            pltpu.SemaphoreType.DMA((2,)),
            pltpu.SemaphoreType.DMA((2,)),
            pltpu.SemaphoreType.DMA((4,)),
        ],
        compiler_params=pltpu.CompilerParams(collective_id=0, has_side_effects=True),
    )(*operands)
    mixed, state, new_norm, new_max = pl.pallas_call(
        combine,
        out_shape=(
            shape((owned, token_count), BF16),
            shape((rows, qk, dv), F32),
            shape((rows, qk), F32),
            shape((1, rows), F32),
        ),
        in_specs=[hbm] * 6,
        out_specs=(vmem, hbm, vmem, vmem),
        scratch_shapes=[
            pltpu.VMEM((chips, owned // 2, LANES), BF16),
            pltpu.VMEM((owned, token_count), BF16),
            pltpu.VMEM((2, token_count), jnp.int32),
            pltpu.VMEM((2, token_count), F32),
            pltpu.VMEM((rows, pack_width), F32),
            pltpu.VMEM((rows, qk, dv), F32),
            pltpu.VMEM((rows, qk, dv), F32),
            pltpu.SemaphoreType.DMA((5,)),
            pltpu.SemaphoreType.DMA((rows,)),
            pltpu.SemaphoreType.DMA((rows,)),
        ],
    )(parts, mid, tgt, route_weight.T, pack, memory.reshape(rows, qk, dv))
    return (mixed.T, state[:, None], new_norm[:, None], new_max.T)


def solution(mesh):
    nx = mesh.shape["tp"]
    nc = 2
    nz = nx * nc
    ny = mesh.shape["ep"] // (nc * nz)
    finer = Mesh(mesh.devices.reshape(nz, ny, nc, nx), ("z", "y", "c", "x"))
    ep = ("z", "y", "c")
    in_specs = (
        P(ep, None),
        P(),
        P(None, "x"),
        P(None, "x"),
        P(None, "x"),
        P(None, "x"),
        P(),
        P(),
        P(),
        P("x"),
        P("x", None),
        P(ep, "x", None, None),
        P(ep, "x", None),
        P(ep, "x"),
        P(),
        P(),
        P(),
        P(ep, None, "x"),
        P(ep, None, "x"),
        P(ep, "x", None),
    )
    out_specs = (P(None, ep), P(ep, "x", None, None), P(ep, "x", None), P(ep, "x"))
    return jax.shard_map(
        functools.partial(shards, (nz, ny, nc, nx)),
        mesh=finer,
        in_specs=in_specs,
        out_specs=out_specs,
        check_vma=False,
    )
```

```python
import functools

import jax
import jax.numpy as jnp
from jax import lax
from jax.experimental import pallas as pl
from jax.experimental.pallas import tpu as pltpu
from jax.sharding import Mesh
from jax.sharding import PartitionSpec as P

MESH = pl.DeviceIdType.MESH
CAP = 32
LANES = 128
EPS = 1e-06
F32 = jnp.float32
BF16 = jnp.bfloat16


def dot(a, b):
    return jnp.dot(a, b, preferred_element_type=F32)


def kernel(
    sizes,
    tok_h,
    mix_h,
    wq_h,
    wk_h,
    wv_h,
    wo_h,
    wi_h,
    wf_h,
    fb_h,
    hg_h,
    wout_h,
    mem_h,
    nrm_h,
    rmax_h,
    fg_h,
    route_h,
    wgate_h,
    wup_h,
    wdown_h,
    frecv,
    mrecv,
    tgt_ref,
    pack_ref,
    state_ref,
    tok,
    mix,
    wq,
    wk,
    wv,
    wo,
    wi,
    wf,
    fb,
    hg,
    wout,
    mem,
    nrm,
    rmax,
    fg,
    route,
    wgate,
    wup,
    wdown,
    load_sem,
    tgt,
    pack,
    place,
    psend,
    precv,
    csend,
    crecv,
    esend,
    erecv,
    rsend,
    rrecv,
    msend,
    dsend,
    psem,
    csem,
    esem,
    rsem,
    msem,
    dsem,
    out_sem,
    plane_sem,
    state,
):
    nz, ny, nc, nx = sizes
    z, y, c, x = (lax.axis_index(a) for a in ("z", "y", "c", "x"))
    zy = z * ny + y
    ep = zy * nc + c
    rows, width = tok.shape
    groups = nx * nc
    quarter = width // nx
    chips = nz * ny
    owned = width // (chips * nc)
    owners = LANES // owned
    group = x * nc + c
    expert_count = chips * nc
    token_count = route.shape[1]

    barrier = pltpu.get_barrier_semaphore()

    def greet(target):
        pl.semaphore_signal(barrier, inc=1, device_id=target, device_id_type=MESH)

    y_order = sorted(range(ny), key=lambda d: -min(d, ny - d))

    def ring_z(i):
        shift = nz // 2 + jnp.where(i % 2 == 0, i // 2, -((i + 1) // 2))
        return lax.rem(z + shift, nz)

    z_order = sorted(range(1, nz), key=lambda d: -min(d, nz - d))
    for dz in z_order:
        tz = lax.rem(z + dz, nz)
        for dc in range(nc):
            greet((tz, y, lax.rem(c + dc, nc), x))
    for dy in y_order[:-1]:
        greet((z, lax.rem(y + dy, ny), c, x))
    for dx in range(nx):
        for dc in range(nc):
            if dx + dc > 0:
                greet((z, y, lax.rem(c + dc, nc), lax.rem(x + dx, nx)))
    source_group = ep // owners
    source_x, source_c = source_group // nc, source_group % nc
    from_self = source_group == group

    hbm = (tok_h, mix_h, wq_h, wk_h, wv_h, wo_h, wi_h, wf_h, fb_h, hg_h, wout_h, mem_h, nrm_h, rmax_h)
    hbm += (fg_h, route_h, wgate_h, wup_h, wdown_h)
    vmem = (tok, mix, wq, wk, wv, wo, wi, wf, fb, hg, wout, mem, nrm, rmax)
    vmem += (fg, route, wgate, wup, wdown)
    loads = [pltpu.make_async_copy(h, v, load_sem.at[i]) for i, (h, v) in enumerate(zip(hbm, vmem))]
    for load in loads:
        load.start()

    for i in range(14):
        loads[i].wait()
    tokens = tok[...].astype(F32)
    mean = jnp.mean(tokens * tokens, axis=1, keepdims=True)
    normed = (tokens * lax.rsqrt(mean + EPS) * mix[...]).astype(BF16)
    query16 = dot(normed, wq[...]).astype(BF16)
    query = query16.astype(F32)
    scaled_key = dot(normed, wk[...]).astype(BF16).astype(F32) * wq.shape[1] ** (-0.5)
    value = dot(normed, wv[...]).astype(BF16).astype(F32)
    ogate = dot(normed, wo[...]).astype(BF16).astype(F32)
    floats = normed.astype(F32)
    head_row = lax.broadcasted_iota(jnp.int32, wi.shape, 0) == x
    in_row = jnp.sum(jnp.where(head_row, wi[...].astype(F32), 0.0), axis=0, keepdims=True)
    forget_row = jnp.sum(jnp.where(head_row, wf[...].astype(F32), 0.0), axis=0, keepdims=True)
    log_in = jnp.sum(floats * in_row, axis=1, keepdims=True)
    head_lane = lax.broadcasted_iota(jnp.int32, fb.shape, 1) == x
    bias = jnp.sum(jnp.where(head_lane, fb[...], 0.0), axis=1, keepdims=True)
    forget_pre = jnp.sum(floats * forget_row, axis=1, keepdims=True) + bias
    log_forget = jnp.minimum(forget_pre, 0.0) - jnp.log1p(jnp.exp(-jnp.abs(forget_pre)))
    diagonal = lax.broadcasted_iota(jnp.int32, (rows, rows), 0) == lax.broadcasted_iota(
        jnp.int32, (rows, rows), 1
    )
    old_max = jnp.sum(
        jnp.where(diagonal, jnp.broadcast_to(rmax[...], (rows, rows)), 0.0), axis=1, keepdims=True
    )
    carried = log_forget + old_max
    new_max = jnp.maximum(carried, log_in)
    keep = jnp.exp(carried - new_max)
    admit = jnp.exp(log_in - new_max)
    akey = admit * scaled_key
    norm_state = keep * nrm[...] + akey
    qk = wq.shape[1]
    pack[:, 0:qk] = norm_state
    pack[:, qk:] = jnp.broadcast_to(new_max, (rows, LANES))
    row_of = lax.broadcasted_iota(jnp.int32, value.shape, 0)
    kept = jnp.zeros_like(value)
    for t in range(rows):
        kept = jnp.where(row_of == t, dot(query16, mem[t].astype(BF16)), kept)
    numer = keep * kept + jnp.sum(query * akey, axis=1, keepdims=True) * value
    denom = jnp.sum(query * norm_state, axis=1, keepdims=True)
    read = numer / jnp.maximum(jnp.abs(denom), jnp.exp(-new_max))
    scale = lax.rsqrt(jnp.mean(read * read, axis=1, keepdims=True) + EPS)
    gated = (jax.nn.sigmoid(ogate) * read * scale * hg[...]).astype(BF16)
    partial = dot(gated, wout[...]).astype(BF16)
    for i in range(nx):
        psend[i] = partial[:, i * quarter : (i + 1) * quarter]
    pl.semaphore_wait(barrier, (nz - 1) * nc + ny - 1 + nx * nc - 1)

    for dy in y_order[:-1]:
        pl.semaphore_signal(
            plane_sem, inc=1, device_id=(z, lax.rem(y + dy, ny), c, x), device_id_type=MESH
        )

    for dx in range(1, nx):
        tx = lax.rem(x + dx, nx)
        pltpu.make_async_remote_copy(
            src_ref=psend.at[tx],
            dst_ref=precv.at[dx - 1],
            send_sem=psem.at[0, dx - 1],
            recv_sem=psem.at[1, dx - 1],
            device_id=(z, y, c, tx),
            device_id_type=MESH,
        ).start()

    loads[15].wait()
    expert_of = lax.broadcasted_iota(jnp.int32, (expert_count, token_count), 0)
    named = [expert_of == route[j : j + 1, :] for j in range(2)]
    either = jnp.where(jnp.logical_or(named[0], named[1]), 1.0, 0.0)
    block = min(256, token_count)
    earlier = (
        lax.broadcasted_iota(jnp.int32, (block, block), 0)
        < lax.broadcasted_iota(jnp.int32, (block, block), 1)
    ).astype(F32).astype(BF16)
    carry = jnp.zeros((expert_count, 1), F32)
    before = []
    for b in range(token_count // block):
        part = either[:, b * block : (b + 1) * block]
        before.append(dot(part.astype(BF16), earlier) + carry)
        carry = carry + jnp.sum(part, axis=1, keepdims=True)
    before = jnp.concatenate(before, axis=1)
    for j in range(2):
        slot = jnp.sum(jnp.where(named[j], before, 0.0), axis=0, keepdims=True)
        tgt[j : j + 1, :] = route[j : j + 1, :] * CAP + slot.astype(jnp.int32)
    slots_here = nc * CAP
    slot_id = lax.broadcasted_iota(jnp.int32, (slots_here, token_count), 0) + zy * slots_here
    hit = jnp.logical_or(slot_id == tgt[0:1, :], slot_id == tgt[1:2, :])
    place[...] = jnp.where(hit, 1.0, 0.0).astype(BF16)
    keeps = [
        pltpu.make_async_copy(tgt, tgt_ref, out_sem.at[0]),
        pltpu.make_async_copy(pack, pack_ref, out_sem.at[1]),
    ]
    for copy in keeps:
        copy.start()

    total = psend[x].astype(F32)
    for dx in range(1, nx):
        copy = pltpu.make_async_remote_copy(
            src_ref=psend.at[0],
            dst_ref=precv.at[dx - 1],
            send_sem=psem.at[0, dx - 1],
            recv_sem=psem.at[1, dx - 1],
            device_id=(z, y, c, lax.rem(x + dx, nx)),
            device_id_type=MESH,
        )
        copy.wait_recv()
        total = total + precv[dx - 1].astype(F32)
    own = tok[:, pl.ds(pl.multiple_of(x * quarter, quarter), quarter)].astype(F32)
    middle = (own + total).astype(BF16)
    for i in range(nc):
        csend[i] = middle[:, i * LANES : (i + 1) * LANES]

    def send_plane(i, carry):
        tz = ring_z(i)

        def send(ty, tc):
            pltpu.make_async_remote_copy(
                src_ref=csend.at[tc],
                dst_ref=crecv.at[ep],
                send_sem=csem.at[0],
                recv_sem=csem.at[1],
                device_id=(tz, ty, tc, x),
                device_id_type=MESH,
            ).start()

        for dy in y_order:
            ty = lax.rem(y + dy, ny)
            for dc in reversed(range(nc)):
                tc = lax.rem(c + dc, nc)
                if dy == 0 and dc == 0:

                    @pl.when(i < nz - 1)
                    def _():
                        send(ty, tc)
                else:
                    send(ty, tc)
        return carry

    pl.semaphore_wait(plane_sem, ny - 1)
    lax.fori_loop(0, nz, send_plane, 0)
    crecv[ep] = csend[c]

    for t in range(rows):
        key_columns = jnp.broadcast_to(akey[t : t + 1, :], (LANES, LANES)).T
        key_columns = jnp.concatenate([key_columns] * (wv.shape[1] // LANES), axis=1)
        state[t] = keep[t : t + 1, :] * mem[t] + key_columns * value[t : t + 1, :]
    keeps.append(pltpu.make_async_copy(state, state_ref, out_sem.at[4]))
    keeps[-1].start()
    others = crecv.at[pl.ds(0, chips * nc - 1)]
    plane = pltpu.make_async_remote_copy(
        src_ref=others,
        dst_ref=others,
        send_sem=csem.at[0],
        recv_sem=csem.at[1],
        device_id=(z, y, lax.rem(c + 1, nc), x),
        device_id_type=MESH,
    )
    plane.wait_recv()
    everyone32 = crecv[...].astype(F32).reshape(token_count, LANES)
    slots = dot(place[...], everyone32.astype(BF16)).astype(BF16)
    for i in range(nc):
        esend[i] = slots[i * CAP : (i + 1) * CAP]

    def chip_row(send, recv, sem, src_of, dst):
        copies = []
        for dx in range(nx):
            for dc in range(nc):
                if dx == 0 and dc == 0:
                    continue
                tx, tc = lax.rem(x + dx, nx), lax.rem(c + dc, nc)
                n = dx * nc + dc - 1
                copy = pltpu.make_async_remote_copy(
                    src_ref=send.at[src_of(tx, tc)],
                    dst_ref=recv.at[dst],
                    send_sem=sem.at[0, n],
                    recv_sem=sem.at[1, n],
                    device_id=(z, y, tc, tx),
                    device_id_type=MESH,
                )
                copy.start()
                copies.append(copy)
        return copies

    to_experts = chip_row(esend, erecv, esem, lambda tx, tc: tc, group)
    erecv[group] = esend[c]

    @pl.when(from_self)
    def _():
        turned = everyone32.T
        for k in range(owners):
            msend[k] = turned[k * owned : (k + 1) * owned, :].astype(BF16)
        pltpu.make_async_copy(msend.at[lax.rem(ep, owners)], mrecv, out_sem.at[2]).start()

    for i in (14, 16, 17, 18):
        loads[i].wait()
    for copy in to_experts:
        copy.wait_recv()
    stacked = jnp.concatenate([erecv[i] for i in range(groups)], axis=1).astype(F32)
    mean = jnp.mean(stacked * stacked, axis=1, keepdims=True)
    routed = (stacked * lax.rsqrt(mean + EPS) * fg[...]).astype(BF16)
    gate_v = dot(routed, wgate[...])
    up_v = dot(routed, wup[...])
    act = (gate_v * jax.nn.sigmoid(gate_v) * up_v).astype(BF16)
    down = dot(act, wdown[...]).astype(BF16)
    for i in range(groups):
        rsend[i] = down[:, i * LANES : (i + 1) * LANES]

    to_groups = chip_row(rsend, rrecv, rsem, lambda tx, tc: tx * nc + tc, group)
    rrecv[group] = rsend[group]

    middle_copies = []
    for dx in range(nx):
        for dc in range(nc):
            if dx + dc > 0:
                tx, tc = lax.rem(x + dx, nx), lax.rem(c + dc, nc)
                copy = pltpu.make_async_remote_copy(
                    src_ref=msend.at[lax.rem(y * nc + tc, owners)],
                    dst_ref=mrecv,
                    send_sem=msem.at[0],
                    recv_sem=msem.at[1],
                    device_id=(z, y, tc, tx),
                    device_id_type=MESH,
                )
                middle_copies.append(copy)

    @pl.when(from_self)
    def _():
        for copy in middle_copies:
            copy.start()

    for copy in to_groups:
        copy.wait_recv()
    results = []
    for i in range(nc):
        result = rrecv[i].astype(F32)
        for j in range(1, nx):
            result = result + rrecv[j * nc + i].astype(F32)
        results.append(result)
    low = lax.broadcasted_iota(jnp.int32, (owners, owned // 2, LANES), 2) < slots_here
    turned = jnp.concatenate(results + results, axis=0).T.reshape(owners, owned, LANES)
    half = owned // 2
    dsend[...] = jnp.where(low, turned[:, :half], turned[:, half:]).astype(BF16)

    def send_owners(i, carry):
        shift = ny // 2 + jnp.where(i % 2 == 0, i // 2, -((i + 1) // 2))
        ty = lax.rem(y + shift, ny)

        def send(tc, tx):
            pltpu.make_async_remote_copy(
                src_ref=dsend.at[ty * nc + tc],
                dst_ref=frecv.at[zy],
                send_sem=dsem.at[0],
                recv_sem=dsem.at[1],
                device_id=(group, ty, tc, tx),
                device_id_type=MESH,
            ).start()

        for dx in sorted(range(nx), key=lambda d: -min(d, nx - d)):
            tx = lax.rem(x + dx, nx)
            for dc in reversed(range(nc)):
                tc = lax.rem(c + dc, nc)
                if dx == 0 and dc == 0:

                    @pl.when(jnp.logical_not(jnp.logical_and(from_self, i == ny - 1)))
                    def _():
                        send(tc, tx)
                else:
                    send(tc, tx)
        return carry

    lax.fori_loop(0, ny, send_owners, 0)

    def arrivals(n):
        part = frecv.at[pl.ds(0, n)]
        return pltpu.make_async_remote_copy(
            src_ref=part,
            dst_ref=part,
            send_sem=dsem.at[0],
            recv_sem=dsem.at[1],
            device_id=(z, y, lax.rem(c + 1, nc), x),
            device_id_type=MESH,
        )

    @pl.when(from_self)
    def _():
        own = pltpu.make_async_copy(dsend.at[lax.rem(ep, owners)], frecv.at[zy], out_sem.at[3])
        own.start()
        arrivals(chips - 1).wait_recv()
        own.wait()
        pltpu.make_async_copy(msend.at[lax.rem(ep, owners)], mrecv, out_sem.at[2]).wait()

    @pl.when(jnp.logical_not(from_self))
    def _():
        middle_copies[0].wait_recv()
        arrivals(chips).wait_recv()

    for copy in keeps:
        copy.wait()

    for dx in range(1, nx):
        pltpu.make_async_remote_copy(
            src_ref=psend.at[0],
            dst_ref=precv.at[dx - 1],
            send_sem=psem.at[0, dx - 1],
            recv_sem=psem.at[1, dx - 1],
            device_id=(z, y, c, lax.rem(x + dx, nx)),
            device_id_type=MESH,
        ).wait_send()
    plane.wait_send()
    for copy in to_experts + to_groups:
        copy.wait_send()

    @pl.when(from_self)
    def _():
        for copy in middle_copies:
            copy.wait_send()
        arrivals(chips - 1).wait_send()

    @pl.when(jnp.logical_not(from_self))
    def _():
        arrivals(chips).wait_send()


def combine(
    parts_h,
    mid_h,
    tgt_h,
    rw_h,
    pack_h,
    state_h,
    mixed_ref,
    newmem_ref,
    newnorm_ref,
    newmax_ref,
    parts,
    mid,
    tgt,
    rw,
    pack,
    state,
    load_sem,
    state_sem,
    sem,
):
    rows, qk, dv = state.shape
    chips, half, _ = parts.shape
    owned = 2 * half
    token_count = tgt.shape[1]
    loads = []
    for i, (h, v) in enumerate(
        ((pack_h, pack), (tgt_h, tgt), (parts_h, parts), (mid_h, mid), (rw_h, rw))
    ):
        loads.append(pltpu.make_async_copy(h, v, load_sem.at[i]))
    moves = [pltpu.make_async_copy(state_h.at[t], state.at[t], state_sem.at[t]) for t in range(rows)]
    for copy in loads + moves:
        copy.start()
    loads[0].wait()
    newnorm_ref[...] = pack[:, 0:qk]
    diagonal = lax.broadcasted_iota(jnp.int32, (rows, LANES), 0) == lax.broadcasted_iota(
        jnp.int32, (rows, LANES), 1
    )
    newmax_ref[...] = jnp.sum(jnp.where(diagonal, pack[:, qk:], 0.0), axis=0, keepdims=True)[:, :rows]
    copies = []
    for t in range(rows):
        moves[t].wait()
        copy = pltpu.make_async_copy(state.at[t], newmem_ref.at[t], sem.at[t])
        copy.start()
        copies.append(copy)
    for copy in loads[1:]:
        copy.wait()

    low = lax.broadcasted_iota(jnp.int32, (chips // 2, half, LANES), 2) < LANES // 2
    both = parts[...].astype(F32).reshape(chips // 2, 2, half, LANES)
    even, odd = both[:, 0], both[:, 1]
    even_turned = pltpu.roll(even, LANES // 2, 2)
    odd_turned = pltpu.roll(odd, LANES // 2, 2)
    held = jnp.concatenate(
        [jnp.where(low, even, odd_turned), jnp.where(low, even_turned, odd)], axis=1
    )
    held = held.reshape(chips // 2 * owned, LANES).astype(BF16)
    lane_id = lax.broadcasted_iota(jnp.int32, (LANES, LANES), 0)
    for k in range(token_count // LANES):
        span = slice(k * LANES, (k + 1) * LANES)
        names = [tgt[j : j + 1, span] for j in range(2)]
        picks = jnp.concatenate(
            [
                jnp.where(lane_id == jnp.bitwise_and(n, LANES - 1), 1.0, 0.0).astype(BF16)
                for n in names
            ],
            axis=1,
        )
        found = dot(held, picks)
        total = []
        for j in range(2):
            place = jnp.broadcast_to(lax.shift_right_logical(names[j], 7), (owned, LANES))
            got = jnp.zeros((owned, LANES), F32)
            for p in range(chips // 2):
                part = found[p * owned : (p + 1) * owned, j * LANES : (j + 1) * LANES]
                got = jnp.where(place == p, part, got)
            total.append(got)
        w0, w1 = rw[0:1, span], rw[1:2, span]
        weighed = total[0] * (w0 / (w0 + w1)) + total[1] * (w1 / (w0 + w1))
        mixed_ref[:, span] = (mid[:, span].astype(F32) + weighed).astype(BF16)
    for copy in copies:
        copy.wait()


def shards(
    sizes,
    tokens,
    mix_gain,
    w_query,
    w_key,
    w_value,
    w_ogate,
    w_igate,
    w_fgate,
    forget_bias,
    head_gain,
    w_out,
    memory,
    normalizer,
    running_max,
    ffn_gain,
    route,
    route_weight,
    w_gate,
    w_up,
    w_down,
):
    nz, ny, nc, nx = sizes
    rows, width = tokens.shape
    qk, dv = memory.shape[2:]
    chips = nz * ny
    quarter = width // nx
    groups = nx * nc
    owned = width // (chips * nc)
    owners = LANES // owned
    token_count = route.shape[0]
    operands = (
        tokens,
        mix_gain.reshape(1, -1),
        w_query,
        w_key,
        w_value,
        w_ogate,
        w_igate.T,
        w_fgate.T,
        forget_bias.reshape(1, -1),
        head_gain.reshape(1, -1),
        w_out,
        memory.reshape(rows, qk, dv),
        normalizer.reshape(rows, qk),
        running_max.T,
        ffn_gain.reshape(1, -1),
        route.T,
        w_gate[0],
        w_up[0],
        w_down[0],
    )
    shape = jax.ShapeDtypeStruct
    vmem = pl.BlockSpec(memory_space=pltpu.VMEM)
    hbm = pl.BlockSpec(memory_space=pl.ANY)
    pack_width = LANES + qk
    parts, mid, tgt, pack, state = pl.pallas_call(
        functools.partial(kernel, sizes),
        out_shape=(
            shape((chips, owned // 2, LANES), BF16),
            shape((owned, token_count), BF16),
            shape((2, token_count), jnp.int32),
            shape((rows, pack_width), F32),
            shape((rows, qk, dv), F32),
        ),
        in_specs=[hbm] * len(operands),
        out_specs=(hbm,) * 5,
        scratch_shapes=[pltpu.VMEM(a.shape, a.dtype) for a in operands]
        + [
            pltpu.SemaphoreType.DMA((len(operands),)),
            pltpu.VMEM((2, token_count), jnp.int32),
            pltpu.VMEM((rows, pack_width), F32),
            pltpu.VMEM((nc * CAP, token_count), BF16),
            pltpu.VMEM((nx, rows, quarter), BF16),
            pltpu.VMEM((nx - 1, rows, quarter), BF16),
            pltpu.VMEM((nc, rows, LANES), BF16),
            pltpu.VMEM((chips * nc, rows, LANES), BF16),
            pltpu.VMEM((nc, CAP, LANES), BF16),
            pltpu.VMEM((groups, CAP, LANES), BF16),
            pltpu.VMEM((groups, CAP, LANES), BF16),
            pltpu.VMEM((groups, CAP, LANES), BF16),
            pltpu.VMEM((owners, owned, token_count), BF16),
            pltpu.VMEM((owners, owned // 2, LANES), BF16),
            pltpu.SemaphoreType.DMA((2, nx - 1)),
            pltpu.SemaphoreType.DMA((2,)),
            pltpu.SemaphoreType.DMA((2, groups - 1)),
            pltpu.SemaphoreType.DMA((2, groups - 1)),
            pltpu.SemaphoreType.DMA((2,)),
            pltpu.SemaphoreType.DMA((2,)),
            pltpu.SemaphoreType.DMA((5,)),
            pltpu.SemaphoreType.REGULAR,
            pltpu.VMEM((rows, qk, dv), F32),
        ],
        compiler_params=pltpu.CompilerParams(collective_id=0, has_side_effects=True),
    )(*operands)
    mixed, state, new_norm, new_max = pl.pallas_call(
        combine,
        out_shape=(
            shape((owned, token_count), BF16),
            shape((rows, qk, dv), F32),
            shape((rows, qk), F32),
            shape((1, rows), F32),
        ),
        in_specs=[hbm] * 6,
        out_specs=(vmem, hbm, vmem, vmem),
        scratch_shapes=[
            pltpu.VMEM((chips, owned // 2, LANES), BF16),
            pltpu.VMEM((owned, token_count), BF16),
            pltpu.VMEM((2, token_count), jnp.int32),
            pltpu.VMEM((2, token_count), F32),
            pltpu.VMEM((rows, pack_width), F32),
            pltpu.VMEM((rows, qk, dv), F32),
            pltpu.SemaphoreType.DMA((5,)),
            pltpu.SemaphoreType.DMA((rows,)),
            pltpu.SemaphoreType.DMA((rows,)),
        ],
    )(parts, mid, tgt, route_weight.T, pack, state)
    return (mixed.T, state[:, None], new_norm[:, None], new_max.T)


def solution(mesh):
    nx = mesh.shape["tp"]
    nc = 2
    nz = nx * nc
    ny = mesh.shape["ep"] // (nc * nz)
    finer = Mesh(mesh.devices.reshape(nz, ny, nc, nx), ("z", "y", "c", "x"))
    ep = ("z", "y", "c")
    in_specs = (
        P(ep, None),
        P(),
        P(None, "x"),
        P(None, "x"),
        P(None, "x"),
        P(None, "x"),
        P(),
        P(),
        P(),
        P("x"),
        P("x", None),
        P(ep, "x", None, None),
        P(ep, "x", None),
        P(ep, "x"),
        P(),
        P(),
        P(),
        P(ep, None, "x"),
        P(ep, None, "x"),
        P(ep, "x", None),
    )
    out_specs = (P(None, ep), P(ep, "x", None, None), P(ep, "x", None), P(ep, "x"))
    return jax.shard_map(
        functools.partial(shards, (nz, ny, nc, nx)),
        mesh=finer,
        in_specs=in_specs,
        out_specs=out_specs,
        check_vma=False,
    )
```

```python
import functools

import jax
import jax.numpy as jnp
from jax import lax
from jax.experimental import pallas as pl
from jax.experimental.pallas import tpu as pltpu
from jax.sharding import Mesh
from jax.sharding import PartitionSpec as P

MESH = pl.DeviceIdType.MESH
CAP = 32
LANES = 128
EPS = 1e-06
F32 = jnp.float32
BF16 = jnp.bfloat16


def dot(a, b):
    return jnp.dot(a, b, preferred_element_type=F32)


def kernel(
    sizes,
    tok_h,
    mix_h,
    wq_h,
    wk_h,
    wv_h,
    wo_h,
    wi_h,
    wf_h,
    fb_h,
    hg_h,
    wout_h,
    mem_h,
    nrm_h,
    rmax_h,
    fg_h,
    route_h,
    wgate_h,
    wup_h,
    wdown_h,
    frecv,
    mrecv,
    tgt_ref,
    pack_ref,
    state_ref,
    tok,
    mix,
    wq,
    wk,
    wv,
    wo,
    wi,
    wf,
    fb,
    hg,
    wout,
    mem,
    nrm,
    rmax,
    fg,
    route,
    wgate,
    wup,
    wdown,
    load_sem,
    tgt,
    pack,
    place,
    psend,
    precv,
    csend,
    crecv,
    esend,
    erecv,
    rsend,
    rrecv,
    msend,
    dsend,
    psem,
    csem,
    esem,
    rsem,
    msem,
    dsem,
    out_sem,
    plane_sem,
    state,
):
    nz, ny, nc, nx = sizes
    z, y, c, x = (lax.axis_index(a) for a in ("z", "y", "c", "x"))
    zy = z * ny + y
    ep = zy * nc + c
    rows, width = tok.shape
    groups = nx * nc
    quarter = width // nx
    chips = nz * ny
    owned = width // (chips * nc)
    owners = LANES // owned
    group = x * nc + c
    side = y % 2
    first_y = y - side
    half_lanes = LANES // 2
    expert_count = chips * nc
    token_count = route.shape[1]

    barrier = pltpu.get_barrier_semaphore()

    def greet(target):
        pl.semaphore_signal(barrier, inc=1, device_id=target, device_id_type=MESH)

    y_order = sorted(range(ny), key=lambda d: -min(d, ny - d))

    def ring_z(i):
        shift = nz // 2 + jnp.where(i % 2 == 0, i // 2, -((i + 1) // 2))
        return lax.rem(z + shift, nz)

    z_order = sorted(range(1, nz), key=lambda d: -min(d, nz - d))
    for dz in z_order:
        tz = lax.rem(z + dz, nz)
        for dc in range(nc):
            greet((tz, y, lax.rem(c + dc, nc), x))
    for dy in y_order[:-1]:
        greet((z, lax.rem(y + dy, ny), c, x))
    for dx in range(nx):
        for dc in range(nc):
            if dx + dc > 0:
                greet((z, y, lax.rem(c + dc, nc), lax.rem(x + dx, nx)))
    for dx in range(1, nx):
        for dc in range(nc):
            greet((z, y + 1 - 2 * side, lax.rem(c + dc, nc), lax.rem(x + dx, nx)))
    source_group = ep // owners
    source_x, source_c = source_group // nc, source_group % nc
    from_self = source_group == group

    pairs = {
        "tok": (tok_h, tok),
        "mix": (mix_h, mix),
        "wq": (wq_h, wq),
        "wk": (wk_h, wk),
        "wv": (wv_h, wv),
        "wo": (wo_h, wo),
        "wi": (wi_h, wi),
        "wf": (wf_h, wf),
        "fb": (fb_h, fb),
        "rmax": (rmax_h, rmax),
        "nrm": (nrm_h, nrm),
        "mem": (mem_h, mem),
        "hg": (hg_h, hg),
        "wout": (wout_h, wout),
        "route": (route_h, route),
        "fg": (fg_h, fg),
        "wgate": (wgate_h, wgate),
        "wup": (wup_h, wup),
        "wdown": (wdown_h, wdown),
    }
    loads = {
        n: pltpu.make_async_copy(h, v, load_sem.at[i]) for i, (n, (h, v)) in enumerate(pairs.items())
    }
    late = ("fg", "wgate", "wup", "wdown")
    for n in loads:
        if n not in late:
            loads[n].start()

    def ready(*names):
        for n in names:
            loads[n].wait()

    ready("tok", "mix")
    tokens = tok[...].astype(F32)
    mean = jnp.mean(tokens * tokens, axis=1, keepdims=True)
    normed = (tokens * lax.rsqrt(mean + EPS) * mix[...]).astype(BF16)
    ready("wq")
    query16 = dot(normed, wq[...]).astype(BF16)
    query = query16.astype(F32)
    ready("wk")
    scaled_key = dot(normed, wk[...]).astype(BF16).astype(F32) * wq.shape[1] ** (-0.5)
    ready("wv")
    value = dot(normed, wv[...]).astype(BF16).astype(F32)
    ready("wo")
    ogate = dot(normed, wo[...]).astype(BF16).astype(F32)
    ready("wi", "wf", "fb", "rmax", "nrm")
    floats = normed.astype(F32)
    head_row = lax.broadcasted_iota(jnp.int32, wi.shape, 0) == x
    in_row = jnp.sum(jnp.where(head_row, wi[...].astype(F32), 0.0), axis=0, keepdims=True)
    forget_row = jnp.sum(jnp.where(head_row, wf[...].astype(F32), 0.0), axis=0, keepdims=True)
    log_in = jnp.sum(floats * in_row, axis=1, keepdims=True)
    head_lane = lax.broadcasted_iota(jnp.int32, fb.shape, 1) == x
    bias = jnp.sum(jnp.where(head_lane, fb[...], 0.0), axis=1, keepdims=True)
    forget_pre = jnp.sum(floats * forget_row, axis=1, keepdims=True) + bias
    log_forget = jnp.minimum(forget_pre, 0.0) - jnp.log1p(jnp.exp(-jnp.abs(forget_pre)))
    diagonal = lax.broadcasted_iota(jnp.int32, (rows, rows), 0) == lax.broadcasted_iota(
        jnp.int32, (rows, rows), 1
    )
    old_max = jnp.sum(
        jnp.where(diagonal, jnp.broadcast_to(rmax[...], (rows, rows)), 0.0), axis=1, keepdims=True
    )
    carried = log_forget + old_max
    new_max = jnp.maximum(carried, log_in)
    keep = jnp.exp(carried - new_max)
    admit = jnp.exp(log_in - new_max)
    akey = admit * scaled_key
    norm_state = keep * nrm[...] + akey
    qk = wq.shape[1]
    pack[:, 0:qk] = norm_state
    pack[:, qk:] = jnp.broadcast_to(new_max, (rows, LANES))
    ready("mem")
    row_of = lax.broadcasted_iota(jnp.int32, value.shape, 0)
    kept = jnp.zeros_like(value)
    for t in range(rows):
        kept = jnp.where(row_of == t, dot(query16, mem[t].astype(BF16)), kept)
    numer = keep * kept + jnp.sum(query * akey, axis=1, keepdims=True) * value
    denom = jnp.sum(query * norm_state, axis=1, keepdims=True)
    read = numer / jnp.maximum(jnp.abs(denom), jnp.exp(-new_max))
    scale = lax.rsqrt(jnp.mean(read * read, axis=1, keepdims=True) + EPS)
    ready("hg", "wout")
    gated = (jax.nn.sigmoid(ogate) * read * scale * hg[...]).astype(BF16)
    partial = dot(gated, wout[...]).astype(BF16)
    for i in range(nx):
        psend[i] = partial[:, i * quarter : (i + 1) * quarter]
    pl.semaphore_wait(barrier, (nz - 1) * nc + ny - 1 + nx * nc - 1 + (nx - 1) * nc)

    for dy in y_order[:-1]:
        pl.semaphore_signal(
            plane_sem, inc=1, device_id=(z, lax.rem(y + dy, ny), c, x), device_id_type=MESH
        )

    for dx in range(1, nx):
        tx = lax.rem(x + dx, nx)
        pltpu.make_async_remote_copy(
            src_ref=psend.at[tx],
            dst_ref=precv.at[dx - 1],
            send_sem=psem.at[0, dx - 1],
            recv_sem=psem.at[1, dx - 1],
            device_id=(z, y, c, tx),
            device_id_type=MESH,
        ).start()

    for n in late:
        loads[n].start()
    ready("route")
    expert_of = lax.broadcasted_iota(jnp.int32, (expert_count, token_count), 0)
    named = [expert_of == route[j : j + 1, :] for j in range(2)]
    either = jnp.where(jnp.logical_or(named[0], named[1]), 1.0, 0.0)
    block = min(256, token_count)
    earlier = (
        lax.broadcasted_iota(jnp.int32, (block, block), 0)
        < lax.broadcasted_iota(jnp.int32, (block, block), 1)
    ).astype(F32).astype(BF16)
    carry = jnp.zeros((expert_count, 1), F32)
    before = []
    for b in range(token_count // block):
        part = either[:, b * block : (b + 1) * block]
        before.append(dot(part.astype(BF16), earlier) + carry)
        carry = carry + jnp.sum(part, axis=1, keepdims=True)
    before = jnp.concatenate(before, axis=1)
    for j in range(2):
        slot = jnp.sum(jnp.where(named[j], before, 0.0), axis=0, keepdims=True)
        tgt[j : j + 1, :] = route[j : j + 1, :] * CAP + slot.astype(jnp.int32)
    slots_here = nc * CAP
    slots_both = 2 * slots_here
    first_slot = (z * ny + first_y) * slots_here
    slot_id = lax.broadcasted_iota(jnp.int32, (slots_both, token_count), 0) + first_slot
    hit = jnp.logical_or(slot_id == tgt[0:1, :], slot_id == tgt[1:2, :])
    place[...] = jnp.where(hit, 1.0, 0.0).astype(BF16)
    keeps = [
        pltpu.make_async_copy(tgt, tgt_ref, out_sem.at[0]),
        pltpu.make_async_copy(pack, pack_ref, out_sem.at[1]),
    ]
    for copy in keeps:
        copy.start()

    total = psend[x].astype(F32)
    for dx in range(1, nx):
        copy = pltpu.make_async_remote_copy(
            src_ref=psend.at[0],
            dst_ref=precv.at[dx - 1],
            send_sem=psem.at[0, dx - 1],
            recv_sem=psem.at[1, dx - 1],
            device_id=(z, y, c, lax.rem(x + dx, nx)),
            device_id_type=MESH,
        )
        copy.wait_recv()
        total = total + precv[dx - 1].astype(F32)
    own = tok[:, pl.ds(pl.multiple_of(x * quarter, quarter), quarter)].astype(F32)
    middle = (own + total).astype(BF16).astype(F32)
    token_half = rows // 2
    low_rows = lax.broadcasted_iota(jnp.int32, (token_half, LANES), 1) < half_lanes
    for i in range(nc):
        tile = middle[:, i * LANES : (i + 1) * LANES]
        turned = pltpu.roll(tile, half_lanes, 1)
        csend[i, 0] = jnp.where(low_rows, tile[:token_half], turned[token_half:]).astype(BF16)
        csend[i, 1] = jnp.where(low_rows, turned[:token_half], tile[token_half:]).astype(BF16)

    def send_plane(i, carry):
        tz = ring_z(i)

        def send(ty, tc):
            pltpu.make_async_remote_copy(
                src_ref=csend.at[tc, ty % 2],
                dst_ref=crecv.at[ep],
                send_sem=csem.at[0],
                recv_sem=csem.at[1],
                device_id=(tz, ty, tc, x),
                device_id_type=MESH,
            ).start()

        for dy in y_order:
            ty = lax.rem(y + dy, ny)
            for dc in reversed(range(nc)):
                tc = lax.rem(c + dc, nc)
                if dy == 0 and dc == 0:

                    @pl.when(i < nz - 1)
                    def _():
                        send(ty, tc)
                else:
                    send(ty, tc)
        return carry

    pl.semaphore_wait(plane_sem, ny - 1)
    lax.fori_loop(0, nz, send_plane, 0)
    crecv[ep] = csend[c, side]

    for t in range(rows):
        key_columns = jnp.broadcast_to(akey[t : t + 1, :], (LANES, LANES)).T
        key_columns = jnp.concatenate([key_columns] * (wv.shape[1] // LANES), axis=1)
        state[t] = keep[t : t + 1, :] * mem[t] + key_columns * value[t : t + 1, :]
    keeps.append(pltpu.make_async_copy(state, state_ref, out_sem.at[4]))
    keeps[-1].start()
    others = crecv.at[pl.ds(0, chips * nc - 1)]
    plane = pltpu.make_async_remote_copy(
        src_ref=others,
        dst_ref=others,
        send_sem=csem.at[0],
        recv_sem=csem.at[1],
        device_id=(z, y, lax.rem(c + 1, nc), x),
        device_id_type=MESH,
    )
    plane.wait_recv()
    packed = crecv[...].astype(F32)
    everyone32 = jnp.concatenate([packed, pltpu.roll(packed, half_lanes, 2)], axis=1)
    everyone32 = everyone32.reshape(token_count, LANES)
    slots = dot(place[...], everyone32.astype(BF16))
    half_cap = CAP // 2
    low_slots = lax.broadcasted_iota(jnp.int32, (half_cap, LANES), 1) < half_lanes
    for i in range(2 * nc):
        upper = slots[i * CAP : i * CAP + half_cap]
        lower = slots[i * CAP + half_cap : (i + 1) * CAP]
        esend[i] = jnp.where(low_slots, upper, pltpu.roll(lower, half_lanes, 1)).astype(BF16)

    x_order = sorted(range(nx), key=lambda d: -min(d, nx - d))

    def chip_row(send, recv, sem, src_of, dst):
        copies = []
        for dx in x_order:
            for dc in reversed(range(nc)):
                if dx == 0 and dc == 0:
                    continue
                tx, tc = lax.rem(x + dx, nx), lax.rem(c + dc, nc)
                n = dx * nc + dc - 1
                copy = pltpu.make_async_remote_copy(
                    src_ref=send.at[src_of(tx, tc)],
                    dst_ref=recv.at[dst],
                    send_sem=sem.at[0, n],
                    recv_sem=sem.at[1, n],
                    device_id=(z, y, tc, tx),
                    device_id_type=MESH,
                )
                copy.start()
                copies.append(copy)
        return copies

    to_experts = []
    for dx in x_order:
        for dy in (1, 0):
            for dc in reversed(range(nc)):
                if dx + dy + dc > 0:
                    tx, tc = lax.rem(x + dx, nx), lax.rem(c + dc, nc)
                    there = side if dy == 0 else 1 - side
                    copy = pltpu.make_async_remote_copy(
                        src_ref=esend.at[there * nc + tc],
                        dst_ref=erecv.at[group, side],
                        send_sem=esem.at[0, len(to_experts)],
                        recv_sem=esem.at[1, len(to_experts)],
                        device_id=(z, first_y + there, tc, tx),
                        device_id_type=MESH,
                    )
                    copy.start()
                    to_experts.append(copy)
    erecv[group, side] = esend[side * nc + c]

    serves = jnp.logical_and(from_self, y // (ny // 2) == side)
    own_half = lax.rem(y, ny // 2) * nc + c

    @pl.when(serves)
    def _():
        turned = everyone32.T
        for k in range(owners // 2):
            msend[k] = turned[k * owned : (k + 1) * owned, :].astype(BF16)
        pltpu.make_async_copy(msend.at[own_half], mrecv, out_sem.at[2]).start()

    ready(*late)
    for copy in to_experts:
        copy.wait_recv()
    stacked = []
    for i in range(groups):
        left, right = erecv[i, 0].astype(F32), erecv[i, 1].astype(F32)
        left_turned = pltpu.roll(left, half_lanes, 1)
        right_turned = pltpu.roll(right, half_lanes, 1)
        tile = [jnp.where(low_slots, left, right_turned), jnp.where(low_slots, left_turned, right)]
        stacked.append(jnp.concatenate(tile, axis=0))
    stacked = jnp.concatenate(stacked, axis=1)
    mean = jnp.mean(stacked * stacked, axis=1, keepdims=True)
    routed = (stacked * lax.rsqrt(mean + EPS) * fg[...]).astype(BF16)
    gate_v = dot(routed, wgate[...])
    up_v = dot(routed, wup[...])
    act = (gate_v * jax.nn.sigmoid(gate_v) * up_v).astype(BF16)
    down = dot(act, wdown[...]).astype(BF16)
    for i in range(groups):
        rsend[i] = down[:, i * LANES : (i + 1) * LANES]

    to_groups = chip_row(rsend, rrecv, rsem, lambda tx, tc: tx * nc + tc, group)
    rrecv[group] = rsend[group]

    middle_copies = []
    for dx in x_order:
        for dy in (1, 0):
            for dc in reversed(range(nc)):
                if dx + dy + dc > 0:
                    tx, tc = lax.rem(x + dx, nx), lax.rem(c + dc, nc)
                    ty = y if dy == 0 else y + 1 - 2 * side
                    copy = pltpu.make_async_remote_copy(
                        src_ref=msend.at[lax.rem(ty, ny // 2) * nc + tc],
                        dst_ref=mrecv,
                        send_sem=msem.at[0],
                        recv_sem=msem.at[1],
                        device_id=(z, ty, tc, tx),
                        device_id_type=MESH,
                    )
                    middle_copies.append(copy)

    @pl.when(serves)
    def _():
        for copy in middle_copies:
            copy.start()

    for copy in to_groups:
        copy.wait_recv()
    results = []
    for i in range(nc):
        result = rrecv[i].astype(F32)
        for j in range(1, nx):
            result = result + rrecv[j * nc + i].astype(F32)
        results.append(result)
    low = lax.broadcasted_iota(jnp.int32, (owners, owned // 2, LANES), 2) < slots_here
    turned = jnp.concatenate(results + results, axis=0).T.reshape(owners, owned, LANES)
    half = owned // 2
    dsend[...] = jnp.where(low, turned[:, :half], turned[:, half:]).astype(BF16)

    def send_owners(i, carry):
        shift = ny // 2 + jnp.where(i % 2 == 0, i // 2, -((i + 1) // 2))
        ty = lax.rem(y + shift, ny)

        def send(tc, tx):
            pltpu.make_async_remote_copy(
                src_ref=dsend.at[ty * nc + tc],
                dst_ref=frecv.at[zy],
                send_sem=dsem.at[0],
                recv_sem=dsem.at[1],
                device_id=(group, ty, tc, tx),
                device_id_type=MESH,
            ).start()

        for dx in x_order:
            tx = lax.rem(x + dx, nx)
            for dc in reversed(range(nc)):
                tc = lax.rem(c + dc, nc)
                if dx == 0 and dc == 0:

                    @pl.when(jnp.logical_not(jnp.logical_and(from_self, i == ny - 1)))
                    def _():
                        send(tc, tx)
                else:
                    send(tc, tx)
        return carry

    lax.fori_loop(0, ny, send_owners, 0)

    def arrivals(n):
        part = frecv.at[pl.ds(0, n)]
        return pltpu.make_async_remote_copy(
            src_ref=part,
            dst_ref=part,
            send_sem=dsem.at[0],
            recv_sem=dsem.at[1],
            device_id=(z, y, lax.rem(c + 1, nc), x),
            device_id_type=MESH,
        )

    @pl.when(from_self)
    def _():
        own = pltpu.make_async_copy(dsend.at[lax.rem(ep, owners)], frecv.at[zy], out_sem.at[3])
        own.start()
        arrivals(chips - 1).wait_recv()
        own.wait()

    @pl.when(jnp.logical_not(from_self))
    def _():
        arrivals(chips).wait_recv()

    @pl.when(serves)
    def _():
        pltpu.make_async_copy(msend.at[own_half], mrecv, out_sem.at[2]).wait()

    @pl.when(jnp.logical_not(serves))
    def _():
        middle_copies[0].wait_recv()

    for copy in keeps:
        copy.wait()

    for dx in range(1, nx):
        pltpu.make_async_remote_copy(
            src_ref=psend.at[0],
            dst_ref=precv.at[dx - 1],
            send_sem=psem.at[0, dx - 1],
            recv_sem=psem.at[1, dx - 1],
            device_id=(z, y, c, lax.rem(x + dx, nx)),
            device_id_type=MESH,
        ).wait_send()
    plane.wait_send()
    for copy in to_experts + to_groups:
        copy.wait_send()

    @pl.when(from_self)
    def _():
        arrivals(chips - 1).wait_send()

    @pl.when(jnp.logical_not(from_self))
    def _():
        arrivals(chips).wait_send()

    @pl.when(serves)
    def _():
        for copy in middle_copies:
            copy.wait_send()


def combine(
    parts_h,
    mid_h,
    tgt_h,
    rw_h,
    pack_h,
    state_h,
    mixed_ref,
    newmem_ref,
    newnorm_ref,
    newmax_ref,
    parts,
    mid,
    tgt,
    rw,
    pack,
    state,
    load_sem,
    state_sem,
    sem,
):
    rows, qk, dv = state.shape
    chips, half, _ = parts.shape
    owned = 2 * half
    token_count = tgt.shape[1]
    loads = []
    for i, (h, v) in enumerate(
        ((pack_h, pack), (tgt_h, tgt), (parts_h, parts), (mid_h, mid), (rw_h, rw))
    ):
        loads.append(pltpu.make_async_copy(h, v, load_sem.at[i]))
    moves = [pltpu.make_async_copy(state_h.at[t], state.at[t], state_sem.at[t]) for t in range(rows)]
    for copy in loads + moves:
        copy.start()
    loads[0].wait()
    newnorm_ref[...] = pack[:, 0:qk]
    diagonal = lax.broadcasted_iota(jnp.int32, (rows, LANES), 0) == lax.broadcasted_iota(
        jnp.int32, (rows, LANES), 1
    )
    newmax_ref[...] = jnp.sum(jnp.where(diagonal, pack[:, qk:], 0.0), axis=0, keepdims=True)[:, :rows]
    copies = []
    for t in range(rows):
        moves[t].wait()
        copy = pltpu.make_async_copy(state.at[t], newmem_ref.at[t], sem.at[t])
        copy.start()
        copies.append(copy)
    for copy in loads[1:]:
        copy.wait()

    low = lax.broadcasted_iota(jnp.int32, (chips // 2, half, LANES), 2) < LANES // 2
    both = parts[...].astype(F32).reshape(chips // 2, 2, half, LANES)
    even, odd = both[:, 0], both[:, 1]
    even_turned = pltpu.roll(even, LANES // 2, 2)
    odd_turned = pltpu.roll(odd, LANES // 2, 2)
    held = jnp.concatenate(
        [jnp.where(low, even, odd_turned), jnp.where(low, even_turned, odd)], axis=1
    )
    held = held.reshape(chips // 2 * owned, LANES).astype(BF16)
    lane_id = lax.broadcasted_iota(jnp.int32, (LANES, LANES), 0)
    for k in range(token_count // LANES):
        span = slice(k * LANES, (k + 1) * LANES)
        names = [tgt[j : j + 1, span] for j in range(2)]
        picks = jnp.concatenate(
            [
                jnp.where(lane_id == jnp.bitwise_and(n, LANES - 1), 1.0, 0.0).astype(BF16)
                for n in names
            ],
            axis=1,
        )
        found = dot(held, picks)
        total = []
        for j in range(2):
            place = jnp.broadcast_to(lax.shift_right_logical(names[j], 7), (owned, LANES))
            got = jnp.zeros((owned, LANES), F32)
            for p in range(chips // 2):
                part = found[p * owned : (p + 1) * owned, j * LANES : (j + 1) * LANES]
                got = jnp.where(place == p, part, got)
            total.append(got)
        w0, w1 = rw[0:1, span], rw[1:2, span]
        weighed = total[0] * (w0 / (w0 + w1)) + total[1] * (w1 / (w0 + w1))
        mixed_ref[:, span] = (mid[:, span].astype(F32) + weighed).astype(BF16)
    for copy in copies:
        copy.wait()


def shards(
    sizes,
    tokens,
    mix_gain,
    w_query,
    w_key,
    w_value,
    w_ogate,
    w_igate,
    w_fgate,
    forget_bias,
    head_gain,
    w_out,
    memory,
    normalizer,
    running_max,
    ffn_gain,
    route,
    route_weight,
    w_gate,
    w_up,
    w_down,
):
    nz, ny, nc, nx = sizes
    rows, width = tokens.shape
    qk, dv = memory.shape[2:]
    chips = nz * ny
    quarter = width // nx
    groups = nx * nc
    owned = width // (chips * nc)
    owners = LANES // owned
    token_count = route.shape[0]
    operands = (
        tokens,
        mix_gain.reshape(1, -1),
        w_query,
        w_key,
        w_value,
        w_ogate,
        w_igate.T,
        w_fgate.T,
        forget_bias.reshape(1, -1),
        head_gain.reshape(1, -1),
        w_out,
        memory.reshape(rows, qk, dv),
        normalizer.reshape(rows, qk),
        running_max.T,
        ffn_gain.reshape(1, -1),
        route.T,
        w_gate[0],
        w_up[0],
        w_down[0],
    )
    shape = jax.ShapeDtypeStruct
    vmem = pl.BlockSpec(memory_space=pltpu.VMEM)
    hbm = pl.BlockSpec(memory_space=pl.ANY)
    pack_width = LANES + qk
    parts, mid, tgt, pack, state = pl.pallas_call(
        functools.partial(kernel, sizes),
        out_shape=(
            shape((chips, owned // 2, LANES), BF16),
            shape((owned, token_count), BF16),
            shape((2, token_count), jnp.int32),
            shape((rows, pack_width), F32),
            shape((rows, qk, dv), F32),
        ),
        in_specs=[hbm] * len(operands),
        out_specs=(hbm,) * 5,
        scratch_shapes=[pltpu.VMEM(a.shape, a.dtype) for a in operands]
        + [
            pltpu.SemaphoreType.DMA((len(operands),)),
            pltpu.VMEM((2, token_count), jnp.int32),
            pltpu.VMEM((rows, pack_width), F32),
            pltpu.VMEM((2 * nc * CAP, token_count), BF16),
            pltpu.VMEM((nx, rows, quarter), BF16),
            pltpu.VMEM((nx - 1, rows, quarter), BF16),
            pltpu.VMEM((nc, 2, rows // 2, LANES), BF16),
            pltpu.VMEM((chips * nc, rows // 2, LANES), BF16),
            pltpu.VMEM((2 * nc, CAP // 2, LANES), BF16),
            pltpu.VMEM((groups, 2, CAP // 2, LANES), BF16),
            pltpu.VMEM((groups, CAP, LANES), BF16),
            pltpu.VMEM((groups, CAP, LANES), BF16),
            pltpu.VMEM((owners // 2, owned, token_count), BF16),
            pltpu.VMEM((owners, owned // 2, LANES), BF16),
            pltpu.SemaphoreType.DMA((2, nx - 1)),
            pltpu.SemaphoreType.DMA((2,)),
            pltpu.SemaphoreType.DMA((2, 2 * groups - 1)),
            pltpu.SemaphoreType.DMA((2, groups - 1)),
            pltpu.SemaphoreType.DMA((2,)),
            pltpu.SemaphoreType.DMA((2,)),
            pltpu.SemaphoreType.DMA((5,)),
            pltpu.SemaphoreType.REGULAR,
            pltpu.VMEM((rows, qk, dv), F32),
        ],
        compiler_params=pltpu.CompilerParams(collective_id=0, has_side_effects=True),
    )(*operands)
    mixed, state, new_norm, new_max = pl.pallas_call(
        combine,
        out_shape=(
            shape((owned, token_count), BF16),
            shape((rows, qk, dv), F32),
            shape((rows, qk), F32),
            shape((1, rows), F32),
        ),
        in_specs=[hbm] * 6,
        out_specs=(vmem, hbm, vmem, vmem),
        scratch_shapes=[
            pltpu.VMEM((chips, owned // 2, LANES), BF16),
            pltpu.VMEM((owned, token_count), BF16),
            pltpu.VMEM((2, token_count), jnp.int32),
            pltpu.VMEM((2, token_count), F32),
            pltpu.VMEM((rows, pack_width), F32),
            pltpu.VMEM((rows, qk, dv), F32),
            pltpu.SemaphoreType.DMA((5,)),
            pltpu.SemaphoreType.DMA((rows,)),
            pltpu.SemaphoreType.DMA((rows,)),
        ],
    )(parts, mid, tgt, route_weight.T, pack, state)
    return (mixed.T, state[:, None], new_norm[:, None], new_max.T)


def solution(mesh):
    nx = mesh.shape["tp"]
    nc = 2
    nz = nx * nc
    ny = mesh.shape["ep"] // (nc * nz)
    finer = Mesh(mesh.devices.reshape(nz, ny, nc, nx), ("z", "y", "c", "x"))
    ep = ("z", "y", "c")
    in_specs = (
        P(ep, None),
        P(),
        P(None, "x"),
        P(None, "x"),
        P(None, "x"),
        P(None, "x"),
        P(),
        P(),
        P(),
        P("x"),
        P("x", None),
        P(ep, "x", None, None),
        P(ep, "x", None),
        P(ep, "x"),
        P(),
        P(),
        P(),
        P(ep, None, "x"),
        P(ep, None, "x"),
        P(ep, "x", None),
    )
    out_specs = (P(None, ep), P(ep, "x", None, None), P(ep, "x", None), P(ep, "x"))
    return jax.shard_map(
        functools.partial(shards, (nz, ny, nc, nx)),
        mesh=finer,
        in_specs=in_specs,
        out_specs=out_specs,
        check_vma=False,
    )
```

```python
import functools

import jax
import jax.numpy as jnp
from jax import lax
from jax.experimental import pallas as pl
from jax.experimental.pallas import tpu as pltpu
from jax.sharding import Mesh
from jax.sharding import PartitionSpec as P

MESH = pl.DeviceIdType.MESH
CAP = 32
LANES = 128
EPS = 1e-06
F32 = jnp.float32
BF16 = jnp.bfloat16


def dot(a, b):
    return jnp.dot(a, b, preferred_element_type=F32)


def kernel(
    sizes,
    tok_h,
    mix_h,
    wq_h,
    wk_h,
    wv_h,
    wo_h,
    wi_h,
    wf_h,
    fb_h,
    hg_h,
    wout_h,
    mem_h,
    nrm_h,
    rmax_h,
    fg_h,
    route_h,
    wgate_h,
    wup_h,
    wdown_h,
    frecv,
    mrecv,
    tgt_ref,
    pack_ref,
    state_ref,
    tok,
    mix,
    wq,
    wk,
    wv,
    wo,
    wi,
    wf,
    fb,
    hg,
    wout,
    mem,
    nrm,
    rmax,
    fg,
    route,
    wgate,
    wup,
    wdown,
    load_sem,
    tgt,
    pack,
    place,
    psend,
    precv,
    csend,
    crecv,
    esend,
    erecv,
    rsend,
    rrecv,
    msend,
    dsend,
    psem,
    csem,
    esem,
    rsem,
    msem,
    dsem,
    out_sem,
    plane_sem,
    state,
):
    nz, ny, nc, nx = sizes
    z, y, c, x = (lax.axis_index(a) for a in ("z", "y", "c", "x"))
    zy = z * ny + y
    ep = zy * nc + c
    rows, width = tok.shape
    groups = nx * nc
    quarter = width // nx
    chips = nz * ny
    owned = width // (chips * nc)
    owners = LANES // owned
    group = x * nc + c
    side = y % 2
    first_y = y - side
    half_lanes = LANES // 2
    expert_count = chips * nc
    token_count = route.shape[1]

    pairs = {
        "tok": (tok_h, tok),
        "mix": (mix_h, mix),
        "wq": (wq_h, wq),
        "wk": (wk_h, wk),
        "wv": (wv_h, wv),
        "wo": (wo_h, wo),
        "wi": (wi_h, wi),
        "wf": (wf_h, wf),
        "fb": (fb_h, fb),
        "rmax": (rmax_h, rmax),
        "nrm": (nrm_h, nrm),
        "mem": (mem_h, mem),
        "hg": (hg_h, hg),
        "wout": (wout_h, wout),
        "route": (route_h, route),
        "fg": (fg_h, fg),
        "wgate": (wgate_h, wgate),
        "wup": (wup_h, wup),
        "wdown": (wdown_h, wdown),
    }
    loads = {
        n: pltpu.make_async_copy(h, v, load_sem.at[i]) for i, (n, (h, v)) in enumerate(pairs.items())
    }
    late = ("fg", "wgate", "wup", "wdown")
    for n in loads:
        if n not in late:
            loads[n].start()

    def ready(*names):
        for n in names:
            loads[n].wait()

    barrier = pltpu.get_barrier_semaphore()

    def greet(target):
        pl.semaphore_signal(barrier, inc=1, device_id=target, device_id_type=MESH)

    y_order = sorted(range(ny), key=lambda d: -min(d, ny - d))

    def ring_z(i):
        shift = nz // 2 + jnp.where(i % 2 == 0, i // 2, -((i + 1) // 2))
        return lax.rem(z + shift, nz)

    z_order = sorted(range(1, nz), key=lambda d: -min(d, nz - d))
    for dz in z_order:
        tz = lax.rem(z + dz, nz)
        for dc in range(nc):
            greet((tz, y, lax.rem(c + dc, nc), x))
    for dy in y_order[:-1]:
        greet((z, lax.rem(y + dy, ny), c, x))
    for dx in range(nx):
        for dc in range(nc):
            if dx + dc > 0:
                greet((z, y, lax.rem(c + dc, nc), lax.rem(x + dx, nx)))
    for dx in range(1, nx):
        for dc in range(nc):
            greet((z, y + 1 - 2 * side, lax.rem(c + dc, nc), lax.rem(x + dx, nx)))
    source_group = ep // owners
    from_self = source_group == group
    result_group = lax.rem(x + nx - lax.rem(z, nx), nx) * nc + c
    result_from_self = source_group == result_group

    ready("tok", "mix")
    tokens = tok[...].astype(F32)
    mean = jnp.mean(tokens * tokens, axis=1, keepdims=True)
    normed = (tokens * lax.rsqrt(mean + EPS) * mix[...]).astype(BF16)
    ready("wq")
    query16 = dot(normed, wq[...]).astype(BF16)
    query = query16.astype(F32)
    ready("wk")
    scaled_key = dot(normed, wk[...]).astype(BF16).astype(F32) * wq.shape[1] ** (-0.5)
    ready("wv", "wo")
    value = dot(normed, wv[...]).astype(BF16).astype(F32)
    ogate = dot(normed, wo[...]).astype(BF16).astype(F32)
    ready("wi", "wf", "fb", "rmax", "nrm")
    floats = normed.astype(F32)
    head_row = lax.broadcasted_iota(jnp.int32, wi.shape, 0) == x
    in_row = jnp.sum(jnp.where(head_row, wi[...].astype(F32), 0.0), axis=0, keepdims=True)
    forget_row = jnp.sum(jnp.where(head_row, wf[...].astype(F32), 0.0), axis=0, keepdims=True)
    log_in = jnp.sum(floats * in_row, axis=1, keepdims=True)
    head_lane = lax.broadcasted_iota(jnp.int32, fb.shape, 1) == x
    bias = jnp.sum(jnp.where(head_lane, fb[...], 0.0), axis=1, keepdims=True)
    forget_pre = jnp.sum(floats * forget_row, axis=1, keepdims=True) + bias
    log_forget = jnp.minimum(forget_pre, 0.0) - jnp.log1p(jnp.exp(-jnp.abs(forget_pre)))
    diagonal = lax.broadcasted_iota(jnp.int32, (rows, rows), 0) == lax.broadcasted_iota(
        jnp.int32, (rows, rows), 1
    )
    old_max = jnp.sum(
        jnp.where(diagonal, jnp.broadcast_to(rmax[...], (rows, rows)), 0.0), axis=1, keepdims=True
    )
    carried = log_forget + old_max
    new_max = jnp.maximum(carried, log_in)
    keep = jnp.exp(carried - new_max)
    admit = jnp.exp(log_in - new_max)
    akey = admit * scaled_key
    norm_state = keep * nrm[...] + akey
    qk = wq.shape[1]
    pack[:, 0:qk] = norm_state
    pack[:, qk:] = jnp.broadcast_to(new_max, (rows, LANES))
    ready("mem", "hg", "wout")
    row_of = lax.broadcasted_iota(jnp.int32, value.shape, 0)
    kept = jnp.zeros_like(value)
    for t in range(rows):
        kept = jnp.where(row_of == t, dot(query16, mem[t].astype(BF16)), kept)
    numer = keep * kept + jnp.sum(query * akey, axis=1, keepdims=True) * value
    denom = jnp.sum(query * norm_state, axis=1, keepdims=True)
    read = numer / jnp.maximum(jnp.abs(denom), jnp.exp(-new_max))
    scale = lax.rsqrt(jnp.mean(read * read, axis=1, keepdims=True) + EPS)
    gated = (jax.nn.sigmoid(ogate) * read * scale * hg[...]).astype(BF16)
    partial = dot(gated, wout[...]).astype(BF16)
    for i in range(nx):
        psend[i] = partial[:, i * quarter : (i + 1) * quarter]
    pl.semaphore_wait(barrier, (nz - 1) * nc + ny - 1 + nx * nc - 1 + (nx - 1) * nc)

    for dy in y_order[:-1]:
        pl.semaphore_signal(
            plane_sem, inc=1, device_id=(z, lax.rem(y + dy, ny), c, x), device_id_type=MESH
        )

    x_order = sorted(range(nx), key=lambda d: -min(d, nx - d))
    for dx in x_order[:-1]:
        tx = lax.rem(x + dx, nx)
        pltpu.make_async_remote_copy(
            src_ref=psend.at[tx],
            dst_ref=precv.at[dx - 1],
            send_sem=psem.at[0, dx - 1],
            recv_sem=psem.at[1, dx - 1],
            device_id=(z, y, c, tx),
            device_id_type=MESH,
        ).start()

    for n in late:
        loads[n].start()
    ready("route")
    expert_of = lax.broadcasted_iota(jnp.int32, (expert_count, token_count), 0)
    named = [expert_of == route[j : j + 1, :] for j in range(2)]
    either = jnp.where(jnp.logical_or(named[0], named[1]), 1.0, 0.0)
    block = min(256, token_count)
    earlier = (
        lax.broadcasted_iota(jnp.int32, (block, block), 0)
        < lax.broadcasted_iota(jnp.int32, (block, block), 1)
    ).astype(F32).astype(BF16)
    carry = jnp.zeros((expert_count, 1), F32)
    before = []
    for b in range(token_count // block):
        part = either[:, b * block : (b + 1) * block]
        before.append(dot(part.astype(BF16), earlier) + carry)
        carry = carry + jnp.sum(part, axis=1, keepdims=True)
    before = jnp.concatenate(before, axis=1)
    for j in range(2):
        slot = jnp.sum(jnp.where(named[j], before, 0.0), axis=0, keepdims=True)
        tgt[j : j + 1, :] = route[j : j + 1, :] * CAP + slot.astype(jnp.int32)
    slots_here = nc * CAP
    slots_both = 2 * slots_here
    first_slot = (z * ny + first_y) * slots_here
    slot_id = lax.broadcasted_iota(jnp.int32, (slots_both, token_count), 0) + first_slot
    hit = jnp.logical_or(slot_id == tgt[0:1, :], slot_id == tgt[1:2, :])
    place[...] = jnp.where(hit, 1.0, 0.0).astype(BF16)
    keeps = [
        pltpu.make_async_copy(tgt, tgt_ref, out_sem.at[0]),
        pltpu.make_async_copy(pack, pack_ref, out_sem.at[1]),
    ]
    for copy in keeps:
        copy.start()

    total = psend[x].astype(F32)
    for dx in range(1, nx):
        copy = pltpu.make_async_remote_copy(
            src_ref=psend.at[0],
            dst_ref=precv.at[dx - 1],
            send_sem=psem.at[0, dx - 1],
            recv_sem=psem.at[1, dx - 1],
            device_id=(z, y, c, lax.rem(x + dx, nx)),
            device_id_type=MESH,
        )
        copy.wait_recv()
        total = total + precv[dx - 1].astype(F32)
    own = tok[:, pl.ds(pl.multiple_of(x * quarter, quarter), quarter)].astype(F32)
    middle = (own + total).astype(BF16).astype(F32)
    token_half = rows // 2
    low_rows = lax.broadcasted_iota(jnp.int32, (token_half, LANES), 1) < half_lanes
    for i in range(nc):
        tile = middle[:, i * LANES : (i + 1) * LANES]
        turned = pltpu.roll(tile, half_lanes, 1)
        csend[i, 0] = jnp.where(low_rows, tile[:token_half], turned[token_half:]).astype(BF16)
        csend[i, 1] = jnp.where(low_rows, turned[:token_half], tile[token_half:]).astype(BF16)

    def send_plane(i, carry):
        tz = ring_z(i)

        def send(ty, tc):
            pltpu.make_async_remote_copy(
                src_ref=csend.at[tc, ty % 2],
                dst_ref=crecv.at[ep],
                send_sem=csem.at[0],
                recv_sem=csem.at[1],
                device_id=(tz, ty, tc, x),
                device_id_type=MESH,
            ).start()

        for dy in y_order:
            ty = lax.rem(y + dy, ny)
            for dc in reversed(range(nc)):
                tc = lax.rem(c + dc, nc)
                if dy == 0 and dc == 0:

                    @pl.when(i < nz - 1)
                    def _():
                        send(ty, tc)
                else:
                    send(ty, tc)
        return carry

    pl.semaphore_wait(plane_sem, ny - 1)
    lax.fori_loop(0, nz, send_plane, 0)
    crecv[ep] = csend[c, side]

    for t in range(rows):
        key_columns = jnp.broadcast_to(akey[t : t + 1, :], (LANES, LANES)).T
        key_columns = jnp.concatenate([key_columns] * (wv.shape[1] // LANES), axis=1)
        state[t] = keep[t : t + 1, :] * mem[t] + key_columns * value[t : t + 1, :]
    keeps.append(pltpu.make_async_copy(state, state_ref, out_sem.at[4]))
    keeps[-1].start()
    others = crecv.at[pl.ds(0, chips * nc - 1)]
    plane = pltpu.make_async_remote_copy(
        src_ref=others,
        dst_ref=others,
        send_sem=csem.at[0],
        recv_sem=csem.at[1],
        device_id=(z, y, lax.rem(c + 1, nc), x),
        device_id_type=MESH,
    )
    plane.wait_recv()
    packed = crecv[...].astype(F32)
    everyone32 = jnp.concatenate([packed, pltpu.roll(packed, half_lanes, 2)], axis=1)
    everyone32 = everyone32.reshape(token_count, LANES)
    slots = dot(place[...], everyone32.astype(BF16))
    half_cap = CAP // 2
    low_slots = lax.broadcasted_iota(jnp.int32, (half_cap, LANES), 1) < half_lanes
    for i in range(2 * nc):
        upper = slots[i * CAP : i * CAP + half_cap]
        lower = slots[i * CAP + half_cap : (i + 1) * CAP]
        esend[i] = jnp.where(low_slots, upper, pltpu.roll(lower, half_lanes, 1)).astype(BF16)

    def chip_row(send, recv, sem, src_of, dst):
        copies = []
        for dx in x_order:
            for dc in reversed(range(nc)):
                if dx == 0 and dc == 0:
                    continue
                tx, tc = lax.rem(x + dx, nx), lax.rem(c + dc, nc)
                n = dx * nc + dc - 1
                copy = pltpu.make_async_remote_copy(
                    src_ref=send.at[src_of(tx, tc)],
                    dst_ref=recv.at[dst],
                    send_sem=sem.at[0, n],
                    recv_sem=sem.at[1, n],
                    device_id=(z, y, tc, tx),
                    device_id_type=MESH,
                )
                copy.start()
                copies.append(copy)
        return copies

    to_experts = []
    for dx in x_order:
        for dy in (1, 0):
            for dc in reversed(range(nc)):
                if dx + dy + dc > 0:
                    tx, tc = lax.rem(x + dx, nx), lax.rem(c + dc, nc)
                    there = side if dy == 0 else 1 - side
                    copy = pltpu.make_async_remote_copy(
                        src_ref=esend.at[there * nc + tc],
                        dst_ref=erecv.at[group, side],
                        send_sem=esem.at[0, len(to_experts)],
                        recv_sem=esem.at[1, len(to_experts)],
                        device_id=(z, first_y + there, tc, tx),
                        device_id_type=MESH,
                    )
                    copy.start()
                    to_experts.append(copy)
    erecv[group, side] = esend[side * nc + c]

    serves = jnp.logical_and(from_self, y // (ny // 2) == side)
    own_half = lax.rem(y, ny // 2) * nc + c

    @pl.when(serves)
    def _():
        turned = everyone32.T
        for k in range(owners // 2):
            msend[k] = turned[k * owned : (k + 1) * owned, :].astype(BF16)
        pltpu.make_async_copy(msend.at[own_half], mrecv, out_sem.at[2]).start()

    ready(*late)
    for copy in to_experts:
        copy.wait_recv()
    stacked = []
    for i in range(groups):
        left, right = erecv[i, 0].astype(F32), erecv[i, 1].astype(F32)
        left_turned = pltpu.roll(left, half_lanes, 1)
        right_turned = pltpu.roll(right, half_lanes, 1)
        tile = [jnp.where(low_slots, left, right_turned), jnp.where(low_slots, left_turned, right)]
        stacked.append(jnp.concatenate(tile, axis=0))
    stacked = jnp.concatenate(stacked, axis=1)
    mean = jnp.mean(stacked * stacked, axis=1, keepdims=True)
    routed = (stacked * lax.rsqrt(mean + EPS) * fg[...]).astype(BF16)
    gate_v = dot(routed, wgate[...])
    up_v = dot(routed, wup[...])
    act = (gate_v * jax.nn.sigmoid(gate_v) * up_v).astype(BF16)
    down = dot(act, wdown[...]).astype(BF16)
    for i in range(groups):
        rsend[i] = down[:, i * LANES : (i + 1) * LANES]

    def result_of(tx, tc):
        return lax.rem(tx + nx - lax.rem(z, nx), nx) * nc + tc

    to_groups = chip_row(rsend, rrecv, rsem, result_of, group)
    rrecv[group] = rsend[result_group]

    middle_copies = []
    for dx in x_order:
        for dy in (1, 0):
            for dc in reversed(range(nc)):
                if dx + dy + dc > 0:
                    tx, tc = lax.rem(x + dx, nx), lax.rem(c + dc, nc)
                    ty = y if dy == 0 else y + 1 - 2 * side
                    copy = pltpu.make_async_remote_copy(
                        src_ref=msend.at[lax.rem(ty, ny // 2) * nc + tc],
                        dst_ref=mrecv,
                        send_sem=msem.at[0],
                        recv_sem=msem.at[1],
                        device_id=(z, ty, tc, tx),
                        device_id_type=MESH,
                    )
                    middle_copies.append(copy)

    @pl.when(serves)
    def _():
        for copy in middle_copies:
            copy.start()

    for copy in to_groups:
        copy.wait_recv()
    results = []
    for i in range(nc):
        result = rrecv[i].astype(F32)
        for j in range(1, nx):
            result = result + rrecv[j * nc + i].astype(F32)
        results.append(result)
    low = lax.broadcasted_iota(jnp.int32, (owners, owned // 2, LANES), 2) < slots_here
    turned = jnp.concatenate(results + results, axis=0).T.reshape(owners, owned, LANES)
    half = owned // 2
    dsend[...] = jnp.where(low, turned[:, :half], turned[:, half:]).astype(BF16)

    def send_owners(i, carry):
        shift = ny // 2 + jnp.where(i % 2 == 0, i // 2, -((i + 1) // 2))
        ty = lax.rem(y + shift, ny)

        def send(tc, tx):
            pltpu.make_async_remote_copy(
                src_ref=dsend.at[ty * nc + tc],
                dst_ref=frecv.at[zy],
                send_sem=dsem.at[0],
                recv_sem=dsem.at[1],
                device_id=(result_group, ty, tc, tx),
                device_id_type=MESH,
            ).start()

        for dx in x_order:
            tx = lax.rem(x + dx, nx)
            for dc in reversed(range(nc)):
                tc = lax.rem(c + dc, nc)
                if dx == 0 and dc == 0:

                    @pl.when(jnp.logical_not(jnp.logical_and(result_from_self, i == ny - 1)))
                    def _():
                        send(tc, tx)
                else:
                    send(tc, tx)
        return carry

    lax.fori_loop(0, ny, send_owners, 0)

    def arrivals(n):
        part = frecv.at[pl.ds(0, n)]
        return pltpu.make_async_remote_copy(
            src_ref=part,
            dst_ref=part,
            send_sem=dsem.at[0],
            recv_sem=dsem.at[1],
            device_id=(z, y, lax.rem(c + 1, nc), x),
            device_id_type=MESH,
        )

    @pl.when(result_from_self)
    def _():
        own = pltpu.make_async_copy(dsend.at[lax.rem(ep, owners)], frecv.at[zy], out_sem.at[3])
        own.start()
        arrivals(chips - 1).wait_recv()
        own.wait()

    @pl.when(jnp.logical_not(result_from_self))
    def _():
        arrivals(chips).wait_recv()

    @pl.when(serves)
    def _():
        pltpu.make_async_copy(msend.at[own_half], mrecv, out_sem.at[2]).wait()

    @pl.when(jnp.logical_not(serves))
    def _():
        middle_copies[0].wait_recv()

    for copy in keeps:
        copy.wait()

    for dx in range(1, nx):
        pltpu.make_async_remote_copy(
            src_ref=psend.at[0],
            dst_ref=precv.at[dx - 1],
            send_sem=psem.at[0, dx - 1],
            recv_sem=psem.at[1, dx - 1],
            device_id=(z, y, c, lax.rem(x + dx, nx)),
            device_id_type=MESH,
        ).wait_send()
    plane.wait_send()
    for copy in to_experts + to_groups:
        copy.wait_send()

    @pl.when(result_from_self)
    def _():
        arrivals(chips - 1).wait_send()

    @pl.when(jnp.logical_not(result_from_self))
    def _():
        arrivals(chips).wait_send()

    @pl.when(serves)
    def _():
        for copy in middle_copies:
            copy.wait_send()


def lane_of(name):
    return jnp.bitwise_and(name, LANES - 1).astype(F32).astype(BF16)


def combine(
    parts_h,
    mid_h,
    tgt_h,
    rw_h,
    pack_h,
    state_h,
    mixed_h,
    newmem_h,
    newnorm_h,
    newmax_h,
    mixed,
    newnorm,
    newmax,
    parts,
    mid,
    tgt,
    rw,
    pack,
    state,
    load_sem,
    state_sem,
    sem,
):
    rows, qk, dv = state.shape
    chips, half, _ = parts.shape
    owned = 2 * half
    token_count = tgt.shape[1]
    loads = []
    for i, (h, v) in enumerate(
        ((pack_h, pack), (parts_h, parts), (tgt_h, tgt), (mid_h, mid), (rw_h, rw))
    ):
        loads.append(pltpu.make_async_copy(h, v, load_sem.at[i]))
    moves = [pltpu.make_async_copy(state_h.at[t], state.at[t], state_sem.at[t]) for t in range(rows)]
    for copy in loads + moves:
        copy.start()
    loads[0].wait()
    newnorm[...] = pack[:, 0:qk]
    diagonal = lax.broadcasted_iota(jnp.int32, (rows, LANES), 0) == lax.broadcasted_iota(
        jnp.int32, (rows, LANES), 1
    )
    newmax[...] = jnp.sum(jnp.where(diagonal, pack[:, qk:], 0.0), axis=0, keepdims=True)[:, :rows]
    copies = []
    for t in range(rows):
        moves[t].wait()
        copy = pltpu.make_async_copy(state.at[t], newmem_h.at[t], sem.at[t])
        copy.start()
        copies.append(copy)
    for copy in loads[1:]:
        copy.wait()

    low = lax.broadcasted_iota(jnp.int32, (chips // 2, half, LANES), 2) < LANES // 2
    both = parts[...].astype(F32).reshape(chips // 2, 2, half, LANES)
    even, odd = both[:, 0], both[:, 1]
    even_turned = pltpu.roll(even, LANES // 2, 2)
    odd_turned = pltpu.roll(odd, LANES // 2, 2)
    held = jnp.concatenate(
        [jnp.where(low, even, odd_turned), jnp.where(low, even_turned, odd)], axis=1
    )
    held = held.reshape(chips // 2 * owned, LANES).astype(BF16)
    lane_id = lax.broadcasted_iota(jnp.int32, (LANES, LANES), 0).astype(F32).astype(BF16)
    for k in range(token_count // LANES):
        span = slice(k * LANES, (k + 1) * LANES)
        names = [tgt[j : j + 1, span] for j in range(2)]
        picks = jnp.concatenate(
            [
                jnp.where(lane_id == lane_of(n), jnp.ones((), BF16), jnp.zeros((), BF16))
                for n in names
            ],
            axis=1,
        )
        found = dot(held, picks)
        total = []
        for j in range(2):
            place = jnp.broadcast_to(lax.shift_right_logical(names[j], 7), (owned, LANES))
            got = jnp.zeros((owned, LANES), F32)
            for p in range(chips // 2):
                part = found[p * owned : (p + 1) * owned, j * LANES : (j + 1) * LANES]
                got = jnp.where(place == p, part, got)
            total.append(got)
        w0, w1 = rw[0:1, span], rw[1:2, span]
        weighed = total[0] * (w0 / (w0 + w1)) + total[1] * (w1 / (w0 + w1))
        mixed[:, span] = (mid[:, span].astype(F32) + weighed).astype(BF16)
    outs = ((mixed, mixed_h), (newnorm, newnorm_h), (newmax, newmax_h))
    for i, (v, h) in enumerate(outs):
        copy = pltpu.make_async_copy(v, h, sem.at[rows + i])
        copy.start()
        copies.append(copy)
    for copy in copies:
        copy.wait()


def shards(
    sizes,
    tokens,
    mix_gain,
    w_query,
    w_key,
    w_value,
    w_ogate,
    w_igate,
    w_fgate,
    forget_bias,
    head_gain,
    w_out,
    memory,
    normalizer,
    running_max,
    ffn_gain,
    route,
    route_weight,
    w_gate,
    w_up,
    w_down,
):
    nz, ny, nc, nx = sizes
    rows, width = tokens.shape
    qk, dv = memory.shape[2:]
    chips = nz * ny
    quarter = width // nx
    groups = nx * nc
    owned = width // (chips * nc)
    owners = LANES // owned
    token_count = route.shape[0]
    operands = (
        tokens,
        mix_gain.reshape(1, -1),
        w_query,
        w_key,
        w_value,
        w_ogate,
        w_igate.T,
        w_fgate.T,
        forget_bias.reshape(1, -1),
        head_gain.reshape(1, -1),
        w_out,
        memory.reshape(rows, qk, dv),
        normalizer.reshape(rows, qk),
        running_max.T,
        ffn_gain.reshape(1, -1),
        route.T,
        w_gate[0],
        w_up[0],
        w_down[0],
    )
    shape = jax.ShapeDtypeStruct
    hbm = pl.BlockSpec(memory_space=pl.ANY)
    pack_width = LANES + qk
    parts, mid, tgt, pack, state = pl.pallas_call(
        functools.partial(kernel, sizes),
        out_shape=(
            shape((chips, owned // 2, LANES), BF16),
            shape((owned, token_count), BF16),
            shape((2, token_count), jnp.int32),
            shape((rows, pack_width), F32),
            shape((rows, qk, dv), F32),
        ),
        in_specs=[hbm] * len(operands),
        out_specs=(hbm,) * 5,
        scratch_shapes=[pltpu.VMEM(a.shape, a.dtype) for a in operands]
        + [
            pltpu.SemaphoreType.DMA((len(operands),)),
            pltpu.VMEM((2, token_count), jnp.int32),
            pltpu.VMEM((rows, pack_width), F32),
            pltpu.VMEM((2 * nc * CAP, token_count), BF16),
            pltpu.VMEM((nx, rows, quarter), BF16),
            pltpu.VMEM((nx - 1, rows, quarter), BF16),
            pltpu.VMEM((nc, 2, rows // 2, LANES), BF16),
            pltpu.VMEM((chips * nc, rows // 2, LANES), BF16),
            pltpu.VMEM((2 * nc, CAP // 2, LANES), BF16),
            pltpu.VMEM((groups, 2, CAP // 2, LANES), BF16),
            pltpu.VMEM((groups, CAP, LANES), BF16),
            pltpu.VMEM((groups, CAP, LANES), BF16),
            pltpu.VMEM((owners // 2, owned, token_count), BF16),
            pltpu.VMEM((owners, owned // 2, LANES), BF16),
            pltpu.SemaphoreType.DMA((2, nx - 1)),
            pltpu.SemaphoreType.DMA((2,)),
            pltpu.SemaphoreType.DMA((2, 2 * groups - 1)),
            pltpu.SemaphoreType.DMA((2, groups - 1)),
            pltpu.SemaphoreType.DMA((2,)),
            pltpu.SemaphoreType.DMA((2,)),
            pltpu.SemaphoreType.DMA((5,)),
            pltpu.SemaphoreType.REGULAR,
            pltpu.VMEM((rows, qk, dv), F32),
        ],
        compiler_params=pltpu.CompilerParams(collective_id=0, has_side_effects=True),
    )(*operands)
    mixed, state, new_norm, new_max = pl.pallas_call(
        combine,
        out_shape=(
            shape((owned, token_count), BF16),
            shape((rows, qk, dv), F32),
            shape((rows, qk), F32),
            shape((1, rows), F32),
        ),
        in_specs=[hbm] * 6,
        out_specs=(hbm,) * 4,
        scratch_shapes=[
            pltpu.VMEM((owned, token_count), BF16),
            pltpu.VMEM((rows, qk), F32),
            pltpu.VMEM((1, rows), F32),
            pltpu.VMEM((chips, owned // 2, LANES), BF16),
            pltpu.VMEM((owned, token_count), BF16),
            pltpu.VMEM((2, token_count), jnp.int32),
            pltpu.VMEM((2, token_count), F32),
            pltpu.VMEM((rows, pack_width), F32),
            pltpu.VMEM((rows, qk, dv), F32),
            pltpu.SemaphoreType.DMA((5,)),
            pltpu.SemaphoreType.DMA((rows,)),
            pltpu.SemaphoreType.DMA((rows + 3,)),
        ],
    )(parts, mid, tgt, route_weight.T, pack, state)
    return (mixed.T, state[:, None], new_norm[:, None], new_max.T)


def solution(mesh):
    nx = mesh.shape["tp"]
    nc = 2
    nz = nx * nc
    ny = mesh.shape["ep"] // (nc * nz)
    finer = Mesh(mesh.devices.reshape(nz, ny, nc, nx), ("z", "y", "c", "x"))
    ep = ("z", "y", "c")
    in_specs = (
        P(ep, None),
        P(),
        P(None, "x"),
        P(None, "x"),
        P(None, "x"),
        P(None, "x"),
        P(),
        P(),
        P(),
        P("x"),
        P("x", None),
        P(ep, "x", None, None),
        P(ep, "x", None),
        P(ep, "x"),
        P(),
        P(),
        P(),
        P(ep, None, "x"),
        P(ep, None, "x"),
        P(ep, "x", None),
    )
    out_specs = (P(None, ep), P(ep, "x", None, None), P(ep, "x", None), P(ep, "x"))
    return jax.shard_map(
        functools.partial(shards, (nz, ny, nc, nx)),
        mesh=finer,
        in_specs=in_specs,
        out_specs=out_specs,
        check_vma=False,
    )
```

```python
import functools

import jax
import jax.numpy as jnp
from jax import lax
from jax.experimental import pallas as pl
from jax.experimental.pallas import tpu as pltpu
from jax.sharding import Mesh
from jax.sharding import PartitionSpec as P

MESH = pl.DeviceIdType.MESH
CAP = 32
LANES = 128
EPS = 1e-06
F32 = jnp.float32
BF16 = jnp.bfloat16


def dot(a, b):
    return jnp.dot(a, b, preferred_element_type=F32)


def kernel(
    sizes,
    tok_h,
    mix_h,
    wq_h,
    wk_h,
    wv_h,
    wo_h,
    wi_h,
    wf_h,
    fb_h,
    hg_h,
    wout_h,
    mem_h,
    nrm_h,
    rmax_h,
    fg_h,
    route_h,
    wgate_h,
    wup_h,
    wdown_h,
    frecv,
    mrecv,
    tgt_ref,
    pack_ref,
    state_ref,
    tok,
    mix,
    wqk,
    wv,
    wo,
    wi,
    wf,
    fb,
    hg,
    wout,
    mem,
    nrm,
    rmax,
    fg,
    route,
    wgateup,
    wdown,
    load_sem,
    tgt,
    pack,
    place,
    psend,
    precv,
    csend,
    crecv,
    esend,
    erecv,
    rsend,
    rrecv,
    msend,
    dsend,
    psem,
    csem,
    esem,
    rsem,
    msem,
    dsem,
    out_sem,
    plane_sem,
    state,
):
    nz, ny, nc, nx = sizes
    z, y, c, x = (lax.axis_index(a) for a in ("z", "y", "c", "x"))
    zy = z * ny + y
    ep = zy * nc + c
    rows, width = tok.shape
    groups = nx * nc
    quarter = width // nx
    chips = nz * ny
    owned = width // (chips * nc)
    owners = LANES // owned
    group = x * nc + c
    side = y % 2
    first_y = y - side
    half_lanes = LANES // 2
    expert_count = chips * nc
    token_count = route.shape[1]

    qk = wqk.shape[1] // 2
    hidden = wgateup.shape[1] // 2
    pairs = {
        "tok": (tok_h, tok),
        "mix": (mix_h, mix),
        "wi": (wi_h, wi),
        "wf": (wf_h, wf),
        "fb": (fb_h, fb),
        "rmax": (rmax_h, rmax),
        "nrm": (nrm_h, nrm),
        "wq": (wq_h, wqk.at[:, 0:qk]),
        "wk": (wk_h, wqk.at[:, qk : 2 * qk]),
        "wv": (wv_h, wv),
        "wo": (wo_h, wo),
        "mem": (mem_h, mem),
        "hg": (hg_h, hg),
        "wout": (wout_h, wout),
        "route": (route_h, route),
        "fg": (fg_h, fg),
        "wgate": (wgate_h, wgateup.at[:, 0:hidden]),
        "wup": (wup_h, wgateup.at[:, hidden : 2 * hidden]),
        "wdown": (wdown_h, wdown),
    }
    loads = {
        n: pltpu.make_async_copy(h, v, load_sem.at[i]) for i, (n, (h, v)) in enumerate(pairs.items())
    }
    late = ("fg", "wgate", "wup", "wdown")
    for n in loads:
        if n not in late:
            loads[n].start()

    def ready(*names):
        for n in names:
            loads[n].wait()

    barrier = pltpu.get_barrier_semaphore()

    def greet(target):
        pl.semaphore_signal(barrier, inc=1, device_id=target, device_id_type=MESH)

    y_order = sorted(range(ny), key=lambda d: -min(d, ny - d))

    def ring_z(i):
        shift = nz // 2 + jnp.where(i % 2 == 0, i // 2, -((i + 1) // 2))
        return lax.rem(z + shift, nz)

    z_order = sorted(range(1, nz), key=lambda d: -min(d, nz - d))
    for dz in z_order:
        tz = lax.rem(z + dz, nz)
        for dc in range(nc):
            greet((tz, y, lax.rem(c + dc, nc), x))
    for dy in y_order[:-1]:
        greet((z, lax.rem(y + dy, ny), c, x))
    for dx in range(nx):
        for dc in range(nc):
            if dx + dc > 0:
                greet((z, y, lax.rem(c + dc, nc), lax.rem(x + dx, nx)))
    for dx in range(1, nx):
        for dc in range(nc):
            greet((z, y + 1 - 2 * side, lax.rem(c + dc, nc), lax.rem(x + dx, nx)))
    source_group = ep // owners
    from_self = source_group == group
    result_group = lax.rem(x + nx - lax.rem(z, nx), nx) * nc + c
    result_from_self = source_group == result_group

    ready("tok", "mix")
    tokens = tok[...].astype(F32)
    mean = jnp.mean(tokens * tokens, axis=1, keepdims=True)
    normed = (tokens * lax.rsqrt(mean + EPS) * mix[...]).astype(BF16)
    ready("wi", "wf", "fb", "rmax", "nrm", "wq", "wk")
    query_key = dot(normed, wqk[...]).astype(BF16)
    query16 = query_key[:, 0:qk]
    query = query16.astype(F32)
    scaled_key = query_key[:, qk : 2 * qk].astype(F32) * qk ** (-0.5)
    floats = normed.astype(F32)
    head_row = lax.broadcasted_iota(jnp.int32, wi.shape, 0) == x
    in_row = jnp.sum(jnp.where(head_row, wi[...].astype(F32), 0.0), axis=0, keepdims=True)
    forget_row = jnp.sum(jnp.where(head_row, wf[...].astype(F32), 0.0), axis=0, keepdims=True)
    log_in = jnp.sum(floats * in_row, axis=1, keepdims=True)
    head_lane = lax.broadcasted_iota(jnp.int32, fb.shape, 1) == x
    bias = jnp.sum(jnp.where(head_lane, fb[...], 0.0), axis=1, keepdims=True)
    forget_pre = jnp.sum(floats * forget_row, axis=1, keepdims=True) + bias
    log_forget = jnp.minimum(forget_pre, 0.0) - jnp.log1p(jnp.exp(-jnp.abs(forget_pre)))
    diagonal = lax.broadcasted_iota(jnp.int32, (rows, rows), 0) == lax.broadcasted_iota(
        jnp.int32, (rows, rows), 1
    )
    old_max = jnp.sum(
        jnp.where(diagonal, jnp.broadcast_to(rmax[...], (rows, rows)), 0.0), axis=1, keepdims=True
    )
    carried = log_forget + old_max
    new_max = jnp.maximum(carried, log_in)
    keep = jnp.exp(carried - new_max)
    admit = jnp.exp(log_in - new_max)
    akey = admit * scaled_key
    norm_state = keep * nrm[...] + akey
    pack[:, 0:qk] = norm_state
    pack[:, qk:] = jnp.broadcast_to(new_max, (rows, LANES))
    ready("mem", "hg", "wout")
    ready("wv", "wo")
    value = dot(normed, wv[...]).astype(BF16).astype(F32)
    ogate = dot(normed, wo[...]).astype(BF16).astype(F32)
    row_of = lax.broadcasted_iota(jnp.int32, value.shape, 0)
    kept = jnp.zeros_like(value)
    for t in range(rows):
        kept = jnp.where(row_of == t, dot(query16, mem[t].astype(BF16)), kept)
    numer = keep * kept + jnp.sum(query * akey, axis=1, keepdims=True) * value
    denom = jnp.sum(query * norm_state, axis=1, keepdims=True)
    read = numer / jnp.maximum(jnp.abs(denom), jnp.exp(-new_max))
    scale = lax.rsqrt(jnp.mean(read * read, axis=1, keepdims=True) + EPS)
    gated = (jax.nn.sigmoid(ogate) * read * scale * hg[...]).astype(BF16)
    partial = dot(gated, wout[...]).astype(BF16)
    for i in range(nx):
        psend[i] = partial[:, i * quarter : (i + 1) * quarter]
    pl.semaphore_wait(barrier, (nz - 1) * nc + ny - 1 + nx * nc - 1 + (nx - 1) * nc)

    for dy in y_order[:-1]:
        pl.semaphore_signal(
            plane_sem, inc=1, device_id=(z, lax.rem(y + dy, ny), c, x), device_id_type=MESH
        )

    x_order = sorted(range(nx), key=lambda d: -min(d, nx - d))
    for dx in x_order[:-1]:
        tx = lax.rem(x + dx, nx)
        pltpu.make_async_remote_copy(
            src_ref=psend.at[tx],
            dst_ref=precv.at[dx - 1],
            send_sem=psem.at[0, dx - 1],
            recv_sem=psem.at[1, dx - 1],
            device_id=(z, y, c, tx),
            device_id_type=MESH,
        ).start()

    for n in late:
        loads[n].start()
    ready("route")
    expert_of = lax.broadcasted_iota(jnp.int32, (expert_count, token_count), 0)
    named = [expert_of == route[j : j + 1, :] for j in range(2)]
    either = jnp.where(jnp.logical_or(named[0], named[1]), 1.0, 0.0)
    block = min(256, token_count)
    earlier = (
        lax.broadcasted_iota(jnp.int32, (block, block), 0)
        < lax.broadcasted_iota(jnp.int32, (block, block), 1)
    ).astype(F32).astype(BF16)
    carry = jnp.zeros((expert_count, 1), F32)
    before = []
    for b in range(token_count // block):
        part = either[:, b * block : (b + 1) * block]
        before.append(dot(part.astype(BF16), earlier) + carry)
        carry = carry + jnp.sum(part, axis=1, keepdims=True)
    before = jnp.concatenate(before, axis=1)
    for j in range(2):
        slot = jnp.sum(jnp.where(named[j], before, 0.0), axis=0, keepdims=True)
        tgt[j : j + 1, :] = route[j : j + 1, :] * CAP + slot.astype(jnp.int32)
    slots_here = nc * CAP
    slots_both = 2 * slots_here
    first_slot = (z * ny + first_y) * slots_here
    slot_id = lax.broadcasted_iota(jnp.int32, (slots_both, token_count), 0) + first_slot
    hit = jnp.logical_or(slot_id == tgt[0:1, :], slot_id == tgt[1:2, :])
    place[...] = jnp.where(hit, 1.0, 0.0).astype(BF16)
    keeps = [
        pltpu.make_async_copy(tgt, tgt_ref, out_sem.at[0]),
        pltpu.make_async_copy(pack, pack_ref, out_sem.at[1]),
    ]
    for copy in keeps:
        copy.start()

    total = psend[x].astype(F32)
    for dx in range(1, nx):
        copy = pltpu.make_async_remote_copy(
            src_ref=psend.at[0],
            dst_ref=precv.at[dx - 1],
            send_sem=psem.at[0, dx - 1],
            recv_sem=psem.at[1, dx - 1],
            device_id=(z, y, c, lax.rem(x + dx, nx)),
            device_id_type=MESH,
        )
        copy.wait_recv()
        total = total + precv[dx - 1].astype(F32)
    own = tok[:, pl.ds(pl.multiple_of(x * quarter, quarter), quarter)].astype(F32)
    middle = (own + total).astype(BF16).astype(F32)
    token_half = rows // 2
    low_rows = lax.broadcasted_iota(jnp.int32, (token_half, LANES), 1) < half_lanes
    for i in range(nc):
        tile = middle[:, i * LANES : (i + 1) * LANES]
        turned = pltpu.roll(tile, half_lanes, 1)
        csend[i, 0] = jnp.where(low_rows, tile[:token_half], turned[token_half:]).astype(BF16)
        csend[i, 1] = jnp.where(low_rows, turned[:token_half], tile[token_half:]).astype(BF16)

    def send_plane(i, carry):
        tz = ring_z(i)

        def send(ty, tc):
            pltpu.make_async_remote_copy(
                src_ref=csend.at[tc, ty % 2],
                dst_ref=crecv.at[ep],
                send_sem=csem.at[0],
                recv_sem=csem.at[1],
                device_id=(tz, ty, tc, x),
                device_id_type=MESH,
            ).start()

        for dy in y_order:
            ty = lax.rem(y + dy, ny)
            for dc in reversed(range(nc)):
                tc = lax.rem(c + dc, nc)
                if dy == 0 and dc == 0:

                    @pl.when(i < nz - 1)
                    def _():
                        send(ty, tc)
                else:
                    send(ty, tc)
        return carry

    pl.semaphore_wait(plane_sem, ny - 1)
    lax.fori_loop(0, nz, send_plane, 0)
    crecv[ep] = csend[c, side]

    for t in range(rows):
        key_columns = jnp.broadcast_to(akey[t : t + 1, :], (LANES, LANES)).T
        key_columns = jnp.concatenate([key_columns] * (wv.shape[1] // LANES), axis=1)
        state[t] = keep[t : t + 1, :] * mem[t] + key_columns * value[t : t + 1, :]
    keeps.append(pltpu.make_async_copy(state, state_ref, out_sem.at[4]))
    keeps[-1].start()
    others = crecv.at[pl.ds(0, chips * nc - 1)]
    plane = pltpu.make_async_remote_copy(
        src_ref=others,
        dst_ref=others,
        send_sem=csem.at[0],
        recv_sem=csem.at[1],
        device_id=(z, y, lax.rem(c + 1, nc), x),
        device_id_type=MESH,
    )
    plane.wait_recv()
    packed = crecv[...].astype(F32)
    everyone32 = jnp.concatenate([packed, pltpu.roll(packed, half_lanes, 2)], axis=1)
    everyone32 = everyone32.reshape(token_count, LANES)
    slots = dot(place[...], everyone32.astype(BF16))
    half_cap = CAP // 2
    low_slots = lax.broadcasted_iota(jnp.int32, (half_cap, LANES), 1) < half_lanes
    for i in range(2 * nc):
        upper = slots[i * CAP : i * CAP + half_cap]
        lower = slots[i * CAP + half_cap : (i + 1) * CAP]
        esend[i] = jnp.where(low_slots, upper, pltpu.roll(lower, half_lanes, 1)).astype(BF16)

    def chip_row(send, recv, sem, src_of, dst):
        copies = []
        for dx in x_order:
            for dc in reversed(range(nc)):
                if dx == 0 and dc == 0:
                    continue
                tx, tc = lax.rem(x + dx, nx), lax.rem(c + dc, nc)
                n = dx * nc + dc - 1
                copy = pltpu.make_async_remote_copy(
                    src_ref=send.at[src_of(tx, tc)],
                    dst_ref=recv.at[dst],
                    send_sem=sem.at[0, n],
                    recv_sem=sem.at[1, n],
                    device_id=(z, y, tc, tx),
                    device_id_type=MESH,
                )
                copy.start()
                copies.append(copy)
        return copies

    to_experts = []
    for dx in x_order:
        for dy in (1, 0):
            for dc in reversed(range(nc)):
                if dx + dy + dc > 0:
                    tx, tc = lax.rem(x + dx, nx), lax.rem(c + dc, nc)
                    there = side if dy == 0 else 1 - side
                    copy = pltpu.make_async_remote_copy(
                        src_ref=esend.at[there * nc + tc],
                        dst_ref=erecv.at[group, side],
                        send_sem=esem.at[0, len(to_experts)],
                        recv_sem=esem.at[1, len(to_experts)],
                        device_id=(z, first_y + there, tc, tx),
                        device_id_type=MESH,
                    )
                    copy.start()
                    to_experts.append(copy)
    erecv[group, side] = esend[side * nc + c]

    serves = jnp.logical_and(from_self, y // (ny // 2) == side)
    own_half = lax.rem(y, ny // 2) * nc + c

    @pl.when(serves)
    def _():
        turned = everyone32.T
        for k in range(owners // 2):
            msend[k] = turned[k * owned : (k + 1) * owned, :].astype(BF16)
        pltpu.make_async_copy(msend.at[own_half], mrecv, out_sem.at[2]).start()

    ready(*late)
    for copy in to_experts:
        copy.wait_recv()
    stacked = []
    for i in range(groups):
        left, right = erecv[i, 0].astype(F32), erecv[i, 1].astype(F32)
        left_turned = pltpu.roll(left, half_lanes, 1)
        right_turned = pltpu.roll(right, half_lanes, 1)
        tile = [jnp.where(low_slots, left, right_turned), jnp.where(low_slots, left_turned, right)]
        stacked.append(jnp.concatenate(tile, axis=0))
    stacked = jnp.concatenate(stacked, axis=1)
    scale = lax.rsqrt(jnp.mean(stacked * stacked, axis=1, keepdims=True) + EPS)
    gate_up = dot((stacked * fg[...]).astype(BF16), wgateup[...]) * scale
    gate_v, up_v = gate_up[:, 0:hidden], gate_up[:, hidden : 2 * hidden]
    act = (gate_v * jax.nn.sigmoid(gate_v) * up_v).astype(BF16)
    down = dot(act, wdown[...]).astype(BF16)
    for i in range(groups):
        rsend[i] = down[:, i * LANES : (i + 1) * LANES]

    def result_of(tx, tc):
        return lax.rem(tx + nx - lax.rem(z, nx), nx) * nc + tc

    to_groups = chip_row(rsend, rrecv, rsem, result_of, group)
    rrecv[group] = rsend[result_group]

    middle_copies = []
    for dx in x_order:
        for dy in (1, 0):
            for dc in reversed(range(nc)):
                if dx + dy + dc > 0:
                    tx, tc = lax.rem(x + dx, nx), lax.rem(c + dc, nc)
                    ty = y if dy == 0 else y + 1 - 2 * side
                    copy = pltpu.make_async_remote_copy(
                        src_ref=msend.at[lax.rem(ty, ny // 2) * nc + tc],
                        dst_ref=mrecv,
                        send_sem=msem.at[0],
                        recv_sem=msem.at[1],
                        device_id=(z, ty, tc, tx),
                        device_id_type=MESH,
                    )
                    middle_copies.append(copy)

    @pl.when(serves)
    def _():
        for copy in middle_copies:
            copy.start()

    for copy in to_groups:
        copy.wait_recv()
    results = []
    for i in range(nc):
        result = rrecv[i].astype(F32)
        for j in range(1, nx):
            result = result + rrecv[j * nc + i].astype(F32)
        results.append(result)
    low = lax.broadcasted_iota(jnp.int32, (owners, owned // 2, LANES), 2) < slots_here
    turned = jnp.concatenate(results + results, axis=0).T.reshape(owners, owned, LANES)
    half = owned // 2
    dsend[...] = jnp.where(low, turned[:, :half], turned[:, half:]).astype(BF16)

    def send_owners(i, carry):
        shift = ny // 2 + jnp.where(i % 2 == 0, i // 2, -((i + 1) // 2))
        ty = lax.rem(y + shift, ny)

        def send(tc, tx):
            pltpu.make_async_remote_copy(
                src_ref=dsend.at[ty * nc + tc],
                dst_ref=frecv.at[zy],
                send_sem=dsem.at[0],
                recv_sem=dsem.at[1],
                device_id=(result_group, ty, tc, tx),
                device_id_type=MESH,
            ).start()

        for dx in x_order:
            tx = lax.rem(x + dx, nx)
            for dc in reversed(range(nc)):
                tc = lax.rem(c + dc, nc)
                if dx == 0 and dc == 0:

                    @pl.when(jnp.logical_not(jnp.logical_and(result_from_self, i == ny - 1)))
                    def _():
                        send(tc, tx)
                else:
                    send(tc, tx)
        return carry

    lax.fori_loop(0, ny, send_owners, 0)

    def arrivals(n):
        part = frecv.at[pl.ds(0, n)]
        return pltpu.make_async_remote_copy(
            src_ref=part,
            dst_ref=part,
            send_sem=dsem.at[0],
            recv_sem=dsem.at[1],
            device_id=(z, y, lax.rem(c + 1, nc), x),
            device_id_type=MESH,
        )

    @pl.when(result_from_self)
    def _():
        own = pltpu.make_async_copy(dsend.at[lax.rem(ep, owners)], frecv.at[zy], out_sem.at[3])
        own.start()
        arrivals(chips - 1).wait_recv()
        own.wait()

    @pl.when(jnp.logical_not(result_from_self))
    def _():
        arrivals(chips).wait_recv()

    @pl.when(serves)
    def _():
        pltpu.make_async_copy(msend.at[own_half], mrecv, out_sem.at[2]).wait()

    @pl.when(jnp.logical_not(serves))
    def _():
        middle_copies[0].wait_recv()

    for copy in keeps:
        copy.wait()

    for dx in range(1, nx):
        pltpu.make_async_remote_copy(
            src_ref=psend.at[0],
            dst_ref=precv.at[dx - 1],
            send_sem=psem.at[0, dx - 1],
            recv_sem=psem.at[1, dx - 1],
            device_id=(z, y, c, lax.rem(x + dx, nx)),
            device_id_type=MESH,
        ).wait_send()
    plane.wait_send()
    for copy in to_experts + to_groups:
        copy.wait_send()

    @pl.when(result_from_self)
    def _():
        arrivals(chips - 1).wait_send()

    @pl.when(jnp.logical_not(result_from_self))
    def _():
        arrivals(chips).wait_send()

    @pl.when(serves)
    def _():
        for copy in middle_copies:
            copy.wait_send()


def lane_of(name):
    return jnp.bitwise_and(name, LANES - 1).astype(F32).astype(BF16)


def combine(
    parts_h,
    mid_h,
    tgt_h,
    rw_h,
    pack_h,
    state_h,
    mixed_h,
    newmem_h,
    newnorm_h,
    newmax_h,
    mixed,
    newnorm,
    newmax,
    parts,
    mid,
    tgt,
    rw,
    pack,
    state,
    load_sem,
    state_sem,
    sem,
):
    rows, qk, dv = state.shape
    chips, half, _ = parts.shape
    owned = 2 * half
    token_count = tgt.shape[1]
    loads = []
    for i, (h, v) in enumerate(
        ((pack_h, pack), (parts_h, parts), (tgt_h, tgt), (mid_h, mid), (rw_h, rw))
    ):
        loads.append(pltpu.make_async_copy(h, v, load_sem.at[i]))
    moves = [pltpu.make_async_copy(state_h.at[t], state.at[t], state_sem.at[t]) for t in range(rows)]
    for copy in loads + moves:
        copy.start()
    for copy in loads:
        copy.wait()
    newnorm[...] = pack[:, 0:qk]
    diagonal = lax.broadcasted_iota(jnp.int32, (rows, LANES), 0) == lax.broadcasted_iota(
        jnp.int32, (rows, LANES), 1
    )
    newmax[...] = jnp.sum(jnp.where(diagonal, pack[:, qk:], 0.0), axis=0, keepdims=True)[:, :rows]
    copies = []

    low = lax.broadcasted_iota(jnp.int32, (chips // 2, half, LANES), 2) < LANES // 2
    both = parts[...].astype(F32).reshape(chips // 2, 2, half, LANES)
    even, odd = both[:, 0], both[:, 1]
    even_turned = pltpu.roll(even, LANES // 2, 2)
    odd_turned = pltpu.roll(odd, LANES // 2, 2)
    held = jnp.concatenate(
        [jnp.where(low, even, odd_turned), jnp.where(low, even_turned, odd)], axis=1
    )
    held = held.reshape(chips // 2 * owned, LANES).astype(BF16)
    lane_id = lax.broadcasted_iota(jnp.int32, (LANES, LANES), 0).astype(F32).astype(BF16)
    for k in range(token_count // LANES):
        if k == min(2, token_count // LANES - 1):
            for t in range(rows):
                moves[t].wait()
                copy = pltpu.make_async_copy(state.at[t], newmem_h.at[t], sem.at[t])
                copy.start()
                copies.append(copy)
        span = slice(k * LANES, (k + 1) * LANES)
        names = [tgt[j : j + 1, span] for j in range(2)]
        picks = jnp.concatenate(
            [
                jnp.where(lane_id == lane_of(n), jnp.ones((), BF16), jnp.zeros((), BF16))
                for n in names
            ],
            axis=1,
        )
        found = dot(held, picks)
        total = []
        for j in range(2):
            place = jnp.broadcast_to(lax.shift_right_logical(names[j], 7), (owned, LANES))
            got = jnp.zeros((owned, LANES), F32)
            for p in range(chips // 2):
                part = found[p * owned : (p + 1) * owned, j * LANES : (j + 1) * LANES]
                got = jnp.where(place == p, part, got)
            total.append(got)
        w0, w1 = rw[0:1, span], rw[1:2, span]
        weighed = total[0] * (w0 / (w0 + w1)) + total[1] * (w1 / (w0 + w1))
        mixed[:, span] = (mid[:, span].astype(F32) + weighed).astype(BF16)
    outs = ((mixed, mixed_h), (newnorm, newnorm_h), (newmax, newmax_h))
    for i, (v, h) in enumerate(outs):
        copy = pltpu.make_async_copy(v, h, sem.at[rows + i])
        copy.start()
        copies.append(copy)
    for copy in copies:
        copy.wait()


def shards(
    sizes,
    tokens,
    mix_gain,
    w_query,
    w_key,
    w_value,
    w_ogate,
    w_igate,
    w_fgate,
    forget_bias,
    head_gain,
    w_out,
    memory,
    normalizer,
    running_max,
    ffn_gain,
    route,
    route_weight,
    w_gate,
    w_up,
    w_down,
):
    nz, ny, nc, nx = sizes
    rows, width = tokens.shape
    qk, dv = memory.shape[2:]
    chips = nz * ny
    quarter = width // nx
    groups = nx * nc
    owned = width // (chips * nc)
    owners = LANES // owned
    token_count = route.shape[0]
    operands = (
        tokens,
        mix_gain.reshape(1, -1),
        w_query,
        w_key,
        w_value,
        w_ogate,
        w_igate.T,
        w_fgate.T,
        forget_bias.reshape(1, -1),
        head_gain.reshape(1, -1),
        w_out,
        memory.reshape(rows, qk, dv),
        normalizer.reshape(rows, qk),
        running_max.T,
        ffn_gain.reshape(1, -1),
        route.T,
        w_gate[0],
        w_up[0],
        w_down[0],
    )
    shape = jax.ShapeDtypeStruct
    hbm = pl.BlockSpec(memory_space=pl.ANY)
    pack_width = LANES + qk
    held = [pltpu.VMEM(a.shape, a.dtype) for a in operands]
    held[2] = pltpu.VMEM((width, 2 * qk), BF16)
    held[16] = pltpu.VMEM((width, 2 * w_gate.shape[2]), BF16)
    del held[17], held[3]
    parts, mid, tgt, pack, state = pl.pallas_call(
        functools.partial(kernel, sizes),
        out_shape=(
            shape((chips, owned // 2, LANES), BF16),
            shape((owned, token_count), BF16),
            shape((2, token_count), jnp.int32),
            shape((rows, pack_width), F32),
            shape((rows, qk, dv), F32),
        ),
        in_specs=[hbm] * len(operands),
        out_specs=(hbm,) * 5,
        scratch_shapes=held
        + [
            pltpu.SemaphoreType.DMA((len(operands),)),
            pltpu.VMEM((2, token_count), jnp.int32),
            pltpu.VMEM((rows, pack_width), F32),
            pltpu.VMEM((2 * nc * CAP, token_count), BF16),
            pltpu.VMEM((nx, rows, quarter), BF16),
            pltpu.VMEM((nx - 1, rows, quarter), BF16),
            pltpu.VMEM((nc, 2, rows // 2, LANES), BF16),
            pltpu.VMEM((chips * nc, rows // 2, LANES), BF16),
            pltpu.VMEM((2 * nc, CAP // 2, LANES), BF16),
            pltpu.VMEM((groups, 2, CAP // 2, LANES), BF16),
            pltpu.VMEM((groups, CAP, LANES), BF16),
            pltpu.VMEM((groups, CAP, LANES), BF16),
            pltpu.VMEM((owners // 2, owned, token_count), BF16),
            pltpu.VMEM((owners, owned // 2, LANES), BF16),
            pltpu.SemaphoreType.DMA((2, nx - 1)),
            pltpu.SemaphoreType.DMA((2,)),
            pltpu.SemaphoreType.DMA((2, 2 * groups - 1)),
            pltpu.SemaphoreType.DMA((2, groups - 1)),
            pltpu.SemaphoreType.DMA((2,)),
            pltpu.SemaphoreType.DMA((2,)),
            pltpu.SemaphoreType.DMA((5,)),
            pltpu.SemaphoreType.REGULAR,
            pltpu.VMEM((rows, qk, dv), F32),
        ],
        compiler_params=pltpu.CompilerParams(collective_id=0, has_side_effects=True),
    )(*operands)
    mixed, state, new_norm, new_max = pl.pallas_call(
        combine,
        out_shape=(
            shape((owned, token_count), BF16),
            shape((rows, qk, dv), F32),
            shape((rows, qk), F32),
            shape((1, rows), F32),
        ),
        in_specs=[hbm] * 6,
        out_specs=(hbm,) * 4,
        scratch_shapes=[
            pltpu.VMEM((owned, token_count), BF16),
            pltpu.VMEM((rows, qk), F32),
            pltpu.VMEM((1, rows), F32),
            pltpu.VMEM((chips, owned // 2, LANES), BF16),
            pltpu.VMEM((owned, token_count), BF16),
            pltpu.VMEM((2, token_count), jnp.int32),
            pltpu.VMEM((2, token_count), F32),
            pltpu.VMEM((rows, pack_width), F32),
            pltpu.VMEM((rows, qk, dv), F32),
            pltpu.SemaphoreType.DMA((5,)),
            pltpu.SemaphoreType.DMA((rows,)),
            pltpu.SemaphoreType.DMA((rows + 3,)),
        ],
    )(parts, mid, tgt, route_weight.T, pack, state)
    return (mixed.T, state[:, None], new_norm[:, None], new_max.T)


def solution(mesh):
    nx = mesh.shape["tp"]
    nc = 2
    nz = nx * nc
    ny = mesh.shape["ep"] // (nc * nz)
    finer = Mesh(mesh.devices.reshape(nz, ny, nc, nx), ("z", "y", "c", "x"))
    ep = ("z", "y", "c")
    in_specs = (
        P(ep, None),
        P(),
        P(None, "x"),
        P(None, "x"),
        P(None, "x"),
        P(None, "x"),
        P(),
        P(),
        P(),
        P("x"),
        P("x", None),
        P(ep, "x", None, None),
        P(ep, "x", None),
        P(ep, "x"),
        P(),
        P(),
        P(),
        P(ep, None, "x"),
        P(ep, None, "x"),
        P(ep, "x", None),
    )
    out_specs = (P(None, ep), P(ep, "x", None, None), P(ep, "x", None), P(ep, "x"))
    return jax.shard_map(
        functools.partial(shards, (nz, ny, nc, nx)),
        mesh=finer,
        in_specs=in_specs,
        out_specs=out_specs,
        check_vma=False,
    )
```

```python
import functools

import jax
import jax.numpy as jnp
from jax import lax
from jax.experimental import pallas as pl
from jax.experimental.pallas import tpu as pltpu
from jax.sharding import Mesh
from jax.sharding import PartitionSpec as P

MESH = pl.DeviceIdType.MESH
CAP = 32
LANES = 128
EPS = 1e-06
F32 = jnp.float32
BF16 = jnp.bfloat16


def dot(a, b):
    return jnp.dot(a, b, preferred_element_type=F32)


def kernel(
    sizes,
    tok_h,
    mix_h,
    wq_h,
    wk_h,
    wv_h,
    wo_h,
    wi_h,
    wf_h,
    fb_h,
    hg_h,
    wout_h,
    mem_h,
    nrm_h,
    rmax_h,
    fg_h,
    route_h,
    wgate_h,
    wup_h,
    wdown_h,
    frecv,
    mrecv,
    tgt_ref,
    pack_ref,
    state_ref,
    tok,
    mix,
    wqk,
    wv,
    wo,
    wi,
    wf,
    fb,
    hg,
    wout,
    mem,
    nrm,
    rmax,
    fg,
    route,
    wgateup,
    wdown,
    load_sem,
    tgt,
    pack,
    place,
    psend,
    precv,
    csend,
    crecv,
    esend,
    erecv,
    rsend,
    rrecv,
    msend,
    dsend,
    psem,
    csem,
    esem,
    rsem,
    msem,
    dsem,
    out_sem,
    plane_sem,
    state,
):
    nz, ny, nc, nx = sizes
    z, y, c, x = (lax.axis_index(a) for a in ("z", "y", "c", "x"))
    zy = z * ny + y
    ep = zy * nc + c
    rows, width = tok.shape
    groups = nx * nc
    quarter = width // nx
    chips = nz * ny
    owned = width // (chips * nc)
    owners = LANES // owned
    group = x * nc + c
    side = y % 2
    first_y = y - side
    half_lanes = LANES // 2
    expert_count = chips * nc
    token_count = route.shape[1]

    qk = wqk.shape[1] // 2
    hidden = wgateup.shape[1] // 2
    pairs = {
        "tok": (tok_h, tok),
        "mix": (mix_h, mix),
        "wi": (wi_h, wi),
        "wf": (wf_h, wf),
        "fb": (fb_h, fb),
        "rmax": (rmax_h, rmax),
        "nrm": (nrm_h, nrm),
        "wq": (wq_h, wqk.at[:, 0:qk]),
        "wk": (wk_h, wqk.at[:, qk : 2 * qk]),
        "wv": (wv_h, wv),
        "wo": (wo_h, wo),
        "mem": (mem_h, mem),
        "hg": (hg_h, hg),
        "wout": (wout_h, wout),
        "route": (route_h, route),
        "fg": (fg_h, fg),
        "wgate": (wgate_h, wgateup.at[:, 0:hidden]),
        "wup": (wup_h, wgateup.at[:, hidden : 2 * hidden]),
        "wdown": (wdown_h, wdown),
    }
    loads = {
        n: pltpu.make_async_copy(h, v, load_sem.at[i]) for i, (n, (h, v)) in enumerate(pairs.items())
    }
    late = ("fg", "wgate", "wup", "wdown")
    for n in loads:
        if n not in late:
            loads[n].start()

    def ready(*names):
        for n in names:
            loads[n].wait()

    barrier = pltpu.get_barrier_semaphore()

    def greet(target):
        pl.semaphore_signal(barrier, inc=1, device_id=target, device_id_type=MESH)

    y_order = sorted(range(ny), key=lambda d: -min(d, ny - d))

    def ring_z(i):
        shift = nz // 2 + jnp.where(i % 2 == 0, i // 2, -((i + 1) // 2))
        return lax.rem(z + shift, nz)

    z_order = sorted(range(1, nz), key=lambda d: -min(d, nz - d))
    for dz in z_order:
        tz = lax.rem(z + dz, nz)
        for dc in range(nc):
            greet((tz, y, lax.rem(c + dc, nc), x))
    for dy in y_order[:-1]:
        greet((z, lax.rem(y + dy, ny), c, x))
    for dx in range(nx):
        for dc in range(nc):
            if dx + dc > 0:
                greet((z, y, lax.rem(c + dc, nc), lax.rem(x + dx, nx)))
    for dx in range(1, nx):
        for dc in range(nc):
            greet((z, y + 1 - 2 * side, lax.rem(c + dc, nc), lax.rem(x + dx, nx)))
    source_group = ep // owners
    from_self = source_group == group
    result_group = lax.rem(x + nx - lax.rem(z, nx), nx) * nc + c
    result_from_self = source_group == result_group

    ready("tok", "mix")
    tokens = tok[...].astype(F32)
    mean = jnp.mean(tokens * tokens, axis=1, keepdims=True)
    normed = (tokens * lax.rsqrt(mean + EPS) * mix[...]).astype(BF16)
    ready("wi", "wf", "fb", "rmax", "nrm", "wq", "wk")
    query_key = dot(normed, wqk[...]).astype(BF16)
    query16 = query_key[:, 0:qk]
    query = query16.astype(F32)
    scaled_key = query_key[:, qk : 2 * qk].astype(F32) * qk ** (-0.5)
    floats = normed.astype(F32)
    head_row = lax.broadcasted_iota(jnp.int32, wi.shape, 0) == x
    in_row = jnp.sum(jnp.where(head_row, wi[...].astype(F32), 0.0), axis=0, keepdims=True)
    forget_row = jnp.sum(jnp.where(head_row, wf[...].astype(F32), 0.0), axis=0, keepdims=True)
    log_in = jnp.sum(floats * in_row, axis=1, keepdims=True)
    head_lane = lax.broadcasted_iota(jnp.int32, fb.shape, 1) == x
    bias = jnp.sum(jnp.where(head_lane, fb[...], 0.0), axis=1, keepdims=True)
    forget_pre = jnp.sum(floats * forget_row, axis=1, keepdims=True) + bias
    log_forget = jnp.minimum(forget_pre, 0.0) - jnp.log1p(jnp.exp(-jnp.abs(forget_pre)))
    diagonal = lax.broadcasted_iota(jnp.int32, (rows, rows), 0) == lax.broadcasted_iota(
        jnp.int32, (rows, rows), 1
    )
    old_max = jnp.sum(
        jnp.where(diagonal, jnp.broadcast_to(rmax[...], (rows, rows)), 0.0), axis=1, keepdims=True
    )
    carried = log_forget + old_max
    new_max = jnp.maximum(carried, log_in)
    keep = jnp.exp(carried - new_max)
    admit = jnp.exp(log_in - new_max)
    akey = admit * scaled_key
    norm_state = keep * nrm[...] + akey
    pack[:, 0:qk] = norm_state
    pack[:, qk:] = jnp.broadcast_to(new_max, (rows, LANES))
    ready("mem", "hg", "wout")
    ready("wv", "wo")
    value = dot(normed, wv[...]).astype(BF16).astype(F32)
    ogate = dot(normed, wo[...]).astype(BF16).astype(F32)
    row_of = lax.broadcasted_iota(jnp.int32, value.shape, 0)
    kept = jnp.zeros_like(value)
    for t in range(rows):
        kept = jnp.where(row_of == t, dot(query16, mem[t].astype(BF16)), kept)
    pl.semaphore_wait(barrier, (nz - 1) * nc + ny - 1 + nx * nc - 1 + (nx - 1) * nc)

    for dy in y_order[:-1]:
        pl.semaphore_signal(
            plane_sem, inc=1, device_id=(z, lax.rem(y + dy, ny), c, x), device_id_type=MESH
        )
    numer = keep * kept + jnp.sum(query * akey, axis=1, keepdims=True) * value
    denom = jnp.sum(query * norm_state, axis=1, keepdims=True)
    read = numer / jnp.maximum(jnp.abs(denom), jnp.exp(-new_max))
    scale = lax.rsqrt(jnp.mean(read * read, axis=1, keepdims=True) + EPS)
    gated = (jax.nn.sigmoid(ogate) * read * scale * hg[...]).astype(BF16)
    partial = dot(gated, wout[...]).astype(BF16)
    for i in range(nx):
        psend[i] = partial[:, i * quarter : (i + 1) * quarter]
    x_order = sorted(range(nx), key=lambda d: -min(d, nx - d))
    for dx in x_order[:-1]:
        tx = lax.rem(x + dx, nx)
        pltpu.make_async_remote_copy(
            src_ref=psend.at[tx],
            dst_ref=precv.at[dx - 1],
            send_sem=psem.at[0, dx - 1],
            recv_sem=psem.at[1, dx - 1],
            device_id=(z, y, c, tx),
            device_id_type=MESH,
        ).start()

    for n in late:
        loads[n].start()
    ready("route")
    expert_of = lax.broadcasted_iota(jnp.int32, (expert_count, token_count), 0)
    named = [expert_of == route[j : j + 1, :] for j in range(2)]
    either = jnp.where(jnp.logical_or(named[0], named[1]), 1.0, 0.0)
    block = min(256, token_count)
    earlier = (
        lax.broadcasted_iota(jnp.int32, (block, block), 0)
        < lax.broadcasted_iota(jnp.int32, (block, block), 1)
    ).astype(F32).astype(BF16)
    carry = jnp.zeros((expert_count, 1), F32)
    before = []
    for b in range(token_count // block):
        part = either[:, b * block : (b + 1) * block]
        before.append(dot(part.astype(BF16), earlier) + carry)
        carry = carry + jnp.sum(part, axis=1, keepdims=True)
    before = jnp.concatenate(before, axis=1)
    for j in range(2):
        slot = jnp.sum(jnp.where(named[j], before, 0.0), axis=0, keepdims=True)
        tgt[j : j + 1, :] = route[j : j + 1, :] * CAP + slot.astype(jnp.int32)
    slots_here = nc * CAP
    slots_both = 2 * slots_here
    first_slot = (z * ny + first_y) * slots_here
    slot_id = lax.broadcasted_iota(jnp.int32, (slots_both, token_count), 0) + first_slot
    hit = jnp.logical_or(slot_id == tgt[0:1, :], slot_id == tgt[1:2, :])
    place[...] = jnp.where(hit, 1.0, 0.0).astype(BF16)
    keeps = [
        pltpu.make_async_copy(tgt, tgt_ref, out_sem.at[0]),
        pltpu.make_async_copy(pack, pack_ref, out_sem.at[1]),
    ]
    for copy in keeps:
        copy.start()

    total = psend[x].astype(F32)
    for dx in range(1, nx):
        copy = pltpu.make_async_remote_copy(
            src_ref=psend.at[0],
            dst_ref=precv.at[dx - 1],
            send_sem=psem.at[0, dx - 1],
            recv_sem=psem.at[1, dx - 1],
            device_id=(z, y, c, lax.rem(x + dx, nx)),
            device_id_type=MESH,
        )
        copy.wait_recv()
        total = total + precv[dx - 1].astype(F32)
    own = tok[:, pl.ds(pl.multiple_of(x * quarter, quarter), quarter)].astype(F32)
    middle = (own + total).astype(BF16).astype(F32)
    token_half = rows // 2
    low_rows = lax.broadcasted_iota(jnp.int32, (token_half, LANES), 1) < half_lanes
    for i in range(nc):
        tile = middle[:, i * LANES : (i + 1) * LANES]
        turned = pltpu.roll(tile, half_lanes, 1)
        csend[i, 0] = jnp.where(low_rows, tile[:token_half], turned[token_half:]).astype(BF16)
        csend[i, 1] = jnp.where(low_rows, turned[:token_half], tile[token_half:]).astype(BF16)

    def send_plane(i, carry):
        tz = ring_z(i)

        def send(ty, tc):
            pltpu.make_async_remote_copy(
                src_ref=csend.at[tc, ty % 2],
                dst_ref=crecv.at[ep],
                send_sem=csem.at[0],
                recv_sem=csem.at[1],
                device_id=(tz, ty, tc, x),
                device_id_type=MESH,
            ).start()

        for dy in y_order:
            ty = lax.rem(y + dy, ny)
            for dc in reversed(range(nc)):
                tc = lax.rem(c + dc, nc)
                if dy == 0 and dc == 0:

                    @pl.when(i < nz - 1)
                    def _():
                        send(ty, tc)
                else:
                    send(ty, tc)
        return carry

    pl.semaphore_wait(plane_sem, ny - 1)
    lax.fori_loop(0, nz, send_plane, 0)
    crecv[ep] = csend[c, side]

    for t in range(rows):
        key_columns = jnp.broadcast_to(akey[t : t + 1, :], (LANES, LANES)).T
        key_columns = jnp.concatenate([key_columns] * (wv.shape[1] // LANES), axis=1)
        state[t] = keep[t : t + 1, :] * mem[t] + key_columns * value[t : t + 1, :]
    keeps.append(pltpu.make_async_copy(state, state_ref, out_sem.at[4]))
    keeps[-1].start()
    others = crecv.at[pl.ds(0, chips * nc - 1)]
    plane = pltpu.make_async_remote_copy(
        src_ref=others,
        dst_ref=others,
        send_sem=csem.at[0],
        recv_sem=csem.at[1],
        device_id=(z, y, lax.rem(c + 1, nc), x),
        device_id_type=MESH,
    )
    plane.wait_recv()
    packed = crecv[...].astype(F32)
    everyone32 = jnp.concatenate([packed, pltpu.roll(packed, half_lanes, 2)], axis=1)
    everyone32 = everyone32.reshape(token_count, LANES)
    slots = dot(place[...], everyone32.astype(BF16))
    half_cap = CAP // 2
    low_slots = lax.broadcasted_iota(jnp.int32, (half_cap, LANES), 1) < half_lanes
    for i in range(2 * nc):
        upper = slots[i * CAP : i * CAP + half_cap]
        lower = slots[i * CAP + half_cap : (i + 1) * CAP]
        esend[i] = jnp.where(low_slots, upper, pltpu.roll(lower, half_lanes, 1)).astype(BF16)

    def chip_row(send, recv, sem, src_of, dst):
        copies = []
        for dx in x_order:
            for dc in reversed(range(nc)):
                if dx == 0 and dc == 0:
                    continue
                tx, tc = lax.rem(x + dx, nx), lax.rem(c + dc, nc)
                n = dx * nc + dc - 1
                copy = pltpu.make_async_remote_copy(
                    src_ref=send.at[src_of(tx, tc)],
                    dst_ref=recv.at[dst],
                    send_sem=sem.at[0, n],
                    recv_sem=sem.at[1, n],
                    device_id=(z, y, tc, tx),
                    device_id_type=MESH,
                )
                copy.start()
                copies.append(copy)
        return copies

    to_experts = []
    for dx in x_order:
        for dy in (1, 0):
            for dc in reversed(range(nc)):
                if dx + dy + dc > 0:
                    tx, tc = lax.rem(x + dx, nx), lax.rem(c + dc, nc)
                    there = side if dy == 0 else 1 - side
                    copy = pltpu.make_async_remote_copy(
                        src_ref=esend.at[there * nc + tc],
                        dst_ref=erecv.at[group, side],
                        send_sem=esem.at[0, len(to_experts)],
                        recv_sem=esem.at[1, len(to_experts)],
                        device_id=(z, first_y + there, tc, tx),
                        device_id_type=MESH,
                    )
                    copy.start()
                    to_experts.append(copy)
    erecv[group, side] = esend[side * nc + c]

    serves = jnp.logical_and(from_self, y // (ny // 2) == side)
    own_half = lax.rem(y, ny // 2) * nc + c

    @pl.when(serves)
    def _():
        turned = everyone32.T
        for k in range(owners // 2):
            msend[k] = turned[k * owned : (k + 1) * owned, :].astype(BF16)
        pltpu.make_async_copy(msend.at[own_half], mrecv, out_sem.at[2]).start()

    ready(*late)
    for copy in to_experts:
        copy.wait_recv()
    stacked = []
    for i in range(groups):
        left, right = erecv[i, 0].astype(F32), erecv[i, 1].astype(F32)
        left_turned = pltpu.roll(left, half_lanes, 1)
        right_turned = pltpu.roll(right, half_lanes, 1)
        tile = [jnp.where(low_slots, left, right_turned), jnp.where(low_slots, left_turned, right)]
        stacked.append(jnp.concatenate(tile, axis=0))
    stacked = jnp.concatenate(stacked, axis=1)
    scale = lax.rsqrt(jnp.mean(stacked * stacked, axis=1, keepdims=True) + EPS)
    gate_up = dot((stacked * fg[...]).astype(BF16), wgateup[...]) * scale
    gate_v, up_v = gate_up[:, 0:hidden], gate_up[:, hidden : 2 * hidden]
    act = (gate_v * jax.nn.sigmoid(gate_v) * up_v).astype(BF16)
    down = dot(act, wdown[...]).astype(BF16)
    for i in range(groups):
        rsend[i] = down[:, i * LANES : (i + 1) * LANES]

    def result_of(tx, tc):
        return lax.rem(tx + nx - lax.rem(z, nx), nx) * nc + tc

    to_groups = chip_row(rsend, rrecv, rsem, result_of, group)
    rrecv[group] = rsend[result_group]

    middle_copies = []
    for dx in x_order:
        for dy in (1, 0):
            for dc in reversed(range(nc)):
                if dx + dy + dc > 0:
                    tx, tc = lax.rem(x + dx, nx), lax.rem(c + dc, nc)
                    ty = y if dy == 0 else y + 1 - 2 * side
                    copy = pltpu.make_async_remote_copy(
                        src_ref=msend.at[lax.rem(ty, ny // 2) * nc + tc],
                        dst_ref=mrecv,
                        send_sem=msem.at[0],
                        recv_sem=msem.at[1],
                        device_id=(z, ty, tc, tx),
                        device_id_type=MESH,
                    )
                    middle_copies.append(copy)

    @pl.when(serves)
    def _():
        for copy in middle_copies:
            copy.start()

    for copy in to_groups:
        copy.wait_recv()
    results = []
    for i in range(nc):
        result = rrecv[i].astype(F32)
        for j in range(1, nx):
            result = result + rrecv[j * nc + i].astype(F32)
        results.append(result)
    low = lax.broadcasted_iota(jnp.int32, (owners, owned // 2, LANES), 2) < slots_here
    turned = jnp.concatenate(results + results, axis=0).T.reshape(owners, owned, LANES)
    half = owned // 2
    dsend[...] = jnp.where(low, turned[:, :half], turned[:, half:]).astype(BF16)

    def send_owners(i, carry):
        shift = ny // 2 + jnp.where(i % 2 == 0, i // 2, -((i + 1) // 2))
        ty = lax.rem(y + shift, ny)

        def send(tc, tx):
            pltpu.make_async_remote_copy(
                src_ref=dsend.at[ty * nc + tc],
                dst_ref=frecv.at[zy],
                send_sem=dsem.at[0],
                recv_sem=dsem.at[1],
                device_id=(result_group, ty, tc, tx),
                device_id_type=MESH,
            ).start()

        for dx in x_order:
            tx = lax.rem(x + dx, nx)
            for dc in reversed(range(nc)):
                tc = lax.rem(c + dc, nc)
                if dx == 0 and dc == 0:

                    @pl.when(jnp.logical_not(jnp.logical_and(result_from_self, i == ny - 1)))
                    def _():
                        send(tc, tx)
                else:
                    send(tc, tx)
        return carry

    lax.fori_loop(0, ny, send_owners, 0)

    def arrivals(n):
        part = frecv.at[pl.ds(0, n)]
        return pltpu.make_async_remote_copy(
            src_ref=part,
            dst_ref=part,
            send_sem=dsem.at[0],
            recv_sem=dsem.at[1],
            device_id=(z, y, lax.rem(c + 1, nc), x),
            device_id_type=MESH,
        )

    @pl.when(result_from_self)
    def _():
        own = pltpu.make_async_copy(dsend.at[lax.rem(ep, owners)], frecv.at[zy], out_sem.at[3])
        own.start()
        arrivals(chips - 1).wait_recv()
        own.wait()

    @pl.when(jnp.logical_not(result_from_self))
    def _():
        arrivals(chips).wait_recv()

    @pl.when(serves)
    def _():
        pltpu.make_async_copy(msend.at[own_half], mrecv, out_sem.at[2]).wait()

    @pl.when(jnp.logical_not(serves))
    def _():
        middle_copies[0].wait_recv()

    for copy in keeps:
        copy.wait()

    for dx in range(1, nx):
        pltpu.make_async_remote_copy(
            src_ref=psend.at[0],
            dst_ref=precv.at[dx - 1],
            send_sem=psem.at[0, dx - 1],
            recv_sem=psem.at[1, dx - 1],
            device_id=(z, y, c, lax.rem(x + dx, nx)),
            device_id_type=MESH,
        ).wait_send()
    plane.wait_send()
    for copy in to_experts + to_groups:
        copy.wait_send()

    @pl.when(result_from_self)
    def _():
        arrivals(chips - 1).wait_send()

    @pl.when(jnp.logical_not(result_from_self))
    def _():
        arrivals(chips).wait_send()

    @pl.when(serves)
    def _():
        for copy in middle_copies:
            copy.wait_send()


def lane_of(name):
    return jnp.bitwise_and(name, LANES - 1).astype(F32).astype(BF16)


def combine(
    parts_h,
    mid_h,
    tgt_h,
    rw_h,
    pack_h,
    state_h,
    mixed_h,
    newmem_h,
    newnorm_h,
    newmax_h,
    mixed,
    newnorm,
    newmax,
    parts,
    mid,
    tgt,
    rw,
    pack,
    state,
    load_sem,
    state_sem,
    sem,
):
    rows, qk, dv = state.shape
    chips, half, _ = parts.shape
    owned = 2 * half
    token_count = tgt.shape[1]
    loads = []
    for i, (h, v) in enumerate(
        ((pack_h, pack), (parts_h, parts), (tgt_h, tgt), (mid_h, mid), (rw_h, rw))
    ):
        loads.append(pltpu.make_async_copy(h, v, load_sem.at[i]))
    moves = [pltpu.make_async_copy(state_h.at[t], state.at[t], state_sem.at[t]) for t in range(rows)]
    for copy in loads + moves:
        copy.start()
    for copy in loads:
        copy.wait()
    newnorm[...] = pack[:, 0:qk]
    diagonal = lax.broadcasted_iota(jnp.int32, (rows, LANES), 0) == lax.broadcasted_iota(
        jnp.int32, (rows, LANES), 1
    )
    newmax[...] = jnp.sum(jnp.where(diagonal, pack[:, qk:], 0.0), axis=0, keepdims=True)[:, :rows]
    copies = []

    low = lax.broadcasted_iota(jnp.int32, (chips // 2, half, LANES), 2) < LANES // 2
    both = parts[...].astype(F32).reshape(chips // 2, 2, half, LANES)
    even, odd = both[:, 0], both[:, 1]
    even_turned = pltpu.roll(even, LANES // 2, 2)
    odd_turned = pltpu.roll(odd, LANES // 2, 2)
    held = jnp.concatenate(
        [jnp.where(low, even, odd_turned), jnp.where(low, even_turned, odd)], axis=1
    )
    held = held.reshape(chips // 2 * owned, LANES).astype(BF16)
    lane_id = lax.broadcasted_iota(jnp.int32, (LANES, LANES), 0).astype(F32).astype(BF16)
    for k in range(token_count // LANES):
        if k == min(2, token_count // LANES - 1):
            for t in range(rows):
                moves[t].wait()
                copy = pltpu.make_async_copy(state.at[t], newmem_h.at[t], sem.at[t])
                copy.start()
                copies.append(copy)
        span = slice(k * LANES, (k + 1) * LANES)
        names = [tgt[j : j + 1, span] for j in range(2)]
        picks = jnp.concatenate(
            [
                jnp.where(lane_id == lane_of(n), jnp.ones((), BF16), jnp.zeros((), BF16))
                for n in names
            ],
            axis=1,
        )
        found = dot(held, picks)
        total = []
        for j in range(2):
            place = jnp.broadcast_to(lax.shift_right_logical(names[j], 7), (owned, LANES))
            got = jnp.zeros((owned, LANES), F32)
            for p in range(chips // 2):
                part = found[p * owned : (p + 1) * owned, j * LANES : (j + 1) * LANES]
                got = jnp.where(place == p, part, got)
            total.append(got)
        w0, w1 = rw[0:1, span], rw[1:2, span]
        weighed = total[0] * (w0 / (w0 + w1)) + total[1] * (w1 / (w0 + w1))
        mixed[:, span] = (mid[:, span].astype(F32) + weighed).astype(BF16)
    outs = ((mixed, mixed_h), (newnorm, newnorm_h), (newmax, newmax_h))
    for i, (v, h) in enumerate(outs):
        copy = pltpu.make_async_copy(v, h, sem.at[rows + i])
        copy.start()
        copies.append(copy)
    for copy in copies:
        copy.wait()


def shards(
    sizes,
    tokens,
    mix_gain,
    w_query,
    w_key,
    w_value,
    w_ogate,
    w_igate,
    w_fgate,
    forget_bias,
    head_gain,
    w_out,
    memory,
    normalizer,
    running_max,
    ffn_gain,
    route,
    route_weight,
    w_gate,
    w_up,
    w_down,
):
    nz, ny, nc, nx = sizes
    rows, width = tokens.shape
    qk, dv = memory.shape[2:]
    chips = nz * ny
    quarter = width // nx
    groups = nx * nc
    owned = width // (chips * nc)
    owners = LANES // owned
    token_count = route.shape[0]
    operands = (
        tokens,
        mix_gain.reshape(1, -1),
        w_query,
        w_key,
        w_value,
        w_ogate,
        w_igate.T,
        w_fgate.T,
        forget_bias.reshape(1, -1),
        head_gain.reshape(1, -1),
        w_out,
        memory.reshape(rows, qk, dv),
        normalizer.reshape(rows, qk),
        running_max.T,
        ffn_gain.reshape(1, -1),
        route.T,
        w_gate[0],
        w_up[0],
        w_down[0],
    )
    shape = jax.ShapeDtypeStruct
    hbm = pl.BlockSpec(memory_space=pl.ANY)
    pack_width = LANES + qk
    held = [pltpu.VMEM(a.shape, a.dtype) for a in operands]
    held[2] = pltpu.VMEM((width, 2 * qk), BF16)
    held[16] = pltpu.VMEM((width, 2 * w_gate.shape[2]), BF16)
    del held[17], held[3]
    parts, mid, tgt, pack, state = pl.pallas_call(
        functools.partial(kernel, sizes),
        out_shape=(
            shape((chips, owned // 2, LANES), BF16),
            shape((owned, token_count), BF16),
            shape((2, token_count), jnp.int32),
            shape((rows, pack_width), F32),
            shape((rows, qk, dv), F32),
        ),
        in_specs=[hbm] * len(operands),
        out_specs=(hbm,) * 5,
        scratch_shapes=held
        + [
            pltpu.SemaphoreType.DMA((len(operands),)),
            pltpu.VMEM((2, token_count), jnp.int32),
            pltpu.VMEM((rows, pack_width), F32),
            pltpu.VMEM((2 * nc * CAP, token_count), BF16),
            pltpu.VMEM((nx, rows, quarter), BF16),
            pltpu.VMEM((nx - 1, rows, quarter), BF16),
            pltpu.VMEM((nc, 2, rows // 2, LANES), BF16),
            pltpu.VMEM((chips * nc, rows // 2, LANES), BF16),
            pltpu.VMEM((2 * nc, CAP // 2, LANES), BF16),
            pltpu.VMEM((groups, 2, CAP // 2, LANES), BF16),
            pltpu.VMEM((groups, CAP, LANES), BF16),
            pltpu.VMEM((groups, CAP, LANES), BF16),
            pltpu.VMEM((owners // 2, owned, token_count), BF16),
            pltpu.VMEM((owners, owned // 2, LANES), BF16),
            pltpu.SemaphoreType.DMA((2, nx - 1)),
            pltpu.SemaphoreType.DMA((2,)),
            pltpu.SemaphoreType.DMA((2, 2 * groups - 1)),
            pltpu.SemaphoreType.DMA((2, groups - 1)),
            pltpu.SemaphoreType.DMA((2,)),
            pltpu.SemaphoreType.DMA((2,)),
            pltpu.SemaphoreType.DMA((5,)),
            pltpu.SemaphoreType.REGULAR,
            pltpu.VMEM((rows, qk, dv), F32),
        ],
        compiler_params=pltpu.CompilerParams(collective_id=0, has_side_effects=True),
    )(*operands)
    mixed, state, new_norm, new_max = pl.pallas_call(
        combine,
        out_shape=(
            shape((owned, token_count), BF16),
            shape((rows, qk, dv), F32),
            shape((rows, qk), F32),
            shape((1, rows), F32),
        ),
        in_specs=[hbm] * 6,
        out_specs=(hbm,) * 4,
        scratch_shapes=[
            pltpu.VMEM((owned, token_count), BF16),
            pltpu.VMEM((rows, qk), F32),
            pltpu.VMEM((1, rows), F32),
            pltpu.VMEM((chips, owned // 2, LANES), BF16),
            pltpu.VMEM((owned, token_count), BF16),
            pltpu.VMEM((2, token_count), jnp.int32),
            pltpu.VMEM((2, token_count), F32),
            pltpu.VMEM((rows, pack_width), F32),
            pltpu.VMEM((rows, qk, dv), F32),
            pltpu.SemaphoreType.DMA((5,)),
            pltpu.SemaphoreType.DMA((rows,)),
            pltpu.SemaphoreType.DMA((rows + 3,)),
        ],
    )(parts, mid, tgt, route_weight.T, pack, state)
    return (mixed.T, state[:, None], new_norm[:, None], new_max.T)


def solution(mesh):
    nx = mesh.shape["tp"]
    nc = 2
    nz = nx * nc
    ny = mesh.shape["ep"] // (nc * nz)
    finer = Mesh(mesh.devices.reshape(nz, ny, nc, nx), ("z", "y", "c", "x"))
    ep = ("z", "y", "c")
    in_specs = (
        P(ep, None),
        P(),
        P(None, "x"),
        P(None, "x"),
        P(None, "x"),
        P(None, "x"),
        P(),
        P(),
        P(),
        P("x"),
        P("x", None),
        P(ep, "x", None, None),
        P(ep, "x", None),
        P(ep, "x"),
        P(),
        P(),
        P(),
        P(ep, None, "x"),
        P(ep, None, "x"),
        P(ep, "x", None),
    )
    out_specs = (P(None, ep), P(ep, "x", None, None), P(ep, "x", None), P(ep, "x"))
    return jax.shard_map(
        functools.partial(shards, (nz, ny, nc, nx)),
        mesh=finer,
        in_specs=in_specs,
        out_specs=out_specs,
        check_vma=False,
    )
```
